256 devices in a mesh: sp: 16 (over y, x), tp: 16 (over z, core).
Axes of the slice: x: 4, y: 4, z: 8, core: 2. Of those that a mesh axis runs over, the one named last changes fastest.
Arguments:
- tokens: bfloat16 [8192, 2048], P(('sp', 'tp')), may hold values from -6 to 6
- query_vectors: bfloat16 [8192, 2048], P('sp', 'tp'), may hold values from -8 to 8
- key_vectors: bfloat16 [8192, 2048], P('sp', 'tp'), may hold values from -8 to 8
- value_vectors: bfloat16 [8192, 2048], P('sp', 'tp'), may hold values from -24 to 24
- cum_gate: float32 [8192, 32], P('sp', 'tp'), may hold values from -1028 to 0, as said below
- out_weight: bfloat16 [2048, 2048], P('tp'), may hold values from -0.125 to 0.125
- norm_gain: float32 [2048], replicated, may hold values from 0.1 to 1.9
- gate_weight: bfloat16 [16, 2048, 7168], P('sp', None, 'tp'), may hold values from -0.125 to 0.125
- up_weight: bfloat16 [16, 2048, 7168], P('sp', None, 'tp'), may hold values from -0.125 to 0.125
- down_weight: bfloat16 [16, 7168, 2048], P('sp', 'tp'), may hold values from -0.0625 to 0.0625
- expert_ids: int32 [8192, 2], P(('sp', 'tp')), may hold values from 0 to 15, all different within a row; in each aligned block of 32 rows (0 to 31, 32 to 63, ...) at most 6 rows name the same one
- route_weights: float32 [8192, 2], P(('sp', 'tp')), may hold values from 0.2 to 1
Outputs:
- layer_output: bfloat16 [8192, 2048], P(('sp', 'tp'))
The draws below stay inside these ranges and needn't reach their ends.
Inputs may be any that keep to these rules, and one draw needn't show every extreme that they name: `cum_gate`: along the positions each head's values never rise. `expert_ids`: within the rows of one device no expert is named by more than 6 rows, and in some devices' rows one expert is named by exactly 6; a row names 2 different experts.
All inputs are finite; a program needn't handle non-finite values.
Results may differ from the reference program's by a relative error of at most 0.014.
Values may be sent and summed in bfloat16 or wider, within the bound.
A program may use at most 128 MiB of HBM per device.

```python
import math
import jax
import jax.numpy as jnp
import numpy as np
from jax import lax

D = 2048
HEAD_COUNT = 32
HEAD_DIM = 64
FFE = 7168
TOP = 2
TOK_SP = 512
EXPERTS = 16
TOKEN_COUNT = 8192
TOK_DEV = 32
CAP = 6


def paired_draw(key):
    parallel_flows = jax.random.split(jax.random.fold_in(key, 101), 2)
    width = HEAD_COUNT * HEAD_DIM
    query_part = jax.random.truncated_normal(parallel_flows[0], -6.0, 6.0, (TOKEN_COUNT, width), jnp.float32)
    key_part = jax.random.truncated_normal(parallel_flows[1], -6.0, 6.0, (TOKEN_COUNT, width), jnp.float32)
    return (query_part, key_part)


def draw_query_vectors(key, part):
    query_part, key_part = paired_draw(key)
    return query_part.astype(jnp.bfloat16)


def draw_key_vectors(key, part):
    query_part, key_part = paired_draw(key)
    return key_part.astype(jnp.bfloat16)


def draw_cum_gate(key, part):
    parallel_flows = jax.random.split(jax.random.fold_in(key, 202), 7)
    slow_cut = 8
    slow = jax.random.randint(parallel_flows[0], (HEAD_COUNT,), 0, 16) < slow_cut
    fast_rate = jnp.exp(jax.random.uniform(parallel_flows[1], (HEAD_COUNT,), jnp.float32, math.log(1.0 / 100.0), math.log(1.0 / 30.0)))
    slow_rate = jnp.exp(jax.random.uniform(parallel_flows[2], (HEAD_COUNT,), jnp.float32, 0.0, math.log(3.0))) / TOKEN_COUNT
    rate = jnp.where(slow, slow_rate, fast_rate)
    blocks = TOKEN_COUNT // TOK_SP
    step_levels = 2.0 ** jnp.linspace(-1.0, 1.0, blocks)
    step_levels = step_levels[jax.random.permutation(parallel_flows[3], blocks)]
    factor = jnp.repeat(step_levels, TOK_SP)
    rough = jax.random.uniform(parallel_flows[4], (TOKEN_COUNT, HEAD_COUNT), jnp.float32, 0.3, 1.7)
    descending_steps = rate[None, :] * factor[:, None] * rough
    spike_position = jax.random.randint(parallel_flows[5], (4,), 0, TOKEN_COUNT)
    spike_penalty = -jnp.log(1.0 - jax.random.uniform(parallel_flows[6], (4, HEAD_COUNT), jnp.float32, 0.2, 0.5))
    descending_steps = descending_steps.at[spike_position].add(spike_penalty)
    return jnp.cumsum(-descending_steps, axis=0)


def level_of(rng, shape, cuts, least, top_value):
    gain, own = 1.0, jax.random.fold_in(rng, 6)
    for dim, parts in cuts:
        draws = jnp.exp(jax.random.uniform(jax.random.fold_in(own, dim), (parts,), jnp.float32, least / len(cuts), top_value / len(cuts)))
        gain = gain * jnp.repeat(draws, shape[dim] // parts).reshape([-1 if axis == dim else 1 for axis in range(len(shape))])
    return gain


def routed_block(key, own, number, rows, count, top, limit, slope):
    ranking = jax.random.permutation(key, count)
    crowded, ordinary = portions_of(count, rows * top, limit, slope, True), portions_of(count, rows * top, limit, slope, False)
    places = jnp.arange(count)

    def named(tallies, offset_by):
        used = int((tallies > 0).sum())
        fixed = max(1, used // 4)
        passed = fixed + (places - fixed + offset_by * (used - fixed)) % max(1, count - fixed)
        return jnp.zeros((count,), jnp.int32).at[ranking[jnp.where(places < fixed, places, passed)]].set(jnp.asarray(tallies, jnp.int32))

    tallies = jnp.where(number % 4 == 0, named(crowded, number // 4), named(ordinary, number - number // 4 - 1))
    mixed = jax.random.permutation(jax.random.fold_in(own, 3), count)
    giver, receiver = mixed[0:count // 2 * 2:2], mixed[1:count // 2 * 2:2]
    slack = jnp.minimum(tallies[giver] - 1, limit - tallies[receiver]) // 2
    slack = jnp.where((giver == ranking[0]) | (receiver == ranking[0]) | (tallies[receiver] == 0), 0, jnp.maximum(slack, 0))
    passed = jax.random.randint(jax.random.fold_in(own, 4), (count // 2,), 0, 1 << 20) % (slack + 1)
    tallies = tallies.at[giver].add(-passed).at[receiver].add(passed)
    items = jnp.searchsorted(jnp.cumsum(tallies), jnp.arange(rows * top), side="right").astype(jnp.int32)
    listing = items.reshape(top, rows).T
    listing = listing[jax.random.permutation(jax.random.fold_in(own, 1), rows)]
    offset_by = jax.random.randint(jax.random.fold_in(own, 2), (rows, 1), 0, top)
    return jnp.take_along_axis(listing, (jnp.arange(top)[None, :] + offset_by) % top, axis=1)


def portions_of(count, total, most, skew, full):
    weights = [(1 << 20) // math.isqrt(grade ** skew) + 1 for grade in range(1, count + 1)]
    largest = most if full else min(most, max(-(-total // count), total * weights[0] // sum(weights)))
    least = 1 if total - largest >= count - 1 else 0
    given, surplus = [largest] + [least] * (count - 1), total - largest - least * (count - 1)
    while surplus > 0:
        free = [i for i in range(1, count) if given[i] < largest] or [i for i in range(1, count) if given[i] < most]
        mass, left = sum([weights[i] for i in free]), surplus
        for i in free:
            addition = min(most - given[i], max(1, left * weights[i] // mass), surplus)
            given[i] = given[i] + addition
            surplus = surplus - addition
    return np.array(given)


def scatter_about(key, extent, spread, reach, cuts=(), kind=jnp.bfloat16):
    loudness = level_of(key, extent, cuts, -0.22, 0.18) if cuts else 1.0
    entries = jax.random.normal(key, extent, jnp.float32) * spread * loudness
    return jnp.minimum(jnp.maximum(entries, -reach), reach).astype(kind)


def setup_inputs(seed: int = 0) -> dict:
    key_list = jax.random.split(jax.random.key(seed), 13)
    tokens = scatter_about(key_list[0], (TOKEN_COUNT, D), 1.0, 6.0, ((0, 256),))
    query_vectors = draw_query_vectors(jax.random.fold_in(key_list[12], 71), 0)
    key_vectors = draw_key_vectors(jax.random.fold_in(key_list[12], 71), 0)
    value_vectors = scatter_about(key_list[3], (TOKEN_COUNT, HEAD_COUNT * HEAD_DIM), 4.0, 24.0, ((0, 16), (1, 16)))
    cum_gate = draw_cum_gate(jax.random.fold_in(key_list[12], 71), 0)
    out_weight = scatter_about(key_list[5], (HEAD_COUNT * HEAD_DIM, D), (HEAD_COUNT * HEAD_DIM) ** -0.5, 0.125, ((0, 16),))
    norm_gain = jnp.clip(1.0 + 0.18 * jax.random.normal(key_list[6], (D,), jnp.float32), 0.1, 1.9)
    gate_weight = scatter_about(key_list[7], (EXPERTS, D, FFE), D ** -0.5, 0.125, ((0, 16), (2, 16)))
    up_weight = scatter_about(key_list[8], (EXPERTS, D, FFE), D ** -0.5, 0.125, ((0, 16), (2, 16)))
    down_weight = scatter_about(key_list[9], (EXPERTS, FFE, D), FFE ** -0.5, 0.0625, ((0, 16), (1, 16)))
    expert_ids_keys = jax.random.split(jax.random.fold_in(key_list[10], 1), TOKEN_COUNT // TOK_DEV)
    expert_ids_turns = jax.random.permutation(jax.random.fold_in(key_list[10], 3), TOKEN_COUNT // TOK_DEV)
    expert_ids = jax.vmap(lambda own, number: routed_block(jax.random.fold_in(key_list[10], 2), own, number, TOK_DEV, EXPERTS, TOP, CAP, 1))(expert_ids_keys, expert_ids_turns).reshape((TOKEN_COUNT, TOP))
    route_weights = jnp.clip(0.2 + 0.8 * jax.random.uniform(key_list[11], (TOKEN_COUNT, TOP), jnp.float32) ** level_of(key_list[11], (TOKEN_COUNT, TOP), ((0, 256),), -0.2, 0.2), 0.2, 1.0)
    return {"tokens": tokens, "query_vectors": query_vectors, "key_vectors": key_vectors, "value_vectors": value_vectors, "cum_gate": cum_gate, "out_weight": out_weight, "norm_gain": norm_gain, "gate_weight": gate_weight, "up_weight": up_weight, "down_weight": down_weight, "expert_ids": expert_ids, "route_weights": route_weights}


def reference(tokens, query_vectors, key_vectors, value_vectors, cum_gate, out_weight, norm_gain, gate_weight, up_weight, down_weight, expert_ids, route_weights):
    score_scale = HEAD_DIM ** (-0.5)
    query_block = math.gcd(TOKEN_COUNT, 512)
    block_count = TOKEN_COUNT // query_block
    all_positions = jnp.arange(TOKEN_COUNT, dtype=jnp.int32)

    def head_output(head_index):
        column = (head_index * HEAD_DIM).astype(jnp.int32)
        query_head = lax.dynamic_slice_in_dim(query_vectors, column, HEAD_DIM, 1)
        key_head = lax.dynamic_slice_in_dim(key_vectors, column, HEAD_DIM, 1)
        value_head = lax.dynamic_slice_in_dim(value_vectors, column, HEAD_DIM, 1)
        gate_head = lax.dynamic_slice_in_dim(cum_gate, head_index.astype(jnp.int32), 1, 1)[:, 0]

        def block_output(block_index):
            first_row = (block_index * query_block).astype(jnp.int32)
            query_rows = lax.dynamic_slice_in_dim(query_head, first_row, query_block, 0)
            gate_rows = lax.dynamic_slice_in_dim(gate_head, first_row, query_block, 0)
            scores = jnp.dot(query_rows, key_head.T, preferred_element_type=jnp.float32) * score_scale
            scores = scores + gate_rows[:, None] - gate_head[None, :]
            query_pos = first_row + jnp.arange(query_block, dtype=jnp.int32)
            visible = all_positions[None, :] <= query_pos[:, None]
            scores = jnp.where(visible, scores, -jnp.inf)
            peak = lax.optimization_barrier(jnp.max(scores, axis=1, keepdims=True))
            exponent = jnp.exp(scores - peak)
            denominator = lax.optimization_barrier(jnp.sum(exponent, axis=1))
            probs = exponent.astype(jnp.bfloat16)
            summed = jnp.dot(probs, value_head, preferred_element_type=jnp.float32)
            return (summed / denominator[:, None]).astype(jnp.bfloat16)
        blocks = lax.map(block_output, jnp.arange(block_count, dtype=jnp.int32))
        return blocks.reshape(TOKEN_COUNT, HEAD_DIM)
    per_head = lax.map(head_output, jnp.arange(HEAD_COUNT, dtype=jnp.int32))
    attended = per_head.transpose(1, 0, 2).reshape(TOKEN_COUNT, HEAD_COUNT * HEAD_DIM)
    projected = jnp.dot(attended, out_weight, preferred_element_type=jnp.float32)
    stream = (tokens.astype(jnp.float32) + projected).astype(jnp.bfloat16)
    stream_wide = stream.astype(jnp.float32)
    inverse = lax.rsqrt(lax.optimization_barrier(jnp.mean(stream_wide * stream_wide, axis=1, keepdims=True)) + 1e-05)
    normed = (stream_wide * inverse * norm_gain[None, :]).astype(jnp.bfloat16)
    route_count = TOKEN_COUNT * TOP
    most_rows = TOKEN_COUNT // TOK_DEV * CAP
    flat_ids = expert_ids.reshape(-1)
    route_order = jnp.arange(route_count, dtype=jnp.int32)

    def expert_pass(routed_out, expert_index):
        sort_keys = jnp.where(flat_ids == expert_index, 0, 1) * route_count + route_order
        chosen = jnp.argsort(sort_keys)[:most_rows].astype(jnp.int32)
        valid = flat_ids[chosen] == expert_index
        rows_in = normed[chosen // TOP]
        gate_value = jnp.dot(rows_in, gate_weight[expert_index], preferred_element_type=jnp.float32)
        up_value = jnp.dot(rows_in, up_weight[expert_index], preferred_element_type=jnp.float32)
        hidden = (jax.nn.silu(gate_value) * up_value).astype(jnp.bfloat16)
        expert_out = jnp.dot(hidden, down_weight[expert_index], preferred_element_type=jnp.float32).astype(jnp.bfloat16)
        current = routed_out[chosen]
        routed_out = routed_out.at[chosen].set(jnp.where(valid[:, None], expert_out, current))
        return (routed_out, None)
    routed_out, _ = lax.scan(expert_pass, jnp.zeros((route_count, D), jnp.bfloat16), jnp.arange(EXPERTS, dtype=jnp.int32))
    routed = routed_out.reshape(TOKEN_COUNT, TOP, D).astype(jnp.float32)
    mixture = lax.optimization_barrier(jnp.sum(routed * route_weights[:, :, None], axis=1))
    return (stream_wide + mixture).astype(jnp.bfloat16)
```

```python
import functools
import math

import jax
import jax.numpy as jnp
from jax import lax
from jax.experimental import pallas as pl
from jax.experimental.pallas import tpu as pltpu
from jax.sharding import PartitionSpec as P

NEG_LARGE = -1e30
MESH = pl.DeviceIdType.MESH


def attention_kernel(
    n,
    n_tp,
    tok_dev,
    coef,
    q_ref,
    kv_ref,
    bias_ref,
    out_ref,
    qraw,
    qbuf,
    kvbuf,
    bbuf,
    peak,
    total,
    acc,
    obuf,
    rbuf,
    kv_send,
    kv_recv,
    b_send,
    b_recv,
    q_send,
    q_recv,
    o_send,
    o_recv,
):
    me = lax.axis_index("sp")
    mt = lax.axis_index("tp")
    head = lax.rem(me, 2)
    pair = lax.div(me, 2)
    rows = q_ref.shape[0]
    width = q_ref.shape[1]
    half = width // 2
    last = n - 1 - pair

    def kv_copy(r):
        hr = lax.rem(r, 2)
        return (
            pltpu.make_async_remote_copy(
                src_ref=kv_ref.at[hr],
                dst_ref=kvbuf.at[me],
                send_sem=kv_send.at[r],
                recv_sem=kv_recv.at[me],
                device_id=(r, mt),
                device_id_type=MESH,
            ),
            pltpu.make_async_remote_copy(
                src_ref=bias_ref.at[hr],
                dst_ref=bbuf.at[me],
                send_sem=b_send.at[r],
                recv_sem=b_recv.at[me],
                device_id=(r, mt),
                device_id_type=MESH,
            ),
        )

    q_slot = jnp.where(me < n // 2, 0, 1)
    q_target = 2 * jnp.minimum(me, n - 1 - me)

    def q_copy(h):
        return pltpu.make_async_remote_copy(
            src_ref=q_ref,
            dst_ref=qraw.at[q_slot],
            send_sem=q_send.at[h],
            recv_sem=q_recv.at[q_slot],
            device_id=(q_target + h, mt),
            device_id_type=MESH,
        )

    def q_local():
        return pltpu.make_async_copy(q_ref, qraw.at[q_slot], q_recv.at[q_slot])

    for h in range(2):

        @pl.when(q_target + h != me)
        def _():
            q_copy(h).start()

        @pl.when(q_target + h == me)
        def _():
            q_local().start()

    local_kv = pltpu.make_async_copy(kv_ref.at[head], kvbuf.at[me], kv_recv.at[me])
    local_b = pltpu.make_async_copy(bias_ref.at[head], bbuf.at[me], b_recv.at[me])

    @pl.when(me <= last)
    def _():
        local_kv.start()
        local_b.start()

    def send_body(k, c):
        r = lax.rem(me + k, n)

        @pl.when(me <= n - 1 - lax.div(r, 2))
        def _():
            ck, cb = kv_copy(r)
            cb.start()
            ck.start()

        return c

    lax.fori_loop(1, n, send_body, 0)

    lane = lax.broadcasted_iota(jnp.int32, (rows, width), 1)
    mine = (lane >= half) == (head == 0)
    for slot in range(2):
        pltpu.make_async_copy(q_ref, qraw.at[slot], q_recv.at[slot]).wait()
        qbuf[slot] = jnp.where(mine, qraw[slot].astype(jnp.float32), 0.0).astype(jnp.bfloat16)
    peak[...] = jnp.full(peak.shape, NEG_LARGE, jnp.float32)
    total[...] = jnp.zeros(total.shape, jnp.float32)
    acc[...] = jnp.zeros(acc.shape, jnp.float32)

    sub = min(256, rows)

    def tile(slot, j, diagonal):
        kv = kvbuf[j]
        bias = bbuf[j]
        for i in range(rows // sub):
            rs = pl.ds(i * sub, sub)
            s = lax.dot_general(
                qbuf[slot, rs, :], kv, (((1,), (1,)), ((), ())), preferred_element_type=jnp.float32
            )
            s = s * coef + bias
            if diagonal:
                qp = lax.broadcasted_iota(jnp.int32, s.shape, 0) + i * sub
                kp = lax.broadcasted_iota(jnp.int32, s.shape, 1)
                s = jnp.where(kp <= qp, s, NEG_LARGE)
            old = peak[slot, rs, :]
            new = jnp.maximum(old, jnp.max(s, axis=1, keepdims=True))
            e = jnp.exp2(s - new)
            alpha = jnp.exp2(old - new)
            total[slot, rs, :] = total[slot, rs, :] * alpha + jnp.sum(e, axis=1, keepdims=True)
            acc[slot, rs, :] = acc[slot, rs, :] * alpha + jnp.dot(
                e.astype(jnp.bfloat16), kv, preferred_element_type=jnp.float32
            )
            peak[slot, rs, :] = new

    def compute_body(k, c):
        j = lax.rem(me - k + n, n)

        @pl.when(j <= last)
        def _():
            pltpu.make_async_copy(kv_ref.at[0], kvbuf.at[j], kv_recv.at[j]).wait()
            pltpu.make_async_copy(bias_ref.at[0], bbuf.at[j], b_recv.at[j]).wait()

            @pl.when(j == last)
            def _():
                tile(1, j, True)

            @pl.when(j < last)
            def _():
                tile(1, j, False)

            @pl.when(j == pair)
            def _():
                tile(0, j, True)

            @pl.when(j < pair)
            def _():
                tile(0, j, False)

        return c

    lax.fori_loop(0, n, compute_body, 0)

    for slot in range(2):
        obuf[slot] = (acc[slot] / total[slot]).astype(jnp.bfloat16)

    def o_copy(slot, t):
        chunk = jnp.where(slot == 0, pair, last)
        return pltpu.make_async_remote_copy(
            src_ref=obuf.at[slot, pl.ds(t * tok_dev, tok_dev)],
            dst_ref=rbuf.at[mt, head],
            send_sem=o_send.at[slot, t],
            recv_sem=o_recv,
            device_id=(chunk, t),
            device_id_type=MESH,
        )

    def o_self(slot, t):
        chunk = jnp.where(slot == 0, pair, last)
        return jnp.logical_and(chunk == me, t == mt)

    def o_body(k, c):
        slot = lax.div(k, n_tp)
        t = lax.rem(mt + lax.rem(k, n_tp), n_tp)

        @pl.when(jnp.logical_not(o_self(slot, t)))
        def _():
            o_copy(slot, t).start()

        @pl.when(o_self(slot, t))
        def _():
            pltpu.make_async_copy(
                obuf.at[slot, pl.ds(t * tok_dev, tok_dev)], rbuf.at[mt, head], o_recv
            ).start()

        return c

    lax.fori_loop(0, 2 * n_tp, o_body, 0)

    pltpu.make_async_copy(rbuf, rbuf, o_recv).wait()
    lane32 = lax.broadcasted_iota(jnp.int32, (tok_dev, width), 1)
    for t in range(n_tp):
        out_ref[:, t * width : (t + 1) * width] = jnp.where(
            lane32 < half, rbuf[t, 0].astype(jnp.float32), rbuf[t, 1].astype(jnp.float32)
        ).astype(jnp.bfloat16)

    for h in range(2):

        @pl.when(q_target + h != me)
        def _():
            q_copy(h).wait_send()

    def drain_body(k, c):
        r = lax.rem(me + k, n)

        @pl.when(me <= n - 1 - lax.div(r, 2))
        def _():
            ck, cb = kv_copy(r)
            cb.wait_send()
            ck.wait_send()

        return c

    lax.fori_loop(1, n, drain_body, 0)

    def o_drain(k, c):
        slot = lax.div(k, n_tp)
        t = lax.rem(mt + lax.rem(k, n_tp), n_tp)

        @pl.when(jnp.logical_not(o_self(slot, t)))
        def _():
            o_copy(slot, t).wait_send()

        return c

    lax.fori_loop(0, 2 * n_tp, o_drain, 0)


def attention(query_vectors, key_vectors, value_vectors, cum_gate, tok_dev):
    n = lax.axis_size("sp")
    n_tp = lax.axis_size("tp")
    rows, width = query_vectors.shape
    half = width // 2
    coef = half ** (-0.5) * math.log2(math.e)
    q_swapped = jnp.concatenate([query_vectors[:, half:], query_vectors[:, :half]], axis=1)
    kv = jnp.stack(
        [
            jnp.concatenate([value_vectors[:, :half], key_vectors[:, :half]], axis=1),
            jnp.concatenate([key_vectors[:, half:], value_vectors[:, half:]], axis=1),
        ]
    )
    bias = (cum_gate * (-math.log2(math.e))).T[:, None, :]
    vmem = pl.BlockSpec(memory_space=pltpu.VMEM)
    tiles = n + 1
    return pl.pallas_call(
        functools.partial(attention_kernel, n, n_tp, tok_dev, coef),
        out_shape=jax.ShapeDtypeStruct((tok_dev, n_tp * width), jnp.bfloat16),
        in_specs=[vmem] * 3,
        out_specs=vmem,
        scratch_shapes=[
            pltpu.VMEM((2, rows, width), jnp.bfloat16),
            pltpu.VMEM((2, rows, width), jnp.bfloat16),
            pltpu.VMEM((n, rows, width), jnp.bfloat16),
            pltpu.VMEM((n, 1, rows), jnp.float32),
            pltpu.VMEM((2, rows, 1), jnp.float32),
            pltpu.VMEM((2, rows, 1), jnp.float32),
            pltpu.VMEM((2, rows, width), jnp.float32),
            pltpu.VMEM((2, rows, width), jnp.bfloat16),
            pltpu.VMEM((n_tp, 2, tok_dev, width), jnp.bfloat16),
            pltpu.SemaphoreType.DMA((n,)),
            pltpu.SemaphoreType.DMA((n,)),
            pltpu.SemaphoreType.DMA((n,)),
            pltpu.SemaphoreType.DMA((n,)),
            pltpu.SemaphoreType.DMA((2,)),
            pltpu.SemaphoreType.DMA((2,)),
            pltpu.SemaphoreType.DMA((2, n_tp)),
            pltpu.SemaphoreType.DMA,
        ],
        compiler_params=pltpu.CompilerParams(has_side_effects=True),
        cost_estimate=pl.CostEstimate(
            flops=tiles * rows * rows * width * 4 * 8,
            bytes_accessed=4 << 20,
            transcendentals=tiles * rows * rows,
        ),
        name="attention",
    )(q_swapped, kv, bias)


def shards(
    tokens,
    query_vectors,
    key_vectors,
    value_vectors,
    cum_gate,
    out_weight,
    norm_gain,
    gate_weight,
    up_weight,
    down_weight,
    expert_ids,
    route_weights,
):
    sp_count = lax.axis_size("sp")
    tok_dev = tokens.shape[0]
    model_width = tokens.shape[1]
    token_rows = attention(query_vectors, key_vectors, value_vectors, cum_gate, tok_dev)
    projected = jnp.dot(
        token_rows,
        lax.all_gather(out_weight, "tp", axis=0, tiled=True),
        preferred_element_type=jnp.float32,
    )
    stream_wide = (tokens.astype(jnp.float32) + projected).astype(jnp.bfloat16).astype(jnp.float32)
    inverse = lax.rsqrt(jnp.mean(stream_wide * stream_wide, axis=1, keepdims=True) + 1e-05)
    normed = (stream_wide * inverse * norm_gain[None, :]).astype(jnp.bfloat16)
    n_experts = gate_weight.shape[0] * sp_count
    top_count = expert_ids.shape[1]
    capacity = max(2, 3 * tok_dev * top_count // (2 * n_experts))
    flat_ids = expert_ids.reshape(-1)
    hits = (flat_ids[:, None] == jnp.arange(n_experts, dtype=jnp.int32)[None, :]).astype(jnp.int32)
    earlier = jnp.cumsum(hits, axis=0) - hits
    slot_index = flat_ids * capacity + jnp.sum(earlier * hits, axis=1)
    placement_map = (
        jnp.arange(n_experts * capacity, dtype=jnp.int32)[:, None] == slot_index[None, :]
    ).astype(jnp.bfloat16)
    repeated = jnp.repeat(normed, top_count, axis=0)
    dispatch = jnp.dot(placement_map, repeated, preferred_element_type=jnp.float32).astype(
        jnp.bfloat16
    )
    dispatch = dispatch.reshape(n_experts, capacity, model_width)
    arrived = lax.all_to_all(dispatch, "sp", split_axis=0, concat_axis=0, tiled=True)
    row_block = arrived.reshape(-1, model_width)
    rows_in = lax.all_gather(row_block, "tp", axis=0, tiled=True)
    gate_value = jnp.dot(rows_in, gate_weight[0], preferred_element_type=jnp.float32)
    up_value = jnp.dot(rows_in, up_weight[0], preferred_element_type=jnp.float32)
    hidden = (jax.nn.silu(gate_value) * up_value).astype(jnp.bfloat16)
    summed = lax.psum_scatter(
        jnp.dot(hidden, down_weight[0], preferred_element_type=jnp.float32).astype(jnp.bfloat16),
        "tp",
        scatter_dimension=0,
        tiled=True,
    )
    returned = summed.reshape(arrived.shape)
    back = lax.all_to_all(returned, "sp", split_axis=0, concat_axis=0, tiled=True)
    flat_back = back.reshape(n_experts * capacity, model_width)
    picked = flat_back[slot_index].astype(jnp.float32).reshape(tok_dev, top_count, model_width)
    mixture = jnp.sum(picked * route_weights[:, :, None], axis=1)
    return (stream_wide + mixture).astype(jnp.bfloat16)


def solution(mesh):
    in_specs = (
        P(("sp", "tp"), None),
        P("sp", "tp"),
        P("sp", "tp"),
        P("sp", "tp"),
        P("sp", "tp"),
        P("tp", None),
        P(),
        P("sp", None, "tp"),
        P("sp", None, "tp"),
        P("sp", "tp", None),
        P(("sp", "tp"), None),
        P(("sp", "tp"), None),
    )
    out_specs = P(("sp", "tp"), None)
    return jax.shard_map(shards, mesh=mesh, in_specs=in_specs, out_specs=out_specs, check_vma=False)
```

```python
import functools
import math

import jax
import jax.numpy as jnp
from jax import lax
from jax.experimental import pallas as pl
from jax.experimental.pallas import tpu as pltpu
from jax.sharding import PartitionSpec as P

NEG_LARGE = -1e30
MESH = pl.DeviceIdType.MESH


def attention_kernel(
    n,
    n_tp,
    tok_dev,
    coef,
    q_ref,
    kv_ref,
    bias_ref,
    out_ref,
    qraw,
    qbuf,
    kvbuf,
    bbuf,
    peak,
    total,
    acc,
    obuf,
    rbuf,
    kv_send,
    kv_recv,
    b_send,
    b_recv,
    q_send,
    q_recv,
    o_send,
    o_recv,
):
    me = lax.axis_index("sp")
    mt = lax.axis_index("tp")
    head = lax.rem(me, 2)
    pair = lax.div(me, 2)
    rows = q_ref.shape[0]
    width = q_ref.shape[1]
    half = width // 2
    last = n - 1 - pair

    def kv_copy(r):
        hr = lax.rem(r, 2)
        return (
            pltpu.make_async_remote_copy(
                src_ref=kv_ref.at[hr],
                dst_ref=kvbuf.at[me],
                send_sem=kv_send.at[r],
                recv_sem=kv_recv.at[me],
                device_id=(r, mt),
                device_id_type=MESH,
            ),
            pltpu.make_async_remote_copy(
                src_ref=bias_ref.at[hr],
                dst_ref=bbuf.at[me],
                send_sem=b_send.at[r],
                recv_sem=b_recv.at[me],
                device_id=(r, mt),
                device_id_type=MESH,
            ),
        )

    q_slot = jnp.where(me < n // 2, 0, 1)
    q_target = 2 * jnp.minimum(me, n - 1 - me)

    def q_copy(h):
        return pltpu.make_async_remote_copy(
            src_ref=q_ref,
            dst_ref=qraw.at[q_slot],
            send_sem=q_send.at[h],
            recv_sem=q_recv.at[q_slot],
            device_id=(q_target + h, mt),
            device_id_type=MESH,
        )

    def q_local():
        return pltpu.make_async_copy(q_ref, qraw.at[q_slot], q_recv.at[q_slot])

    for h in range(2):

        @pl.when(q_target + h != me)
        def _():
            q_copy(h).start()

        @pl.when(q_target + h == me)
        def _():
            q_local().start()

    local_kv = pltpu.make_async_copy(kv_ref.at[head], kvbuf.at[me], kv_recv.at[me])
    local_b = pltpu.make_async_copy(bias_ref.at[head], bbuf.at[me], b_recv.at[me])

    @pl.when(me <= last)
    def _():
        local_kv.start()
        local_b.start()

    def send_body(k, c):
        r = lax.rem(me + k, n)

        @pl.when(me <= n - 1 - lax.div(r, 2))
        def _():
            ck, cb = kv_copy(r)
            cb.start()
            ck.start()

        return c

    lax.fori_loop(1, n, send_body, 0)

    lane = lax.broadcasted_iota(jnp.int32, (rows, width), 1)
    mine = (lane >= half) == (head == 0)
    for slot in range(2):
        pltpu.make_async_copy(q_ref, qraw.at[slot], q_recv.at[slot]).wait()
        qbuf[slot] = jnp.where(mine, qraw[slot].astype(jnp.float32), 0.0).astype(jnp.bfloat16)
    peak[...] = jnp.full(peak.shape, NEG_LARGE, jnp.float32)
    total[...] = jnp.zeros(total.shape, jnp.float32)
    acc[...] = jnp.zeros(acc.shape, jnp.float32)

    sub = min(256, rows)

    def tile(slot, j, diagonal):
        kv = kvbuf[j]
        bias = bbuf[j]
        for i in range(rows // sub):
            rs = pl.ds(i * sub, sub)
            s = lax.dot_general(
                qbuf[slot, rs, :], kv, (((1,), (1,)), ((), ())), preferred_element_type=jnp.float32
            )
            s = s * coef + bias
            if diagonal:
                qp = lax.broadcasted_iota(jnp.int32, s.shape, 0) + i * sub
                kp = lax.broadcasted_iota(jnp.int32, s.shape, 1)
                s = jnp.where(kp <= qp, s, NEG_LARGE)
            old = peak[slot, rs, :]
            new = jnp.maximum(old, jnp.max(s, axis=1, keepdims=True))
            e = jnp.exp2(s - new)
            alpha = jnp.exp2(old - new)
            total[slot, rs, :] = total[slot, rs, :] * alpha + jnp.sum(e, axis=1, keepdims=True)
            acc[slot, rs, :] = acc[slot, rs, :] * alpha + jnp.dot(
                e.astype(jnp.bfloat16), kv, preferred_element_type=jnp.float32
            )
            peak[slot, rs, :] = new

    def compute_body(k, c):
        j = lax.rem(me - k + n, n)

        @pl.when(j <= last)
        def _():
            pltpu.make_async_copy(kv_ref.at[0], kvbuf.at[j], kv_recv.at[j]).wait()
            pltpu.make_async_copy(bias_ref.at[0], bbuf.at[j], b_recv.at[j]).wait()

            @pl.when(j == last)
            def _():
                tile(1, j, True)

            @pl.when(j < last)
            def _():
                tile(1, j, False)

            @pl.when(j == pair)
            def _():
                tile(0, j, True)

            @pl.when(j < pair)
            def _():
                tile(0, j, False)

        return c

    lax.fori_loop(0, n, compute_body, 0)

    for slot in range(2):
        obuf[slot] = (acc[slot] / total[slot]).astype(jnp.bfloat16)

    def o_copy(slot, t):
        chunk = jnp.where(slot == 0, pair, last)
        return pltpu.make_async_remote_copy(
            src_ref=obuf.at[slot, pl.ds(t * tok_dev, tok_dev)],
            dst_ref=rbuf.at[mt, head],
            send_sem=o_send.at[slot, t],
            recv_sem=o_recv,
            device_id=(chunk, t),
            device_id_type=MESH,
        )

    def o_self(slot, t):
        chunk = jnp.where(slot == 0, pair, last)
        return jnp.logical_and(chunk == me, t == mt)

    def o_body(k, c):
        slot = lax.div(k, n_tp)
        t = lax.rem(mt + lax.rem(k, n_tp), n_tp)

        @pl.when(jnp.logical_not(o_self(slot, t)))
        def _():
            o_copy(slot, t).start()

        @pl.when(o_self(slot, t))
        def _():
            pltpu.make_async_copy(
                obuf.at[slot, pl.ds(t * tok_dev, tok_dev)], rbuf.at[mt, head], o_recv
            ).start()

        return c

    lax.fori_loop(0, 2 * n_tp, o_body, 0)

    pltpu.make_async_copy(rbuf, rbuf, o_recv).wait()
    lane32 = lax.broadcasted_iota(jnp.int32, (tok_dev, width), 1)
    for t in range(n_tp):
        out_ref[:, t * width : (t + 1) * width] = jnp.where(
            lane32 < half, rbuf[t, 0].astype(jnp.float32), rbuf[t, 1].astype(jnp.float32)
        ).astype(jnp.bfloat16)

    for h in range(2):

        @pl.when(q_target + h != me)
        def _():
            q_copy(h).wait_send()

    def drain_body(k, c):
        r = lax.rem(me + k, n)

        @pl.when(me <= n - 1 - lax.div(r, 2))
        def _():
            ck, cb = kv_copy(r)
            cb.wait_send()
            ck.wait_send()

        return c

    lax.fori_loop(1, n, drain_body, 0)

    def o_drain(k, c):
        slot = lax.div(k, n_tp)
        t = lax.rem(mt + lax.rem(k, n_tp), n_tp)

        @pl.when(jnp.logical_not(o_self(slot, t)))
        def _():
            o_copy(slot, t).wait_send()

        return c

    lax.fori_loop(0, 2 * n_tp, o_drain, 0)


def attention(query_vectors, key_vectors, value_vectors, cum_gate, tok_dev):
    n = lax.axis_size("sp")
    n_tp = lax.axis_size("tp")
    rows, width = query_vectors.shape
    half = width // 2
    coef = half ** (-0.5) * math.log2(math.e)
    q_swapped = jnp.concatenate([query_vectors[:, half:], query_vectors[:, :half]], axis=1)
    kv = jnp.stack(
        [
            jnp.concatenate([value_vectors[:, :half], key_vectors[:, :half]], axis=1),
            jnp.concatenate([key_vectors[:, half:], value_vectors[:, half:]], axis=1),
        ]
    )
    bias = (cum_gate * (-math.log2(math.e))).T[:, None, :]
    vmem = pl.BlockSpec(memory_space=pltpu.VMEM)
    tiles = n + 1
    return pl.pallas_call(
        functools.partial(attention_kernel, n, n_tp, tok_dev, coef),
        out_shape=jax.ShapeDtypeStruct((tok_dev, n_tp * width), jnp.bfloat16),
        in_specs=[vmem] * 3,
        out_specs=vmem,
        scratch_shapes=[
            pltpu.VMEM((2, rows, width), jnp.bfloat16),
            pltpu.VMEM((2, rows, width), jnp.bfloat16),
            pltpu.VMEM((n, rows, width), jnp.bfloat16),
            pltpu.VMEM((n, 1, rows), jnp.float32),
            pltpu.VMEM((2, rows, 1), jnp.float32),
            pltpu.VMEM((2, rows, 1), jnp.float32),
            pltpu.VMEM((2, rows, width), jnp.float32),
            pltpu.VMEM((2, rows, width), jnp.bfloat16),
            pltpu.VMEM((n_tp, 2, tok_dev, width), jnp.bfloat16),
            pltpu.SemaphoreType.DMA((n,)),
            pltpu.SemaphoreType.DMA((n,)),
            pltpu.SemaphoreType.DMA((n,)),
            pltpu.SemaphoreType.DMA((n,)),
            pltpu.SemaphoreType.DMA((2,)),
            pltpu.SemaphoreType.DMA((2,)),
            pltpu.SemaphoreType.DMA((2, n_tp)),
            pltpu.SemaphoreType.DMA,
        ],
        compiler_params=pltpu.CompilerParams(has_side_effects=True),
        cost_estimate=pl.CostEstimate(
            flops=tiles * rows * rows * width * 4 * 8,
            bytes_accessed=4 << 20,
            transcendentals=tiles * rows * rows,
        ),
        name="attention",
    )(q_swapped, kv, bias)

def experts_kernel(
    nz,
    x_ref,
    gate_hbm,
    up_hbm,
    down_hbm,
    out_ref,
    xbuf,
    gate,
    up,
    down,
    pown,
    psend,
    precv,
    rsend,
    rrecv,
    w_sem,
    x_sem,
    ag_send,
    ag_recv,
    d_send,
    d_recv,
    p_send,
    p_recv,
    r_send,
    r_recv,
):
    spi = lax.axis_index("sp")
    tpi = lax.axis_index("tp")
    z = lax.div(tpi, 2)
    core = lax.rem(tpi, 2)
    sign = 1 - 2 * core
    nxt = (spi, lax.rem(z + sign + nz, nz) * 2 + core)
    prv = (spi, lax.rem(z - sign + nz, nz) * 2 + core)
    partner = (spi, z * 2 + 1 - core)
    rows, model = x_ref.shape
    subs = 2
    half = rows // subs

    def mine(k):
        return lax.rem(z - sign * (1 + k) + 2 * nz, nz)

    def theirs(k):
        return lax.rem(z + sign * (1 + k) + 2 * nz, nz)

    def part(s):
        return pl.ds(s * half, half)

    loads = [
        pltpu.make_async_copy(a, b, w_sem.at[i])
        for i, (a, b) in enumerate(((gate_hbm, gate), (up_hbm, up), (down_hbm, down)))
    ]
    for load in loads:
        load.start()
    own = pltpu.make_async_copy(x_ref, xbuf.at[core, z], x_sem)
    own.start()

    barrier = pltpu.get_barrier_semaphore()
    for peer in (nxt, prv, partner):
        pl.semaphore_signal(barrier, inc=1, device_id=peer, device_id_type=MESH)
    pl.semaphore_wait(barrier, 3)
    own.wait()

    def ring(k, s):
        return pltpu.make_async_remote_copy(
            src_ref=xbuf.at[core, mine(k), part(s)],
            dst_ref=xbuf.at[core, mine(k), part(s)],
            send_sem=ag_send.at[k, s],
            recv_sem=ag_recv.at[lax.rem(k + 1, nz), s],
            device_id=nxt,
            device_id_type=MESH,
        )

    def share(k):
        return pltpu.make_async_remote_copy(
            src_ref=xbuf.at[core, mine(k)],
            dst_ref=xbuf.at[core, mine(k)],
            send_sem=d_send.at[k],
            recv_sem=d_recv.at[k],
            device_id=partner,
            device_id_type=MESH,
        )

    def give(k, s):
        return pltpu.make_async_remote_copy(
            src_ref=psend.at[k, part(s)],
            dst_ref=precv.at[k, part(s)],
            send_sem=p_send.at[k, s],
            recv_sem=p_recv.at[k, s],
            device_id=partner,
            device_id_type=MESH,
        )

    def reduce(k, s):
        return pltpu.make_async_remote_copy(
            src_ref=rsend.at[k, part(s)],
            dst_ref=rrecv.at[k, part(s)],
            send_sem=r_send.at[k, s],
            recv_sem=r_recv.at[k, s],
            device_id=nxt,
            device_id_type=MESH,
        )

    for s in range(subs):
        ring(nz - 1, s).start()
    share(nz - 1).start()
    for load in loads:
        load.wait()

    tile = min(512, model)

    def step(k, c):
        @pl.when(k < nz - 1)
        def _():
            for s in range(subs):
                pltpu.make_async_copy(
                    xbuf.at[core, 0, part(s)], xbuf.at[core, mine(k), part(s)], ag_recv.at[k, s]
                ).wait()

                @pl.when(k < nz - 2)
                def _():
                    ring(k, s).start()

            share(k).start()

        pltpu.make_async_copy(
            xbuf.at[1 - core, 0], xbuf.at[1 - core, theirs(k)], d_recv.at[k]
        ).wait()

        x = jnp.concatenate([xbuf[1 - core, theirs(k)], xbuf[core, mine(k)]], axis=0)
        g = jnp.dot(x, gate[...], preferred_element_type=jnp.float32)
        u = jnp.dot(x, up[...], preferred_element_type=jnp.float32)
        hidden = (g / (1.0 + jnp.exp(-g)) * u).astype(jnp.bfloat16)
        for n in range(model // tile):
            cols = slice(n * tile, (n + 1) * tile)
            p = jnp.dot(hidden, down[:, cols], preferred_element_type=jnp.float32)
            psend[k, :, cols] = p[:rows].astype(jnp.bfloat16)
            pown[:, cols] = p[rows:]
        for s in range(subs):
            give(k, s).start()
        for s in range(subs):
            give(k, s).wait_recv()
            total = pown[part(s), :] + precv[k, part(s), :].astype(jnp.float32)

            @pl.when(k > 0)
            def _():
                kk = jnp.maximum(k - 1, 0)
                reduce(kk, s).wait_recv()
                pown[part(s), :] = total + rrecv[kk, part(s), :].astype(jnp.float32)

            @pl.when(k == 0)
            def _():
                pown[part(s), :] = total

            @pl.when(k < nz - 1)
            def _():
                rsend[k, part(s), :] = pown[part(s), :].astype(jnp.bfloat16)
                reduce(k, s).start()

        return c

    lax.fori_loop(0, nz, step, 0)
    out_ref[...] = pown[...].astype(jnp.bfloat16)

    def drain(k, c):
        for s in range(subs):
            give(k, s).wait_send()

            @pl.when(k != nz - 2)
            def _():
                ring(k, s).wait_send()

            @pl.when(k < nz - 1)
            def _():
                reduce(k, s).wait_send()

        share(k).wait_send()
        return c

    lax.fori_loop(0, nz, drain, 0)


def experts(x, gate_weight, up_weight, down_weight):
    nz = lax.axis_size("tp") // 2
    rows, model = x.shape
    inner = gate_weight.shape[1]
    vmem = pl.BlockSpec(memory_space=pltpu.VMEM)
    hbm = pl.BlockSpec(memory_space=pl.ANY)
    bf16 = jnp.bfloat16
    dma = pltpu.SemaphoreType.DMA
    return pl.pallas_call(
        functools.partial(experts_kernel, nz),
        out_shape=jax.ShapeDtypeStruct((rows, model), bf16),
        in_specs=[vmem, hbm, hbm, hbm],
        out_specs=vmem,
        scratch_shapes=[
            pltpu.VMEM((2, nz, rows, model), bf16),
            pltpu.VMEM((model, inner), bf16),
            pltpu.VMEM((model, inner), bf16),
            pltpu.VMEM((inner, model), bf16),
            pltpu.VMEM((rows, model), jnp.float32),
            pltpu.VMEM((nz, rows, model), bf16),
            pltpu.VMEM((nz, rows, model), bf16),
            pltpu.VMEM((nz - 1, rows, model), bf16),
            pltpu.VMEM((nz - 1, rows, model), bf16),
            dma((3,)),
            dma,
            dma((nz, 2)),
            dma((nz, 2)),
            dma((nz,)),
            dma((nz,)),
            dma((nz, 2)),
            dma((nz, 2)),
            dma((nz - 1, 2)),
            dma((nz - 1, 2)),
        ],
        compiler_params=pltpu.CompilerParams(
            collective_id=1, has_side_effects=True, vmem_limit_bytes=60 << 20
        ),
        cost_estimate=pl.CostEstimate(
            flops=2 * nz * rows * 2 * model * inner * 3, bytes_accessed=8 << 20, transcendentals=0
        ),
        name="experts",
    )(x, gate_weight, up_weight, down_weight)


def shards(
    tokens,
    query_vectors,
    key_vectors,
    value_vectors,
    cum_gate,
    out_weight,
    norm_gain,
    gate_weight,
    up_weight,
    down_weight,
    expert_ids,
    route_weights,
):
    sp_count = lax.axis_size("sp")
    tok_dev = tokens.shape[0]
    model_width = tokens.shape[1]
    token_rows = attention(query_vectors, key_vectors, value_vectors, cum_gate, tok_dev)
    projected = jnp.dot(
        token_rows,
        lax.all_gather(out_weight, "tp", axis=0, tiled=True),
        preferred_element_type=jnp.float32,
    )
    stream_wide = (tokens.astype(jnp.float32) + projected).astype(jnp.bfloat16).astype(jnp.float32)
    inverse = lax.rsqrt(jnp.mean(stream_wide * stream_wide, axis=1, keepdims=True) + 1e-05)
    normed = (stream_wide * inverse * norm_gain[None, :]).astype(jnp.bfloat16)
    n_experts = gate_weight.shape[0] * sp_count
    top_count = expert_ids.shape[1]
    capacity = max(2, 3 * tok_dev * top_count // (2 * n_experts))
    flat_ids = expert_ids.reshape(-1)
    hits = (flat_ids[:, None] == jnp.arange(n_experts, dtype=jnp.int32)[None, :]).astype(jnp.int32)
    earlier = jnp.cumsum(hits, axis=0) - hits
    slot_index = flat_ids * capacity + jnp.sum(earlier * hits, axis=1)
    placement_map = (
        jnp.arange(n_experts * capacity, dtype=jnp.int32)[:, None] == slot_index[None, :]
    ).astype(jnp.bfloat16)
    repeated = jnp.repeat(normed, top_count, axis=0)
    dispatch = jnp.dot(placement_map, repeated, preferred_element_type=jnp.float32).astype(
        jnp.bfloat16
    )
    dispatch = dispatch.reshape(n_experts, capacity, model_width)
    arrived = lax.all_to_all(dispatch, "sp", split_axis=0, concat_axis=0, tiled=True)
    row_block = arrived.reshape(-1, model_width)
    summed = experts(row_block, gate_weight[0], up_weight[0], down_weight[0])
    returned = summed.reshape(arrived.shape)
    back = lax.all_to_all(returned, "sp", split_axis=0, concat_axis=0, tiled=True)
    flat_back = back.reshape(n_experts * capacity, model_width)
    picked = flat_back[slot_index].astype(jnp.float32).reshape(tok_dev, top_count, model_width)
    mixture = jnp.sum(picked * route_weights[:, :, None], axis=1)
    return (stream_wide + mixture).astype(jnp.bfloat16)


def solution(mesh):
    in_specs = (
        P(("sp", "tp"), None),
        P("sp", "tp"),
        P("sp", "tp"),
        P("sp", "tp"),
        P("sp", "tp"),
        P("tp", None),
        P(),
        P("sp", None, "tp"),
        P("sp", None, "tp"),
        P("sp", "tp", None),
        P(("sp", "tp"), None),
        P(("sp", "tp"), None),
    )
    out_specs = P(("sp", "tp"), None)
    return jax.shard_map(shards, mesh=mesh, in_specs=in_specs, out_specs=out_specs, check_vma=False)
```

```python
import functools
import math

import jax
import jax.numpy as jnp
from jax import lax
from jax.experimental import pallas as pl
from jax.experimental.pallas import tpu as pltpu
from jax.sharding import PartitionSpec as P

NEG_LARGE = -1e30
MESH = pl.DeviceIdType.MESH
SLOTS = 8


def attention_kernel(
    n,
    n_tp,
    coef,
    q_ref,
    k_ref,
    v_ref,
    gate_ref,
    w_ref,
    tok_ref,
    gain_ref,
    stream_ref,
    normed_ref,
    qraw,
    qbuf,
    kvsend,
    bsend,
    kvbuf,
    bbuf,
    peak,
    total,
    acc,
    obuf,
    rbuf,
    wbuf,
    proj,
    kv_send,
    kv_recv,
    b_send,
    b_recv,
    q_send,
    q_recv,
    o_send,
    o_recv,
    w_send,
    w_recv,
    d_send,
    d_recv,
    own_sem,
):
    me = lax.axis_index("sp")
    mt = lax.axis_index("tp")
    nz = n_tp // 2
    z = lax.div(mt, 2)
    core = lax.rem(mt, 2)
    sign = 1 - 2 * core
    nxt = (me, lax.rem(z + sign + nz, nz) * 2 + core)
    partner = (me, z * 2 + 1 - core)
    mirror = n - 1 - me
    head = lax.div(me, n // 2)
    pair = jnp.minimum(me, mirror)
    last = jnp.maximum(me, mirror)
    own_slot = head
    rows, width = q_ref.shape
    half = width // 2
    tok_dev, model = tok_ref.shape

    barrier = pltpu.get_barrier_semaphore()

    def greet_plane(k, c):
        pl.semaphore_signal(
            barrier, inc=1, device_id=(lax.rem(me + k, n), mt), device_id_type=MESH
        )
        return c

    def greet_heads(k, c):
        t = lax.rem(mt + k, n_tp)
        pl.semaphore_signal(barrier, inc=1, device_id=(me, t), device_id_type=MESH)
        pl.semaphore_signal(barrier, inc=1, device_id=(mirror, t), device_id_type=MESH)
        return c

    lax.fori_loop(1, n, greet_plane, 0)
    lax.fori_loop(1, n_tp, greet_heads, 0)

    own_w = pltpu.make_async_copy(w_ref, wbuf.at[mt], own_sem.at[0])
    own_w.start()
    lane = lax.broadcasted_iota(jnp.int32, (rows, width), 1)
    low = lane < half
    rolled_k = pltpu.roll(k_ref[...].astype(jnp.float32), half, 1)
    values = v_ref[...].astype(jnp.float32)
    kvsend[0] = jnp.where(low, values, rolled_k).astype(jnp.bfloat16)
    kvsend[1] = jnp.where(low, rolled_k, values).astype(jnp.bfloat16)
    bias_rows = gate_ref[...] * (-math.log2(math.e))
    bsend[0] = bias_rows[0:1]
    bsend[1] = bias_rows[1:2]
    mine = low == (head == 1)

    def prepare(raw):
        rolled = pltpu.roll(raw.astype(jnp.float32), half, 1)
        return jnp.where(mine, rolled, 0.0).astype(jnp.bfloat16)

    qbuf[own_slot] = prepare(q_ref[...])
    peak[...] = jnp.full(peak.shape, NEG_LARGE, jnp.float32)
    total[...] = jnp.zeros(total.shape, jnp.float32)
    acc[...] = jnp.zeros(acc.shape, jnp.float32)

    pl.semaphore_wait(barrier, (n - 1) + 2 * (n_tp - 1))

    q_copy = pltpu.make_async_remote_copy(
        src_ref=q_ref,
        dst_ref=qraw,
        send_sem=q_send,
        recv_sem=q_recv,
        device_id=(mirror, mt),
        device_id_type=MESH,
    )
    q_copy.start()

    w_half = w_ref.shape[0] // 2

    def w_mine(k):
        return lax.rem(z - sign * (1 + k) + 2 * nz, nz) * 2 + core

    def w_theirs(k):
        return lax.rem(z + sign * (1 + k) + 2 * nz, nz) * 2 + 1 - core

    def w_ring(k, s, src):
        return pltpu.make_async_remote_copy(
            src_ref=src.at[pl.ds(s * w_half, w_half)],
            dst_ref=wbuf.at[w_mine(k), pl.ds(s * w_half, w_half)],
            send_sem=w_send.at[k, s],
            recv_sem=w_recv.at[lax.rem(k + 1, nz), s],
            device_id=nxt,
            device_id_type=MESH,
        )

    def w_share(k, s, src):
        return pltpu.make_async_remote_copy(
            src_ref=src.at[pl.ds(s * w_half, w_half)],
            dst_ref=wbuf.at[w_mine(k), pl.ds(s * w_half, w_half)],
            send_sem=d_send.at[k, s],
            recv_sem=d_recv.at[k, s],
            device_id=partner,
            device_id_type=MESH,
        )

    for s in range(2):
        w_ring(nz - 1, s, w_ref).start()

    def kv_copy(r):
        hr = lax.div(r, n // 2)
        return (
            pltpu.make_async_remote_copy(
                src_ref=kvsend.at[hr],
                dst_ref=kvbuf.at[me],
                send_sem=kv_send.at[r],
                recv_sem=kv_recv.at[me],
                device_id=(r, mt),
                device_id_type=MESH,
            ),
            pltpu.make_async_remote_copy(
                src_ref=bsend.at[hr],
                dst_ref=bbuf.at[me],
                send_sem=b_send.at[r],
                recv_sem=b_recv.at[me],
                device_id=(r, mt),
                device_id_type=MESH,
            ),
        )

    def send_body(k, c):
        r = lax.rem(me + k, n)

        @pl.when(me <= jnp.maximum(r, n - 1 - r))
        def _():
            ck, cb = kv_copy(r)
            cb.start()
            ck.start()

        return c

    lax.fori_loop(1, n, send_body, 0)
    for s in range(2):
        w_share(nz - 1, s, w_ref).start()

    sub = min(256, rows)

    def tile(slot, kv_at, bias_at, diagonal):
        for i in range(rows // sub):
            kv = kv_at[...]
            rs = pl.ds(i * sub, sub)
            s = lax.dot_general(
                qbuf[slot, rs, :], kv, (((1,), (1,)), ((), ())), preferred_element_type=jnp.float32
            )
            s = s * coef + bias_at[...]
            if diagonal:
                qp = lax.broadcasted_iota(jnp.int32, s.shape, 0) + i * sub
                kp = lax.broadcasted_iota(jnp.int32, s.shape, 1)
                s = jnp.where(kp <= qp, s, NEG_LARGE)
            old = peak[slot, rs, :]
            new = jnp.maximum(old, jnp.max(s, axis=1, keepdims=True))
            e = jnp.exp2(s - new)
            alpha = jnp.exp2(old - new)
            total[slot, rs, :] = total[slot, rs, :] * alpha + jnp.sum(e, axis=1, keepdims=True)
            acc[slot, rs, :] = acc[slot, rs, :] * alpha + jnp.dot(
                e.astype(jnp.bfloat16), kv, preferred_element_type=jnp.float32
            )
            peak[slot, rs, :] = new

    tile(own_slot, kvsend.at[head], bsend.at[head], True)
    pltpu.make_async_copy(q_ref, qraw, q_recv).wait()
    qbuf[1 - own_slot] = prepare(qraw[...])

    @pl.when(me < last)
    def _():
        tile(1, kvsend.at[head], bsend.at[head], False)

    def w_event(i):
        k = lax.div(i, 2)
        s = lax.rem(i, 2)
        block = wbuf.at[w_mine(k)]
        pltpu.make_async_copy(
            w_ref.at[pl.ds(0, w_half)], block.at[pl.ds(s * w_half, w_half)], w_recv.at[k, s]
        ).wait()

        @pl.when(k < nz - 2)
        def _():
            w_ring(k, s, block).start()

        w_share(k, s, block).start()

    events = 2 * (nz - 1)
    early = min(nz - 1, (n - 1) // 2)

    def compute_body(k, c):
        j = lax.rem(me - k + n, n)

        @pl.when(jnp.logical_and(lax.rem(k, 2) == 0, lax.div(k, 2) <= early))
        def _():
            w_event(lax.div(k, 2) - 1)

        @pl.when(j <= last)
        def _():
            pltpu.make_async_copy(kvsend.at[0], kvbuf.at[j], kv_recv.at[j]).wait()
            pltpu.make_async_copy(bsend.at[0], bbuf.at[j], b_recv.at[j]).wait()

            def slot_body(slot, c):
                end = jnp.where(slot == 0, pair, last)

                @pl.when(j == end)
                def _():
                    tile(slot, kvbuf.at[j], bbuf.at[j], True)

                @pl.when(j < end)
                def _():
                    tile(slot, kvbuf.at[j], bbuf.at[j], False)

                return c

            lax.fori_loop(0, 2, slot_body, 0)

        return c

    lax.fori_loop(1, n, compute_body, 0)

    for slot in range(2):
        obuf[slot] = (acc[slot] / total[slot]).astype(jnp.bfloat16)

    def o_target(slot):
        return jnp.where(slot == 0, pair, last)

    def o_copy(slot, t):
        return pltpu.make_async_remote_copy(
            src_ref=obuf.at[slot, pl.ds(t * tok_dev, tok_dev)],
            dst_ref=rbuf.at[mt, head],
            send_sem=o_send.at[slot, t],
            recv_sem=o_recv,
            device_id=(o_target(slot), t),
            device_id_type=MESH,
        )

    def o_self(slot, t):
        return jnp.logical_and(o_target(slot) == me, t == mt)

    def o_body(k, c):
        slot = lax.rem(k, 2)
        t = lax.rem(mt + n_tp // 2 + lax.div(k, 2), n_tp)

        @pl.when(jnp.logical_not(o_self(slot, t)))
        def _():
            o_copy(slot, t).start()

        @pl.when(o_self(slot, t))
        def _():
            pltpu.make_async_copy(
                obuf.at[slot, pl.ds(t * tok_dev, tok_dev)], rbuf.at[mt, head], o_recv
            ).start()

        return c

    lax.fori_loop(0, 2 * n_tp, o_body, 0)

    def late_event(i, c):
        w_event(i)
        return c

    steps_before = min(5, nz - 1)
    lax.fori_loop(early, 2 * steps_before, late_event, 0)

    pltpu.make_async_copy(rbuf, rbuf, o_recv).wait()
    own_w.wait()
    for s in range(2):
        pltpu.make_async_copy(
            w_ref.at[pl.ds(0, w_half)], wbuf.at[mt, pl.ds(s * w_half, w_half)], d_recv.at[nz - 1, s]
        ).wait()
    low32 = lax.broadcasted_iota(jnp.int32, (tok_dev, width), 1) < half

    def product(t):
        piece = jnp.where(
            low32, rbuf[t, 0].astype(jnp.float32), rbuf[t, 1].astype(jnp.float32)
        ).astype(jnp.bfloat16)
        return jnp.dot(piece, wbuf[t], preferred_element_type=jnp.float32)

    proj[...] = product(mt)
    proj[...] += product(z * 2 + 1 - core)

    def project(k, c):
        @pl.when(k >= steps_before)
        def _():
            for s in range(2):
                w_event(2 * k + s)

        for s in range(2):
            pltpu.make_async_copy(
                w_ref.at[pl.ds(0, w_half)],
                wbuf.at[w_theirs(k), pl.ds(s * w_half, w_half)],
                d_recv.at[k, s],
            ).wait()
        proj[...] += product(w_mine(k))
        proj[...] += product(w_theirs(k))
        return c

    lax.fori_loop(0, nz - 1, project, 0)
    stream = (tok_ref[...].astype(jnp.float32) + proj[...]).astype(jnp.bfloat16)
    stream_ref[...] = stream
    wide = stream.astype(jnp.float32)
    inverse = lax.rsqrt(jnp.mean(wide * wide, axis=1, keepdims=True) + 1e-05)
    normed_ref[...] = (wide * inverse * gain_ref[...]).astype(jnp.bfloat16)

    q_copy.wait_send()

    def drain_body(k, c):
        r = lax.rem(me + k, n)

        @pl.when(me <= jnp.maximum(r, n - 1 - r))
        def _():
            ck, cb = kv_copy(r)
            cb.wait_send()
            ck.wait_send()

        return c

    lax.fori_loop(1, n, drain_body, 0)

    def o_drain(k, c):
        slot = lax.rem(k, 2)
        t = lax.div(k, 2)

        @pl.when(jnp.logical_not(o_self(slot, t)))
        def _():
            o_copy(slot, t).wait_send()

        return c

    lax.fori_loop(0, 2 * n_tp, o_drain, 0)

    def w_drain(k, c):
        for s in range(2):
            w_share(k, s, w_ref).wait_send()

            @pl.when(k != nz - 2)
            def _():
                w_ring(k, s, w_ref).wait_send()

        return c

    lax.fori_loop(0, nz, w_drain, 0)


def attention(query_vectors, key_vectors, value_vectors, cum_gate, out_weight, tokens, norm_gain):
    n = lax.axis_size("sp")
    n_tp = lax.axis_size("tp")
    nz = n_tp // 2
    rows, width = query_vectors.shape
    tok_dev, model = tokens.shape
    coef = (width // 2) ** (-0.5) * math.log2(math.e)
    vmem = pl.BlockSpec(memory_space=pltpu.VMEM)
    bf16, f32 = jnp.bfloat16, jnp.float32
    dma = pltpu.SemaphoreType.DMA
    result = jax.ShapeDtypeStruct((tok_dev, model), bf16)
    return pl.pallas_call(
        functools.partial(attention_kernel, n, n_tp, coef),
        out_shape=(result, result),
        in_specs=[vmem] * 7,
        out_specs=(vmem, vmem),
        scratch_shapes=[
            pltpu.VMEM((rows, width), bf16),
            pltpu.VMEM((2, rows, width), bf16),
            pltpu.VMEM((2, rows, width), bf16),
            pltpu.VMEM((2, 1, rows), f32),
            pltpu.VMEM((n, rows, width), bf16),
            pltpu.VMEM((n, 1, rows), f32),
            pltpu.VMEM((2, rows, 1), f32),
            pltpu.VMEM((2, rows, 1), f32),
            pltpu.VMEM((2, rows, width), f32),
            pltpu.VMEM((2, rows, width), bf16),
            pltpu.VMEM((n_tp, 2, tok_dev, width), bf16),
            pltpu.VMEM((n_tp, width, model), bf16),
            pltpu.VMEM((tok_dev, model), f32),
            dma((n,)),
            dma((n,)),
            dma((n,)),
            dma((n,)),
            dma,
            dma,
            dma((2, n_tp)),
            dma,
            dma((nz, 2)),
            dma((nz, 2)),
            dma((nz, 2)),
            dma((nz, 2)),
            dma((1,)),
        ],
        compiler_params=pltpu.CompilerParams(
            collective_id=0, has_side_effects=True, vmem_limit_bytes=48 << 20
        ),
        name="attention",
    )(
        query_vectors,
        key_vectors,
        value_vectors,
        cum_gate.T,
        out_weight,
        tokens,
        norm_gain[None, :],
    )


def experts_kernel(
    nz,
    n,
    capacity,
    normed_ref,
    stream_ref,
    place_ref,
    pick_ref,
    route_ref,
    gate_hbm,
    up_hbm,
    down_hbm,
    out_ref,
    packed,
    arrived,
    xbuf,
    gate,
    up,
    down,
    pown,
    psend,
    precv,
    rsend,
    rrecv,
    spread,
    back,
    w_sem,
    a_send,
    a_recv,
    b_send,
    b_recv,
    ag_send,
    ag_recv,
    d_send,
    d_recv,
    p_send,
    p_recv,
    r_send,
    r_recv,
):
    spi = lax.axis_index("sp")
    tpi = lax.axis_index("tp")
    z = lax.div(tpi, 2)
    core = lax.rem(tpi, 2)
    sign = 1 - 2 * core
    nxt = (spi, lax.rem(z + sign + nz, nz) * 2 + core)
    prv = (spi, lax.rem(z - sign + nz, nz) * 2 + core)
    partner = (spi, z * 2 + 1 - core)
    model = normed_ref.shape[1]
    rows = n * capacity
    padded = n * SLOTS
    subs = 2
    half = rows // subs
    bf16, f32 = jnp.bfloat16, jnp.float32

    loads = [
        pltpu.make_async_copy(a, b, w_sem.at[i])
        for i, (a, b) in enumerate(((gate_hbm, gate), (up_hbm, up), (down_hbm, down)))
    ]
    for load in loads:
        load.start()

    barrier = pltpu.get_barrier_semaphore()

    def greet(k, c):
        pl.semaphore_signal(
            barrier, inc=1, device_id=(lax.rem(spi + k, n), tpi), device_id_type=MESH
        )
        return c

    lax.fori_loop(1, n, greet, 0)
    for peer in (nxt, prv, partner):
        pl.semaphore_signal(barrier, inc=1, device_id=peer, device_id_type=MESH)

    block = jnp.dot(place_ref[...], normed_ref[...], preferred_element_type=f32).astype(bf16)
    for e in range(n):
        packed[e] = block[e * SLOTS : (e + 1) * SLOTS]
    pl.semaphore_wait(barrier, n - 1 + 3)

    def to_expert(e):
        return pltpu.make_async_remote_copy(
            src_ref=packed.at[e],
            dst_ref=arrived.at[spi],
            send_sem=a_send.at[e],
            recv_sem=a_recv,
            device_id=(e, tpi),
            device_id_type=MESH,
        )

    def to_token(s):
        return pltpu.make_async_remote_copy(
            src_ref=spread.at[s],
            dst_ref=back.at[spi],
            send_sem=b_send.at[s],
            recv_sem=b_recv,
            device_id=(s, tpi),
            device_id_type=MESH,
        )

    def dispatch_body(k, c):
        to_expert(lax.rem(spi + k, n)).start()
        return c

    pltpu.make_async_copy(packed.at[spi], arrived.at[spi], a_recv).start()
    lax.fori_loop(1, n, dispatch_body, 0)

    def mine(k):
        return lax.rem(z - sign * (1 + k) + 2 * nz, nz)

    def theirs(k):
        return lax.rem(z + sign * (1 + k) + 2 * nz, nz)

    def part(s):
        return pl.ds(s * half, half)

    def ring(k, s):
        return pltpu.make_async_remote_copy(
            src_ref=xbuf.at[core, mine(k), part(s)],
            dst_ref=xbuf.at[core, mine(k), part(s)],
            send_sem=ag_send.at[k, s],
            recv_sem=ag_recv.at[lax.rem(k + 1, nz), s],
            device_id=nxt,
            device_id_type=MESH,
        )

    def share(k):
        return pltpu.make_async_remote_copy(
            src_ref=xbuf.at[core, mine(k)],
            dst_ref=xbuf.at[core, mine(k)],
            send_sem=d_send.at[k],
            recv_sem=d_recv.at[k],
            device_id=partner,
            device_id_type=MESH,
        )

    def give(k, s):
        return pltpu.make_async_remote_copy(
            src_ref=psend.at[k, part(s)],
            dst_ref=precv.at[k, part(s)],
            send_sem=p_send.at[k, s],
            recv_sem=p_recv.at[k, s],
            device_id=partner,
            device_id_type=MESH,
        )

    def reduce(k, s):
        return pltpu.make_async_remote_copy(
            src_ref=rsend.at[k, part(s)],
            dst_ref=rrecv.at[k, part(s)],
            send_sem=r_send.at[k, s],
            recv_sem=r_recv.at[k, s],
            device_id=nxt,
            device_id_type=MESH,
        )

    compact = lax.broadcasted_iota(jnp.int32, (rows, padded), 0)
    wide = lax.broadcasted_iota(jnp.int32, (rows, padded), 1)
    keep = (lax.div(compact, capacity) * SLOTS + lax.rem(compact, capacity) == wide).astype(bf16)
    pltpu.make_async_copy(arrived, arrived, a_recv).wait()
    xbuf[core, z] = jnp.dot(
        keep, arrived[...].reshape(padded, model), preferred_element_type=f32
    ).astype(bf16)
    for s in range(subs):
        ring(nz - 1, s).start()
    share(nz - 1).start()
    for load in loads:
        load.wait()

    tile = min(512, model)
    across = (((1,), (1,)), ((), ()))

    def step(k, c):
        @pl.when(k < nz - 1)
        def _():
            for s in range(subs):
                pltpu.make_async_copy(
                    xbuf.at[core, 0, part(s)], xbuf.at[core, mine(k), part(s)], ag_recv.at[k, s]
                ).wait()

                @pl.when(k < nz - 2)
                def _():
                    ring(k, s).start()

            share(k).start()

        pltpu.make_async_copy(
            xbuf.at[1 - core, 0], xbuf.at[1 - core, theirs(k)], d_recv.at[k]
        ).wait()

        x = jnp.concatenate([xbuf[1 - core, theirs(k)], xbuf[core, mine(k)]], axis=0)
        g = lax.dot_general(x, gate[...], across, preferred_element_type=f32)
        u = lax.dot_general(x, up[...], across, preferred_element_type=f32)
        hidden = (g / (1.0 + jnp.exp(-g)) * u).astype(bf16)
        for i in range(model // tile):
            cols = slice(i * tile, (i + 1) * tile)
            p = jnp.dot(hidden, down[:, cols], preferred_element_type=f32)
            psend[k, :, cols] = p[:rows].astype(bf16)
            pown[:, cols] = p[rows:]
        for s in range(subs):
            give(k, s).start()
        for s in range(subs):
            give(k, s).wait_recv()
            total = pown[part(s), :] + precv[k, part(s), :].astype(f32)

            @pl.when(k > 0)
            def _():
                kk = jnp.maximum(k - 1, 0)
                reduce(kk, s).wait_recv()
                pown[part(s), :] = total + rrecv[kk, part(s), :].astype(f32)

            @pl.when(k == 0)
            def _():
                pown[part(s), :] = total

            @pl.when(k < nz - 1)
            def _():
                rsend[k, part(s), :] = pown[part(s), :].astype(bf16)
                reduce(k, s).start()

        return c

    lax.fori_loop(0, nz, step, 0)

    finished = pown[...].astype(bf16)
    scattered = lax.dot_general(
        keep, finished, (((0,), (0,)), ((), ())), preferred_element_type=f32
    ).astype(bf16)
    for s in range(n):
        spread[s] = scattered[s * SLOTS : (s + 1) * SLOTS]
    pltpu.make_async_copy(spread.at[spi], back.at[spi], b_recv).start()

    def return_body(k, c):
        to_token(lax.rem(spi + k, n)).start()
        return c

    lax.fori_loop(1, n, return_body, 0)

    def drain(k, c):
        for s in range(subs):
            give(k, s).wait_send()

            @pl.when(k != nz - 2)
            def _():
                ring(k, s).wait_send()

            @pl.when(k < nz - 1)
            def _():
                reduce(k, s).wait_send()

        share(k).wait_send()
        return c

    lax.fori_loop(0, nz, drain, 0)

    def drain_plane(k, c):
        to_expert(lax.rem(spi + k, n)).wait_send()
        return c

    lax.fori_loop(1, n, drain_plane, 0)

    pltpu.make_async_copy(back, back, b_recv).wait()
    rows_back = back[...].reshape(padded, model)
    mixture = jnp.zeros(stream_ref.shape, f32)
    for r in range(pick_ref.shape[0]):
        picked = jnp.dot(pick_ref[r], rows_back, preferred_element_type=f32)
        mixture = mixture + picked * route_ref[:, r : r + 1]
    out_ref[...] = (stream_ref[...].astype(f32) + mixture).astype(bf16)

    def drain_back(k, c):
        to_token(lax.rem(spi + k, n)).wait_send()
        return c

    lax.fori_loop(1, n, drain_back, 0)


def experts(normed, stream, expert_ids, route_weights, gate_weight, up_weight, down_weight):
    nz = lax.axis_size("tp") // 2
    n = lax.axis_size("sp")
    tok_dev, model = normed.shape
    top = expert_ids.shape[1]
    capacity = max(2, 3 * tok_dev * top // (2 * n))
    rows = n * capacity
    padded = n * SLOTS
    inner = gate_weight.shape[2]
    bf16 = jnp.bfloat16
    flat_ids = expert_ids.reshape(-1)
    order = jnp.arange(tok_dev * top, dtype=jnp.int32)
    same = flat_ids[:, None] == flat_ids[None, :]
    rank = jnp.sum((same & (order[None, :] < order[:, None])).astype(jnp.int32), axis=1)
    slot = (flat_ids * SLOTS + rank).reshape(tok_dev, top)
    numbers = jnp.arange(padded, dtype=jnp.int32)
    place = jnp.any(numbers[:, None, None] == slot[None], axis=2).astype(bf16)
    pick = (slot.T[:, :, None] == numbers[None, None, :]).astype(bf16)
    vmem = pl.BlockSpec(memory_space=pltpu.VMEM)
    hbm = pl.BlockSpec(memory_space=pl.ANY)
    dma = pltpu.SemaphoreType.DMA
    return pl.pallas_call(
        functools.partial(experts_kernel, nz, n, capacity),
        out_shape=jax.ShapeDtypeStruct((tok_dev, model), bf16),
        in_specs=[vmem] * 5 + [hbm] * 3,
        out_specs=vmem,
        scratch_shapes=[
            pltpu.VMEM((n, SLOTS, model), bf16),
            pltpu.VMEM((n, SLOTS, model), bf16),
            pltpu.VMEM((2, nz, rows, model), bf16),
            pltpu.VMEM((inner, model), bf16),
            pltpu.VMEM((inner, model), bf16),
            pltpu.VMEM((inner, model), bf16),
            pltpu.VMEM((rows, model), jnp.float32),
            pltpu.VMEM((nz, rows, model), bf16),
            pltpu.VMEM((nz, rows, model), bf16),
            pltpu.VMEM((nz - 1, rows, model), bf16),
            pltpu.VMEM((nz - 1, rows, model), bf16),
            pltpu.VMEM((n, SLOTS, model), bf16),
            pltpu.VMEM((n, SLOTS, model), bf16),
            dma((3,)),
            dma((n,)),
            dma,
            dma((n,)),
            dma,
            dma((nz, 2)),
            dma((nz, 2)),
            dma((nz,)),
            dma((nz,)),
            dma((nz, 2)),
            dma((nz, 2)),
            dma((nz - 1, 2)),
            dma((nz - 1, 2)),
        ],
        compiler_params=pltpu.CompilerParams(
            collective_id=1, has_side_effects=True, vmem_limit_bytes=60 << 20
        ),
        name="experts",
    )(
        normed,
        stream,
        place,
        pick,
        route_weights,
        jnp.swapaxes(gate_weight[0], 0, 1),
        jnp.swapaxes(up_weight[0], 0, 1),
        down_weight[0],
    )


def shards(
    tokens,
    query_vectors,
    key_vectors,
    value_vectors,
    cum_gate,
    out_weight,
    norm_gain,
    gate_weight,
    up_weight,
    down_weight,
    expert_ids,
    route_weights,
):
    stream, normed = attention(
        query_vectors, key_vectors, value_vectors, cum_gate, out_weight, tokens, norm_gain
    )
    return experts(
        normed, stream, expert_ids, route_weights, gate_weight, up_weight, down_weight
    )


def solution(mesh):
    in_specs = (
        P(("sp", "tp"), None),
        P("sp", "tp"),
        P("sp", "tp"),
        P("sp", "tp"),
        P("sp", "tp"),
        P("tp", None),
        P(),
        P("sp", None, "tp"),
        P("sp", None, "tp"),
        P("sp", "tp", None),
        P(("sp", "tp"), None),
        P(("sp", "tp"), None),
    )
    out_specs = P(("sp", "tp"), None)
    return jax.shard_map(shards, mesh=mesh, in_specs=in_specs, out_specs=out_specs, check_vma=False)
```

```python
import functools
import math

import jax
import jax.numpy as jnp
from jax import lax
from jax.experimental import pallas as pl
from jax.experimental.pallas import tpu as pltpu
from jax.sharding import PartitionSpec as P

NEG_LARGE = -1e30
MESH = pl.DeviceIdType.MESH
SLOTS = 8


def layer_kernel(
    n,
    n_tp,
    coef,
    capacity,
    q_hbm,
    k_hbm,
    v_hbm,
    gate_ref,
    w_hbm,
    tok_hbm,
    gain_ref,
    ids_ref,
    route_ref,
    wg_hbm,
    wu_hbm,
    wd_hbm,
    out_ref,
    q_ref,
    k_ref,
    v_ref,
    w_ref,
    tok_ref,
    gate,
    up,
    down,
    qraw,
    qbuf,
    kvsend,
    bsend,
    kvbuf,
    bbuf,
    peak,
    total,
    acc,
    obuf,
    rbuf,
    wbuf,
    proj,
    stream_ref,
    place,
    keep,
    ext,
    packed,
    arrived,
    xbuf,
    pown,
    psend,
    precv,
    rsend,
    rrecv,
    spread,
    back,
    in_sem,
    kv_send,
    kv_recv,
    b_send,
    b_recv,
    q_send,
    q_recv,
    o_send,
    o_recv,
    w_send,
    w_recv,
    d_send,
    d_recv,
    own_sem,
    x_send,
    x_recv,
    a_send,
    a_recv,
    s_send,
    s_recv,
    p_send,
    p_recv,
    r_send,
    r_recv,
    t_send,
    t_recv,
):
    me = lax.axis_index("sp")
    mt = lax.axis_index("tp")
    nz = n_tp // 2
    z = lax.div(mt, 2)
    core = lax.rem(mt, 2)
    sign = 1 - 2 * core
    nxt = (me, lax.rem(z + sign + nz, nz) * 2 + core)
    partner = (me, z * 2 + 1 - core)
    mirror = n - 1 - me
    head = lax.div(me, n // 2)
    pair = jnp.minimum(me, mirror)
    last = jnp.maximum(me, mirror)
    own_slot = head
    rows, width = q_ref.shape
    half = width // 2
    tok_dev, model = tok_ref.shape
    bf16, f32 = jnp.bfloat16, jnp.float32
    expert_rows = n * capacity
    padded = n * SLOTS

    loads = [
        pltpu.make_async_copy(a, b, in_sem.at[i])
        for i, (a, b) in enumerate(
            (
                (k_hbm, k_ref),
                (v_hbm, v_ref),
                (q_hbm, q_ref),
                (w_hbm, w_ref),
                (tok_hbm, tok_ref),
                (wg_hbm, gate),
                (wu_hbm, up),
                (wd_hbm, down),
            )
        )
    ]
    for load in loads:
        load.start()

    barrier = pltpu.get_barrier_semaphore()

    def greet_plane(k, c):
        pl.semaphore_signal(
            barrier, inc=1, device_id=(lax.rem(me + k, n), mt), device_id_type=MESH
        )
        return c

    def greet_heads(k, c):
        t = lax.rem(mt + k, n_tp)
        pl.semaphore_signal(barrier, inc=1, device_id=(me, t), device_id_type=MESH)
        pl.semaphore_signal(barrier, inc=1, device_id=(mirror, t), device_id_type=MESH)
        return c

    lax.fori_loop(1, n, greet_plane, 0)
    lax.fori_loop(1, n_tp, greet_heads, 0)

    own_w = pltpu.make_async_copy(w_hbm, wbuf.at[mt], own_sem.at[0])
    own_w.start()
    for load in loads[:5]:
        load.wait()
    lane = lax.broadcasted_iota(jnp.int32, (rows, width), 1)
    low = lane < half
    rolled_k = pltpu.roll(k_ref[...].astype(jnp.float32), half, 1)
    values = v_ref[...].astype(jnp.float32)
    kvsend[0] = jnp.where(low, values, rolled_k).astype(jnp.bfloat16)
    kvsend[1] = jnp.where(low, rolled_k, values).astype(jnp.bfloat16)
    bias_rows = gate_ref[...] * (-math.log2(math.e))
    bsend[0] = bias_rows[0:1]
    bsend[1] = bias_rows[1:2]
    mine = low == (head == 1)

    def prepare(raw):
        rolled = pltpu.roll(raw.astype(jnp.float32), half, 1)
        return jnp.where(mine, rolled, 0.0).astype(jnp.bfloat16)

    qbuf[own_slot] = prepare(q_ref[...])
    peak[...] = jnp.full(peak.shape, NEG_LARGE, jnp.float32)
    total[...] = jnp.zeros(total.shape, jnp.float32)
    acc[...] = jnp.zeros(acc.shape, jnp.float32)

    pl.semaphore_wait(barrier, (n - 1) + 2 * (n_tp - 1))

    q_copy = pltpu.make_async_remote_copy(
        src_ref=q_ref,
        dst_ref=qraw,
        send_sem=q_send,
        recv_sem=q_recv,
        device_id=(mirror, mt),
        device_id_type=MESH,
    )
    q_copy.start()

    w_half = w_ref.shape[0] // 2

    def w_mine(k):
        return lax.rem(z - sign * (1 + k) + 2 * nz, nz) * 2 + core

    def w_theirs(k):
        return lax.rem(z + sign * (1 + k) + 2 * nz, nz) * 2 + 1 - core

    def w_ring(k, s, src):
        return pltpu.make_async_remote_copy(
            src_ref=src.at[pl.ds(s * w_half, w_half)],
            dst_ref=wbuf.at[w_mine(k), pl.ds(s * w_half, w_half)],
            send_sem=w_send.at[k, s],
            recv_sem=w_recv.at[lax.rem(k + 1, nz), s],
            device_id=nxt,
            device_id_type=MESH,
        )

    def w_share(k, s, src):
        return pltpu.make_async_remote_copy(
            src_ref=src.at[pl.ds(s * w_half, w_half)],
            dst_ref=wbuf.at[w_mine(k), pl.ds(s * w_half, w_half)],
            send_sem=d_send.at[k, s],
            recv_sem=d_recv.at[k, s],
            device_id=partner,
            device_id_type=MESH,
        )

    for s in range(2):
        w_ring(nz - 1, s, w_ref).start()

    def kv_copy(r):
        hr = lax.div(r, n // 2)
        return (
            pltpu.make_async_remote_copy(
                src_ref=kvsend.at[hr],
                dst_ref=kvbuf.at[me],
                send_sem=kv_send.at[r],
                recv_sem=kv_recv.at[me],
                device_id=(r, mt),
                device_id_type=MESH,
            ),
            pltpu.make_async_remote_copy(
                src_ref=bsend.at[hr],
                dst_ref=bbuf.at[me],
                send_sem=b_send.at[r],
                recv_sem=b_recv.at[me],
                device_id=(r, mt),
                device_id_type=MESH,
            ),
        )

    def send_body(k, c):
        r = lax.rem(me + k, n)

        @pl.when(me <= jnp.maximum(r, n - 1 - r))
        def _():
            ck, cb = kv_copy(r)
            cb.start()
            ck.start()

        return c

    lax.fori_loop(1, n, send_body, 0)
    for s in range(2):
        w_share(nz - 1, s, w_ref).start()

    sub = min(256, rows)

    def tile(slot, kv_at, bias_at, diagonal):
        for i in range(rows // sub):
            kv = kv_at[...]
            rs = pl.ds(i * sub, sub)
            s = lax.dot_general(
                qbuf[slot, rs, :], kv, (((1,), (1,)), ((), ())), preferred_element_type=jnp.float32
            )
            s = s * coef + bias_at[...]
            if diagonal:
                qp = lax.broadcasted_iota(jnp.int32, s.shape, 0) + i * sub
                kp = lax.broadcasted_iota(jnp.int32, s.shape, 1)
                s = jnp.where(kp <= qp, s, NEG_LARGE)
            old = peak[slot, rs, :]
            new = jnp.maximum(old, jnp.max(s, axis=1, keepdims=True))
            e = jnp.exp2(s - new)
            alpha = jnp.exp2(old - new)
            total[slot, rs, :] = total[slot, rs, :] * alpha + jnp.sum(e, axis=1, keepdims=True)
            acc[slot, rs, :] = acc[slot, rs, :] * alpha + jnp.dot(
                e.astype(jnp.bfloat16), kv, preferred_element_type=jnp.float32
            )
            peak[slot, rs, :] = new

    tile(own_slot, kvsend.at[head], bsend.at[head], True)
    pltpu.make_async_copy(q_ref, qraw, q_recv).wait()
    qbuf[1 - own_slot] = prepare(qraw[...])

    @pl.when(me < last)
    def _():
        tile(1, kvsend.at[head], bsend.at[head], False)

    def w_event(i):
        k = lax.div(i, 2)
        s = lax.rem(i, 2)
        block = wbuf.at[w_mine(k)]
        pltpu.make_async_copy(
            w_ref.at[pl.ds(0, w_half)], block.at[pl.ds(s * w_half, w_half)], w_recv.at[k, s]
        ).wait()

        @pl.when(k < nz - 2)
        def _():
            w_ring(k, s, block).start()

        w_share(k, s, block).start()

    events = 2 * (nz - 1)
    early = max(0, min(events, n - 3))

    def compute_body(k, c):
        j = lax.rem(me - k + n, n)

        @pl.when(jnp.logical_and(k >= 3, k - 3 < early))
        def _():
            w_event(k - 3)

        @pl.when(j <= last)
        def _():
            pltpu.make_async_copy(kvsend.at[0], kvbuf.at[j], kv_recv.at[j]).wait()
            pltpu.make_async_copy(bsend.at[0], bbuf.at[j], b_recv.at[j]).wait()

            def slot_body(slot, c):
                end = jnp.where(slot == 0, pair, last)

                @pl.when(j == end)
                def _():
                    tile(slot, kvbuf.at[j], bbuf.at[j], True)

                @pl.when(j < end)
                def _():
                    tile(slot, kvbuf.at[j], bbuf.at[j], False)

                return c

            lax.fori_loop(0, 2, slot_body, 0)

        return c

    lax.fori_loop(1, n, compute_body, 0)

    for slot in range(2):
        obuf[slot] = (acc[slot] / total[slot]).astype(jnp.bfloat16)

    def o_target(slot):
        return jnp.where(slot == 0, pair, last)

    def o_copy(slot, t):
        return pltpu.make_async_remote_copy(
            src_ref=obuf.at[slot, pl.ds(t * tok_dev, tok_dev)],
            dst_ref=rbuf.at[mt, head],
            send_sem=o_send.at[slot, t],
            recv_sem=o_recv,
            device_id=(o_target(slot), t),
            device_id_type=MESH,
        )

    def o_self(slot, t):
        return jnp.logical_and(o_target(slot) == me, t == mt)

    def o_body(k, c):
        slot = lax.rem(k, 2)
        t = lax.rem(mt + n_tp // 2 + lax.div(k, 2), n_tp)

        @pl.when(jnp.logical_not(o_self(slot, t)))
        def _():
            o_copy(slot, t).start()

        @pl.when(o_self(slot, t))
        def _():
            pltpu.make_async_copy(
                obuf.at[slot, pl.ds(t * tok_dev, tok_dev)], rbuf.at[mt, head], o_recv
            ).start()

        return c

    lax.fori_loop(0, 2 * n_tp, o_body, 0)

    def late_event(i, c):
        w_event(i)
        return c

    lax.fori_loop(early, events, late_event, 0)

    number = lax.broadcasted_iota(jnp.int32, (n, tok_dev), 0)
    before = (
        lax.broadcasted_iota(jnp.int32, (tok_dev, tok_dev), 0)
        < lax.broadcasted_iota(jnp.int32, (tok_dev, tok_dev), 1)
    ).astype(bf16)
    expand = (
        lax.div(lax.broadcasted_iota(jnp.int32, (padded, n), 0), SLOTS)
        == lax.broadcasted_iota(jnp.int32, (padded, n), 1)
    ).astype(bf16)
    inside = lax.rem(lax.broadcasted_iota(jnp.int32, (padded, tok_dev), 0), SLOTS).astype(f32)
    taken = jnp.zeros((n, 1), f32)
    for r in range(ids_ref.shape[0]):
        named = (number == ids_ref[r : r + 1, :]).astype(f32)
        rank = jnp.dot(named.astype(bf16), before, preferred_element_type=f32) + taken
        taken = taken + jnp.sum(named, axis=1, keepdims=True)
        named_at = jnp.dot(expand, named.astype(bf16), preferred_element_type=f32)
        rank_at = jnp.dot(expand, rank.astype(bf16), preferred_element_type=f32)
        place[r] = jnp.where(rank_at == inside, named_at, 0.0).astype(bf16)
    compact = lax.broadcasted_iota(jnp.int32, (expert_rows, padded), 0)
    spaced = lax.broadcasted_iota(jnp.int32, (expert_rows, padded), 1)
    keep[...] = (
        lax.div(compact, capacity) * SLOTS + lax.rem(compact, capacity) == spaced
    ).astype(bf16)
    eye = (
        lax.broadcasted_iota(jnp.int32, (padded, padded), 0)
        == lax.broadcasted_iota(jnp.int32, (padded, padded), 1)
    ).astype(bf16)
    first = (((0,), (0,)), ((), ()))
    sent_to = place[0]
    for r in range(1, ids_ref.shape[0]):
        sent_to = sent_to + place[r]
    ext[nz - 1, :, model:] = lax.dot_general(
        sent_to, eye, first, preferred_element_type=f32
    ).astype(bf16)

    pltpu.make_async_copy(rbuf, rbuf, o_recv).wait()
    own_w.wait()
    for s in range(2):
        pltpu.make_async_copy(
            w_ref.at[pl.ds(0, w_half)], wbuf.at[mt, pl.ds(s * w_half, w_half)], d_recv.at[nz - 1, s]
        ).wait()
    low32 = lax.broadcasted_iota(jnp.int32, (tok_dev, width), 1) < half

    def product(t):
        piece = jnp.where(
            low32, rbuf[t, 0].astype(jnp.float32), rbuf[t, 1].astype(jnp.float32)
        ).astype(jnp.bfloat16)
        return jnp.dot(piece, wbuf[t], preferred_element_type=jnp.float32)

    proj[...] = product(mt)
    proj[...] += product(z * 2 + 1 - core)

    def project(k, c):
        for s in range(2):
            pltpu.make_async_copy(
                w_ref.at[pl.ds(0, w_half)],
                wbuf.at[w_theirs(k), pl.ds(s * w_half, w_half)],
                d_recv.at[k, s],
            ).wait()
        proj[...] += product(w_mine(k))
        proj[...] += product(w_theirs(k))
        return c

    lax.fori_loop(0, nz - 1, project, 0)
    stream = (tok_ref[...].astype(f32) + proj[...]).astype(bf16)
    stream_ref[...] = stream
    stream_wide = stream.astype(f32)
    inverse = lax.rsqrt(jnp.mean(stream_wide * stream_wide, axis=1, keepdims=True) + 1e-05)
    ext[nz - 1, :, :model] = (stream_wide * inverse * gain_ref[...]).astype(bf16)

    def ring(k):
        return pltpu.make_async_remote_copy(
            src_ref=ext.at[k],
            dst_ref=ext.at[lax.rem(k + 1, nz)],
            send_sem=x_send.at[k],
            recv_sem=x_recv.at[lax.rem(k + 1, nz)],
            device_id=nxt,
            device_id_type=MESH,
        )

    def to_expert(k, e):
        return pltpu.make_async_remote_copy(
            src_ref=packed.at[k, e],
            dst_ref=arrived.at[k, me],
            send_sem=a_send.at[k, e],
            recv_sem=a_recv.at[k],
            device_id=(e, mt),
            device_id_type=MESH,
        )

    def share(k):
        return pltpu.make_async_remote_copy(
            src_ref=xbuf.at[core, k],
            dst_ref=xbuf.at[core, k],
            send_sem=s_send.at[k],
            recv_sem=s_recv.at[k],
            device_id=partner,
            device_id_type=MESH,
        )

    parts = 2
    part_rows = expert_rows // parts

    def part(s):
        return pl.ds(s * part_rows, part_rows)

    def give(k, s):
        return pltpu.make_async_remote_copy(
            src_ref=psend.at[k, part(s)],
            dst_ref=precv.at[k, part(s)],
            send_sem=p_send.at[k, s],
            recv_sem=p_recv.at[k, s],
            device_id=partner,
            device_id_type=MESH,
        )

    def reduce(k, s):
        return pltpu.make_async_remote_copy(
            src_ref=rsend.at[k, part(s)],
            dst_ref=rrecv.at[k, part(s)],
            send_sem=r_send.at[k, s],
            recv_sem=r_recv.at[k, s],
            device_id=nxt,
            device_id_type=MESH,
        )

    def to_token(s):
        return pltpu.make_async_remote_copy(
            src_ref=spread.at[s],
            dst_ref=back.at[me],
            send_sem=t_send.at[s],
            recv_sem=t_recv,
            device_id=(s, mt),
            device_id_type=MESH,
        )

    def dispatch(k):
        @pl.when(k < nz - 1)
        def _():
            pltpu.make_async_copy(ext.at[0], ext.at[k], x_recv.at[k]).wait()

        @pl.when(k != nz - 2)
        def _():
            ring(k).start()

        block = lax.dot_general(
            ext[k, :, model:], ext[k, :, :model], first, preferred_element_type=f32
        ).astype(bf16)
        for e in range(n):
            packed[k, e] = block[e * SLOTS : (e + 1) * SLOTS]
        pltpu.make_async_copy(packed.at[k, me], arrived.at[k, me], a_recv.at[k]).start()

        def send(i, c):
            to_expert(k, lax.rem(me + i, n)).start()
            return c

        lax.fori_loop(1, n, send, 0)

    def first_dispatch(i, c):
        dispatch(lax.rem(i + nz - 1, nz))
        return c

    ahead = min(2, nz - 1)
    lax.fori_loop(0, ahead + 1, first_dispatch, 0)
    for load in loads[5:]:
        load.wait()

    col_tile = min(512, model)
    across = (((1,), (1,)), ((), ()))

    def step(k, c):
        @pl.when(k + ahead < nz - 1)
        def _():
            dispatch(k + ahead)

        pltpu.make_async_copy(arrived.at[k], arrived.at[k], a_recv.at[k]).wait()
        xbuf[core, k] = jnp.dot(
            keep[...], arrived[k].reshape(padded, model), preferred_element_type=f32
        ).astype(bf16)
        share(k).start()
        pltpu.make_async_copy(xbuf.at[1 - core, 0], xbuf.at[1 - core, k], s_recv.at[k]).wait()

        x = jnp.concatenate([xbuf[1 - core, k], xbuf[core, k]], axis=0)
        g = lax.dot_general(x, gate[...], across, preferred_element_type=f32)
        u = lax.dot_general(x, up[...], across, preferred_element_type=f32)
        hidden = (g / (1.0 + jnp.exp(-g)) * u).astype(bf16)
        for i in range(model // col_tile):
            cols = slice(i * col_tile, (i + 1) * col_tile)
            p = jnp.dot(hidden, down[:, cols], preferred_element_type=f32)
            psend[k, :, cols] = p[:expert_rows].astype(bf16)
            pown[:, cols] = p[expert_rows:]
        for s in range(parts):
            give(k, s).start()
        for s in range(parts):
            give(k, s).wait_recv()
            both = pown[part(s), :] + precv[k, part(s), :].astype(f32)

            @pl.when(k > 0)
            def _():
                kk = jnp.maximum(k - 1, 0)
                reduce(kk, s).wait_recv()
                pown[part(s), :] = both + rrecv[kk, part(s), :].astype(f32)

            @pl.when(k == 0)
            def _():
                pown[part(s), :] = both

            @pl.when(k < nz - 1)
            def _():
                rsend[k, part(s), :] = pown[part(s), :].astype(bf16)
                reduce(k, s).start()

        return c

    lax.fori_loop(0, nz, step, 0)

    scattered = lax.dot_general(
        keep[...], pown[...].astype(bf16), first, preferred_element_type=f32
    ).astype(bf16)
    for s in range(n):
        spread[s] = scattered[s * SLOTS : (s + 1) * SLOTS]
    pltpu.make_async_copy(spread.at[me], back.at[me], t_recv).start()

    def return_body(k, c):
        to_token(lax.rem(me + k, n)).start()
        return c

    lax.fori_loop(1, n, return_body, 0)

    q_copy.wait_send()

    def drain_body(k, c):
        r = lax.rem(me + k, n)

        @pl.when(me <= jnp.maximum(r, n - 1 - r))
        def _():
            ck, cb = kv_copy(r)
            cb.wait_send()
            ck.wait_send()

        return c

    lax.fori_loop(1, n, drain_body, 0)

    def o_drain(k, c):
        slot = lax.rem(k, 2)
        t = lax.div(k, 2)

        @pl.when(jnp.logical_not(o_self(slot, t)))
        def _():
            o_copy(slot, t).wait_send()

        return c

    lax.fori_loop(0, 2 * n_tp, o_drain, 0)

    def w_drain(k, c):
        for s in range(2):
            w_share(k, s, w_ref).wait_send()

            @pl.when(k != nz - 2)
            def _():
                w_ring(k, s, w_ref).wait_send()

        return c

    lax.fori_loop(0, nz, w_drain, 0)

    def drain(k, c):
        for s in range(parts):
            give(k, s).wait_send()

            @pl.when(k < nz - 1)
            def _():
                reduce(k, s).wait_send()

        @pl.when(k != nz - 2)
        def _():
            ring(k).wait_send()

        share(k).wait_send()

        def drain_send(i, c):
            to_expert(k, lax.rem(me + i, n)).wait_send()
            return c

        lax.fori_loop(1, n, drain_send, 0)
        return c

    lax.fori_loop(0, nz, drain, 0)

    pltpu.make_async_copy(back, back, t_recv).wait()
    rows_back = back[...].reshape(padded, model)
    diagonal = lax.broadcasted_iota(jnp.int32, (tok_dev, tok_dev), 0) == lax.broadcasted_iota(
        jnp.int32, (tok_dev, tok_dev), 1
    )
    mixture = jnp.zeros((tok_dev, model), f32)
    for r in range(ids_ref.shape[0]):
        picked = lax.dot_general(place[r], rows_back, first, preferred_element_type=f32)
        weight = jnp.sum(
            jnp.where(diagonal, route_ref[r : r + 1, :], 0.0), axis=1, keepdims=True
        )
        mixture = mixture + picked * weight
    out_ref[...] = (stream_ref[...].astype(f32) + mixture).astype(bf16)

    def drain_back(k, c):
        to_token(lax.rem(me + k, n)).wait_send()
        return c

    lax.fori_loop(1, n, drain_back, 0)


def shards(
    tokens,
    query_vectors,
    key_vectors,
    value_vectors,
    cum_gate,
    out_weight,
    norm_gain,
    gate_weight,
    up_weight,
    down_weight,
    expert_ids,
    route_weights,
):
    n = lax.axis_size("sp")
    n_tp = lax.axis_size("tp")
    nz = n_tp // 2
    rows, width = query_vectors.shape
    tok_dev, model = tokens.shape
    top = expert_ids.shape[1]
    inner = gate_weight.shape[2]
    capacity = max(2, 3 * tok_dev * top // (2 * n))
    assert capacity <= SLOTS and gate_weight.shape[0] == 1
    expert_rows = n * capacity
    padded = n * SLOTS
    coef = (width // 2) ** (-0.5) * math.log2(math.e)
    vmem = pl.BlockSpec(memory_space=pltpu.VMEM)
    hbm = pl.BlockSpec(memory_space=pl.ANY)
    bf16, f32 = jnp.bfloat16, jnp.float32
    dma = pltpu.SemaphoreType.DMA
    return pl.pallas_call(
        functools.partial(layer_kernel, n, n_tp, coef, capacity),
        out_shape=jax.ShapeDtypeStruct((tok_dev, model), bf16),
        in_specs=[hbm, hbm, hbm, vmem, hbm, hbm, vmem, vmem, vmem, hbm, hbm, hbm],
        out_specs=vmem,
        scratch_shapes=[
            pltpu.VMEM((rows, width), bf16),
            pltpu.VMEM((rows, width), bf16),
            pltpu.VMEM((rows, width), bf16),
            pltpu.VMEM((width, model), bf16),
            pltpu.VMEM((tok_dev, model), bf16),
            pltpu.VMEM((inner, model), bf16),
            pltpu.VMEM((inner, model), bf16),
            pltpu.VMEM((inner, model), bf16),
            pltpu.VMEM((rows, width), bf16),
            pltpu.VMEM((2, rows, width), bf16),
            pltpu.VMEM((2, rows, width), bf16),
            pltpu.VMEM((2, 1, rows), f32),
            pltpu.VMEM((n, rows, width), bf16),
            pltpu.VMEM((n, 1, rows), f32),
            pltpu.VMEM((2, rows, 1), f32),
            pltpu.VMEM((2, rows, 1), f32),
            pltpu.VMEM((2, rows, width), f32),
            pltpu.VMEM((2, rows, width), bf16),
            pltpu.VMEM((n_tp, 2, tok_dev, width), bf16),
            pltpu.VMEM((n_tp, width, model), bf16),
            pltpu.VMEM((tok_dev, model), f32),
            pltpu.VMEM((tok_dev, model), bf16),
            pltpu.VMEM((top, padded, tok_dev), bf16),
            pltpu.VMEM((expert_rows, padded), bf16),
            pltpu.VMEM((nz, tok_dev, model + padded), bf16),
            pltpu.VMEM((nz, n, SLOTS, model), bf16),
            pltpu.VMEM((nz, n, SLOTS, model), bf16),
            pltpu.VMEM((2, nz, expert_rows, model), bf16),
            pltpu.VMEM((expert_rows, model), f32),
            pltpu.VMEM((nz, expert_rows, model), bf16),
            pltpu.VMEM((nz, expert_rows, model), bf16),
            pltpu.VMEM((nz - 1, expert_rows, model), bf16),
            pltpu.VMEM((nz - 1, expert_rows, model), bf16),
            pltpu.VMEM((n, SLOTS, model), bf16),
            pltpu.VMEM((n, SLOTS, model), bf16),
            dma((8,)),
            dma((n,)),
            dma((n,)),
            dma((n,)),
            dma((n,)),
            dma,
            dma,
            dma((2, n_tp)),
            dma,
            dma((nz, 2)),
            dma((nz, 2)),
            dma((nz, 2)),
            dma((nz, 2)),
            dma((1,)),
            dma((nz,)),
            dma((nz,)),
            dma((nz, n)),
            dma((nz,)),
            dma((nz,)),
            dma((nz,)),
            dma((nz, 2)),
            dma((nz, 2)),
            dma((nz - 1, 2)),
            dma((nz - 1, 2)),
            dma((n,)),
            dma,
        ],
        compiler_params=pltpu.CompilerParams(
            collective_id=0, has_side_effects=True, vmem_limit_bytes=67000000
        ),
        name="layer",
    )(
        query_vectors,
        key_vectors,
        value_vectors,
        cum_gate.T,
        out_weight,
        tokens,
        norm_gain[None, :],
        expert_ids.T,
        route_weights.T,
        jnp.swapaxes(gate_weight[0], 0, 1),
        jnp.swapaxes(up_weight[0], 0, 1),
        down_weight[0],
    )


def solution(mesh):
    in_specs = (
        P(("sp", "tp"), None),
        P("sp", "tp"),
        P("sp", "tp"),
        P("sp", "tp"),
        P("sp", "tp"),
        P("tp", None),
        P(),
        P("sp", None, "tp"),
        P("sp", None, "tp"),
        P("sp", "tp", None),
        P(("sp", "tp"), None),
        P(("sp", "tp"), None),
    )
    out_specs = P(("sp", "tp"), None)
    return jax.shard_map(shards, mesh=mesh, in_specs=in_specs, out_specs=out_specs, check_vma=False)
```

```python
import functools
import math

import jax
import jax.numpy as jnp
from jax import lax
from jax.experimental import pallas as pl
from jax.experimental.pallas import tpu as pltpu
from jax.sharding import PartitionSpec as P

NEG_LARGE = -1e30
MESH = pl.DeviceIdType.MESH
SLOTS = 8


def layer_kernel(
    n,
    n_tp,
    coef,
    capacity,
    q_hbm,
    k_hbm,
    v_hbm,
    gate_ref,
    w_hbm,
    tok_hbm,
    gain_ref,
    ids_ref,
    route_ref,
    wg_hbm,
    wu_hbm,
    wd_hbm,
    out_ref,
    q_ref,
    k_ref,
    v_ref,
    w_ref,
    tok_ref,
    gate,
    up,
    down,
    qraw,
    qbuf,
    kvsend,
    bsend,
    kvbuf,
    bbuf,
    peak,
    total,
    acc,
    obuf,
    rbuf,
    wbuf,
    proj,
    stream_ref,
    place,
    keep,
    keep_tail,
    folds,
    ext,
    packed,
    arrived,
    xbuf,
    pown,
    psend,
    precv,
    rsend,
    rrecv,
    spread,
    back,
    in_sem,
    kv_send,
    kv_recv,
    b_send,
    b_recv,
    q_send,
    q_recv,
    o_send,
    o_recv,
    w_send,
    w_recv,
    d_send,
    d_recv,
    v_send,
    v_recv,
    own_sem,
    x_send,
    x_recv,
    a_send,
    a_recv,
    s_send,
    s_recv,
    p_send,
    p_recv,
    r_send,
    r_recv,
    t_send,
    t_recv,
):
    me = lax.axis_index("sp")
    mt = lax.axis_index("tp")
    nz = n_tp // 2
    z = lax.div(mt, 2)
    core = lax.rem(mt, 2)
    sign = 1 - 2 * core
    nxt = (me, lax.rem(z + sign + nz, nz) * 2 + core)
    partner = (me, z * 2 + 1 - core)
    mirror = n - 1 - me
    head = lax.div(me, n // 2)
    pair = jnp.minimum(me, mirror)
    last = jnp.maximum(me, mirror)
    own_slot = head
    rows, width = q_ref.shape
    half = width // 2
    tok_dev, model = tok_ref.shape
    bf16, f32 = jnp.bfloat16, jnp.float32
    expert_rows = n * capacity
    padded = n * SLOTS

    loads = [
        pltpu.make_async_copy(a, b, in_sem.at[i])
        for i, (a, b) in enumerate(
            (
                (k_hbm, k_ref),
                (v_hbm, v_ref),
                (q_hbm, q_ref),
                (w_hbm, w_ref),
                (tok_hbm, tok_ref),
                (wg_hbm, gate),
                (wu_hbm, up),
                (wd_hbm, down),
            )
        )
    ]
    for load in loads:
        load.start()

    barrier = pltpu.get_barrier_semaphore()

    def greet_plane(k, c):
        pl.semaphore_signal(
            barrier, inc=1, device_id=(lax.rem(me + k, n), mt), device_id_type=MESH
        )
        return c

    def greet_heads(k, c):
        t = lax.rem(mt + k, n_tp)
        pl.semaphore_signal(barrier, inc=1, device_id=(me, t), device_id_type=MESH)
        pl.semaphore_signal(barrier, inc=1, device_id=(mirror, t), device_id_type=MESH)
        return c

    lax.fori_loop(1, n, greet_plane, 0)
    lax.fori_loop(1, n_tp, greet_heads, 0)

    own_w = pltpu.make_async_copy(w_hbm, wbuf.at[mt], own_sem.at[0])
    own_w.start()
    for load in loads[:5]:
        load.wait()
    lane = lax.broadcasted_iota(jnp.int32, (rows, width), 1)
    low = lane < half
    rolled_k = pltpu.roll(k_ref[...].astype(jnp.float32), half, 1)
    values = v_ref[...].astype(jnp.float32)
    kvsend[0] = jnp.where(low, values, rolled_k).astype(jnp.bfloat16)
    kvsend[1] = jnp.where(low, rolled_k, values).astype(jnp.bfloat16)
    bias_rows = gate_ref[...] * (-math.log2(math.e))
    bsend[0] = bias_rows[0:1]
    bsend[1] = bias_rows[1:2]
    mine = low == (head == 1)

    def prepare(raw):
        rolled = pltpu.roll(raw.astype(jnp.float32), half, 1)
        return jnp.where(mine, rolled, 0.0).astype(jnp.bfloat16)

    qbuf[own_slot] = prepare(q_ref[...])
    peak[...] = jnp.full(peak.shape, NEG_LARGE, jnp.float32)
    total[...] = jnp.zeros(total.shape, jnp.float32)
    acc[...] = jnp.zeros(acc.shape, jnp.float32)

    pl.semaphore_wait(barrier, (n - 1) + 2 * (n_tp - 1))

    q_copy = pltpu.make_async_remote_copy(
        src_ref=q_ref,
        dst_ref=qraw,
        send_sem=q_send,
        recv_sem=q_recv,
        device_id=(mirror, mt),
        device_id_type=MESH,
    )
    q_copy.start()

    w_half = w_ref.shape[0] // 2
    w_sub = w_half // 2
    w_quarter = w_half // 4
    side = math.isqrt(n)
    row = lax.div(me, side)
    column = lax.rem(me, side)
    colour = lax.rem(row + column, 2)
    neighbours = (
        row * side + lax.rem(column + 1, side),
        row * side + lax.rem(column + side - 1, side),
        lax.rem(row + 1, side) * side + column,
        lax.rem(row + side - 1, side) * side + column,
    )

    def sub_rows(s):
        return pl.ds(colour * w_half + s * w_sub, w_sub)

    def quarter_rows(i):
        return pl.ds(colour * w_half + i * w_quarter, w_quarter)

    other_rows = pl.ds((1 - colour) * w_half, w_half)

    def w_mine(k):
        return lax.rem(z - sign * (1 + k) + 2 * nz, nz) * 2 + core

    def w_theirs(k):
        return lax.rem(z + sign * (1 + k) + 2 * nz, nz) * 2 + 1 - core

    def w_ring(k, s, src):
        return pltpu.make_async_remote_copy(
            src_ref=src.at[sub_rows(s)],
            dst_ref=wbuf.at[w_mine(k), sub_rows(s)],
            send_sem=w_send.at[k, s],
            recv_sem=w_recv.at[lax.rem(k + 1, nz), s],
            device_id=nxt,
            device_id_type=MESH,
        )

    def w_plane(k, i, target, src):
        return pltpu.make_async_remote_copy(
            src_ref=src.at[quarter_rows(i)],
            dst_ref=wbuf.at[w_mine(k), quarter_rows(i)],
            send_sem=v_send.at[k, i],
            recv_sem=v_recv.at[k],
            device_id=(target, mt),
            device_id_type=MESH,
        )

    def w_share(k, s, src):
        return pltpu.make_async_remote_copy(
            src_ref=src.at[sub_rows(s)],
            dst_ref=wbuf.at[w_mine(k), sub_rows(s)],
            send_sem=d_send.at[k, s],
            recv_sem=d_recv.at[k, s],
            device_id=partner,
            device_id_type=MESH,
        )

    def w_share_rest(k, src):
        return pltpu.make_async_remote_copy(
            src_ref=src.at[other_rows],
            dst_ref=wbuf.at[w_mine(k), other_rows],
            send_sem=d_send.at[k, 2],
            recv_sem=d_recv.at[k, 2],
            device_id=partner,
            device_id_type=MESH,
        )

    for s in range(2):
        w_ring(nz - 1, s, w_ref).start()

    def kv_copy(r):
        hr = lax.div(r, n // 2)
        return (
            pltpu.make_async_remote_copy(
                src_ref=kvsend.at[hr],
                dst_ref=kvbuf.at[me],
                send_sem=kv_send.at[r],
                recv_sem=kv_recv.at[me],
                device_id=(r, mt),
                device_id_type=MESH,
            ),
            pltpu.make_async_remote_copy(
                src_ref=bsend.at[hr],
                dst_ref=bbuf.at[me],
                send_sem=b_send.at[r],
                recv_sem=b_recv.at[me],
                device_id=(r, mt),
                device_id_type=MESH,
            ),
        )

    def send_body(k, c):
        r = lax.rem(me + k, n)

        @pl.when(me <= jnp.maximum(r, n - 1 - r))
        def _():
            ck, cb = kv_copy(r)
            cb.start()
            ck.start()

        return c

    lax.fori_loop(1, n, send_body, 0)
    for s in range(2):
        w_share(nz - 1, s, w_ref).start()
    w_share_rest(nz - 1, w_ref).start()

    sub = min(256, rows)

    def tile(slot, kv_at, bias_at, diagonal):
        for i in range(rows // sub):
            kv = kv_at[...]
            rs = pl.ds(i * sub, sub)
            s = lax.dot_general(
                qbuf[slot, rs, :], kv, (((1,), (1,)), ((), ())), preferred_element_type=jnp.float32
            )
            s = s * coef + bias_at[...]
            if diagonal:
                qp = lax.broadcasted_iota(jnp.int32, s.shape, 0) + i * sub
                kp = lax.broadcasted_iota(jnp.int32, s.shape, 1)
                s = jnp.where(kp <= qp, s, NEG_LARGE)
            old = peak[slot, rs, :]
            new = jnp.maximum(old, jnp.max(s, axis=1, keepdims=True))
            e = jnp.exp2(s - new)
            alpha = jnp.exp2(old - new)
            total[slot, rs, :] = total[slot, rs, :] * alpha + jnp.sum(e, axis=1, keepdims=True)
            acc[slot, rs, :] = acc[slot, rs, :] * alpha + jnp.dot(
                e.astype(jnp.bfloat16), kv, preferred_element_type=jnp.float32
            )
            peak[slot, rs, :] = new

    tile(own_slot, kvsend.at[head], bsend.at[head], True)
    pltpu.make_async_copy(q_ref, qraw, q_recv).wait()
    qbuf[1 - own_slot] = prepare(qraw[...])

    @pl.when(me < last)
    def _():
        tile(1, kvsend.at[head], bsend.at[head], False)

    def w_event(i):
        k = lax.div(i, 2)
        s = lax.rem(i, 2)
        block = wbuf.at[w_mine(k)]
        pltpu.make_async_copy(
            w_ref.at[pl.ds(0, w_sub)], block.at[sub_rows(s)], w_recv.at[k, s]
        ).wait()

        @pl.when(k < nz - 2)
        def _():
            w_ring(k, s, block).start()

        for j in range(2):
            target = jnp.where(s == 0, neighbours[j], neighbours[2 + j])
            w_plane(k, 2 * s + j, target, block).start()
        w_share(k, s, block).start()

    def w_rest(k, c):
        block = wbuf.at[w_mine(k)]
        pltpu.make_async_copy(
            w_ref.at[pl.ds(0, w_half)], block.at[other_rows], v_recv.at[k]
        ).wait()
        w_share_rest(k, block).start()
        return c

    def w_partner(k, t):
        for s in range(2):
            pltpu.make_async_copy(
                w_ref.at[pl.ds(0, w_sub)], wbuf.at[t, sub_rows(s)], d_recv.at[k, s]
            ).wait()
        pltpu.make_async_copy(
            w_ref.at[pl.ds(0, w_half)], wbuf.at[t, other_rows], d_recv.at[k, 2]
        ).wait()

    events = 2 * (nz - 1)
    early = max(0, min(events, n - 2))

    def compute_body(k, c):
        j = lax.rem(me - k + n, n)

        @pl.when(jnp.logical_and(k >= 2, k - 2 < early))
        def _():
            w_event(k - 2)

        @pl.when(j <= last)
        def _():
            pltpu.make_async_copy(kvsend.at[0], kvbuf.at[j], kv_recv.at[j]).wait()
            pltpu.make_async_copy(bsend.at[0], bbuf.at[j], b_recv.at[j]).wait()

            def slot_body(slot, c):
                end = jnp.where(slot == 0, pair, last)

                @pl.when(j == end)
                def _():
                    tile(slot, kvbuf.at[j], bbuf.at[j], True)

                @pl.when(j < end)
                def _():
                    tile(slot, kvbuf.at[j], bbuf.at[j], False)

                return c

            lax.fori_loop(0, 2, slot_body, 0)

        return c

    lax.fori_loop(1, n, compute_body, 0)

    for slot in range(2):
        obuf[slot] = (acc[slot] / total[slot]).astype(jnp.bfloat16)

    def o_target(slot):
        return jnp.where(slot == 0, pair, last)

    def o_copy(slot, t):
        return pltpu.make_async_remote_copy(
            src_ref=obuf.at[slot, pl.ds(t * tok_dev, tok_dev)],
            dst_ref=rbuf.at[mt, head],
            send_sem=o_send.at[slot, t],
            recv_sem=o_recv,
            device_id=(o_target(slot), t),
            device_id_type=MESH,
        )

    def o_self(slot, t):
        return jnp.logical_and(o_target(slot) == me, t == mt)

    def o_body(k, c):
        slot = lax.rem(k, 2)
        t = lax.rem(mt + n_tp // 2 + lax.div(k, 2), n_tp)

        @pl.when(jnp.logical_not(o_self(slot, t)))
        def _():
            o_copy(slot, t).start()

        @pl.when(o_self(slot, t))
        def _():
            pltpu.make_async_copy(
                obuf.at[slot, pl.ds(t * tok_dev, tok_dev)], rbuf.at[mt, head], o_recv
            ).start()

        return c

    lax.fori_loop(0, 2 * n_tp, o_body, 0)

    def late_event(i, c):
        w_event(i)
        return c

    lax.fori_loop(early, events, late_event, 0)
    lax.fori_loop(0, nz - 1, w_rest, 0)

    number = lax.broadcasted_iota(jnp.int32, (n, tok_dev), 0)
    before = (
        lax.broadcasted_iota(jnp.int32, (tok_dev, tok_dev), 0)
        < lax.broadcasted_iota(jnp.int32, (tok_dev, tok_dev), 1)
    ).astype(bf16)
    expand = (
        lax.div(lax.broadcasted_iota(jnp.int32, (padded, n), 0), SLOTS)
        == lax.broadcasted_iota(jnp.int32, (padded, n), 1)
    ).astype(bf16)
    inside = lax.rem(lax.broadcasted_iota(jnp.int32, (padded, tok_dev), 0), SLOTS).astype(f32)
    eye = (
        lax.broadcasted_iota(jnp.int32, (padded, padded), 0)
        == lax.broadcasted_iota(jnp.int32, (padded, padded), 1)
    ).astype(bf16)
    first = (((0,), (0,)), ((), ()))
    taken = jnp.zeros((n, 1), f32)
    for r in range(ids_ref.shape[0]):
        named = (number == ids_ref[r : r + 1, :]).astype(f32)
        rank = jnp.dot(named.astype(bf16), before, preferred_element_type=f32) + taken
        taken = taken + jnp.sum(named, axis=1, keepdims=True)
        named_at = jnp.dot(expand, named.astype(bf16), preferred_element_type=f32)
        rank_at = jnp.dot(expand, rank.astype(bf16), preferred_element_type=f32)
        placed = jnp.where(rank_at == inside, named_at, 0.0).astype(bf16)
        place[r] = lax.dot_general(placed, eye, first, preferred_element_type=f32).astype(bf16)
    compact = lax.broadcasted_iota(jnp.int32, (expert_rows, padded), 0)
    spaced = lax.broadcasted_iota(jnp.int32, (expert_rows, padded), 1)
    keep[...] = (
        lax.div(compact, capacity) * SLOTS + lax.rem(compact, capacity) == spaced
    ).astype(bf16)
    spare = SLOTS - capacity
    each = capacity // spare
    third = lax.broadcasted_iota(jnp.int32, (expert_rows, each * padded), 1)
    kept = lax.broadcasted_iota(jnp.int32, (expert_rows, each * padded), 0)
    kept_in = lax.rem(kept, capacity)
    keep_tail[...] = jnp.logical_and(
        lax.rem(third, padded)
        == lax.div(kept, capacity) * SLOTS + capacity + lax.div(kept_in, each),
        lax.div(third, padded) == lax.rem(kept_in, each),
    ).astype(bf16)
    slot = lax.broadcasted_iota(jnp.int32, (padded, each * padded), 0)
    target = lax.broadcasted_iota(jnp.int32, (padded, each * padded), 1)
    target_row = lax.rem(target, padded)
    target_in = lax.rem(target_row, SLOTS)
    folds[...] = jnp.logical_and(
        target_in >= capacity,
        slot
        == lax.div(target_row, SLOTS) * SLOTS
        + (target_in - capacity) * each
        + lax.div(target, padded),
    ).astype(bf16)
    sent_to = place[0]
    for r in range(1, ids_ref.shape[0]):
        sent_to = sent_to + place[r]
    ext[nz - 1, :, model:] = sent_to

    pltpu.make_async_copy(rbuf, rbuf, o_recv).wait()
    own_w.wait()
    w_partner(nz - 1, z * 2 + 1 - core)
    low32 = lax.broadcasted_iota(jnp.int32, (tok_dev, width), 1) < half

    def product(t):
        piece = jnp.where(
            low32, rbuf[t, 0].astype(jnp.float32), rbuf[t, 1].astype(jnp.float32)
        ).astype(jnp.bfloat16)
        return jnp.dot(piece, wbuf[t], preferred_element_type=jnp.float32)

    proj[...] = product(mt)
    proj[...] += product(z * 2 + 1 - core)

    def project(k, c):
        w_partner(k, w_theirs(k))
        proj[...] += product(w_mine(k))
        proj[...] += product(w_theirs(k))
        return c

    lax.fori_loop(0, nz - 1, project, 0)
    stream = (tok_ref[...].astype(f32) + proj[...]).astype(bf16)
    stream_ref[...] = stream
    stream_wide = stream.astype(f32)
    inverse = lax.rsqrt(jnp.mean(stream_wide * stream_wide, axis=1, keepdims=True) + 1e-05)
    ext[nz - 1, :, :model] = (stream_wide * inverse * gain_ref[...]).astype(bf16)

    def ring(k):
        return pltpu.make_async_remote_copy(
            src_ref=ext.at[k],
            dst_ref=ext.at[lax.rem(k + 1, nz)],
            send_sem=x_send.at[k],
            recv_sem=x_recv.at[lax.rem(k + 1, nz)],
            device_id=nxt,
            device_id_type=MESH,
        )

    def to_expert(k, e):
        return pltpu.make_async_remote_copy(
            src_ref=packed.at[k, e],
            dst_ref=arrived.at[k, me],
            send_sem=a_send.at[k, e],
            recv_sem=a_recv.at[k],
            device_id=(e, mt),
            device_id_type=MESH,
        )

    def share(k):
        return pltpu.make_async_remote_copy(
            src_ref=xbuf.at[core, k],
            dst_ref=xbuf.at[core, k],
            send_sem=s_send.at[k],
            recv_sem=s_recv.at[k],
            device_id=partner,
            device_id_type=MESH,
        )

    parts = 2
    part_rows = expert_rows // parts

    def part(s):
        return pl.ds(s * part_rows, part_rows)

    def give(k, s):
        return pltpu.make_async_remote_copy(
            src_ref=psend.at[k, part(s)],
            dst_ref=precv.at[k, part(s)],
            send_sem=p_send.at[k, s],
            recv_sem=p_recv.at[k, s],
            device_id=partner,
            device_id_type=MESH,
        )

    def reduce(k, s):
        return pltpu.make_async_remote_copy(
            src_ref=rsend.at[k, part(s)],
            dst_ref=rrecv.at[k, part(s)],
            send_sem=r_send.at[k, s],
            recv_sem=r_recv.at[k, s],
            device_id=nxt,
            device_id_type=MESH,
        )

    def to_token(s):
        return pltpu.make_async_remote_copy(
            src_ref=spread.at[s],
            dst_ref=back.at[me],
            send_sem=t_send.at[s],
            recv_sem=t_recv,
            device_id=(s, mt),
            device_id_type=MESH,
        )

    body = model * capacity // SLOTS
    fold = body // each

    def unfolded(flat):
        return jnp.concatenate([flat[:, j * fold : (j + 1) * fold] for j in range(each)], axis=0)

    def dispatch(k):
        @pl.when(k < nz - 1)
        def _():
            pltpu.make_async_copy(ext.at[0], ext.at[k], x_recv.at[k]).wait()

        @pl.when(k != nz - 2)
        def _():
            ring(k).start()

        main = ext[k, :, model:]
        tails = jnp.dot(main, folds[...], preferred_element_type=f32).astype(bf16)
        last_columns = ext[k, :, body:model]
        for j in range(each):
            cols = slice(j * fold, (j + 1) * fold)
            block = lax.dot_general(
                jnp.concatenate([main, tails[:, j * padded : (j + 1) * padded]], axis=0),
                jnp.concatenate([ext[k, :, cols], last_columns], axis=0),
                first,
                preferred_element_type=f32,
            ).astype(bf16)
            for e in range(n):
                packed[k, e, :, cols] = block[e * SLOTS : (e + 1) * SLOTS]
        pltpu.make_async_copy(packed.at[k, me], arrived.at[k, me], a_recv.at[k]).start()

        def send(i, c):
            to_expert(k, lax.rem(me + i, n)).start()
            return c

        lax.fori_loop(1, n, send, 0)

    def first_dispatch(i, c):
        dispatch(lax.rem(i + nz - 1, nz))
        return c

    ahead = min(2, nz - 1)
    lax.fori_loop(0, ahead + 1, first_dispatch, 0)
    for load in loads[5:]:
        load.wait()

    col_tile = min(512, model)
    across = (((1,), (1,)), ((), ()))

    def step(k, c):
        @pl.when(k + ahead < nz - 1)
        def _():
            dispatch(k + ahead)

        pltpu.make_async_copy(arrived.at[k], arrived.at[k], a_recv.at[k]).wait()
        flat = arrived[k].reshape(padded, body)
        xbuf[core, k, :, :body] = jnp.dot(
            keep[...], flat, preferred_element_type=f32
        ).astype(bf16)
        xbuf[core, k, :, body:] = jnp.dot(
            keep_tail[...], unfolded(flat), preferred_element_type=f32
        ).astype(bf16)
        share(k).start()
        pltpu.make_async_copy(xbuf.at[1 - core, 0], xbuf.at[1 - core, k], s_recv.at[k]).wait()

        x = jnp.concatenate([xbuf[1 - core, k], xbuf[core, k]], axis=0)
        g = lax.dot_general(x, gate[...], across, preferred_element_type=f32)
        u = lax.dot_general(x, up[...], across, preferred_element_type=f32)
        hidden = (g / (1.0 + jnp.exp(-g)) * u).astype(bf16)
        for i in range(model // col_tile):
            cols = slice(i * col_tile, (i + 1) * col_tile)
            p = jnp.dot(hidden, down[:, cols], preferred_element_type=f32)
            psend[k, :, cols] = p[:expert_rows].astype(bf16)
            pown[:, cols] = p[expert_rows:]
        for s in range(parts):
            give(k, s).start()
        for s in range(parts):
            give(k, s).wait_recv()
            both = pown[part(s), :] + precv[k, part(s), :].astype(f32)

            @pl.when(k > 0)
            def _():
                kk = jnp.maximum(k - 1, 0)
                reduce(kk, s).wait_recv()
                pown[part(s), :] = both + rrecv[kk, part(s), :].astype(f32)

            @pl.when(k == 0)
            def _():
                pown[part(s), :] = both

            @pl.when(k < nz - 1)
            def _():
                rsend[k, part(s), :] = pown[part(s), :].astype(bf16)
                reduce(k, s).start()

        return c

    lax.fori_loop(0, nz, step, 0)

    for j in range(each):
        cols = slice(j * fold, (j + 1) * fold)
        scattered = lax.dot_general(
            jnp.concatenate([keep[...], keep_tail[:, j * padded : (j + 1) * padded]], axis=0),
            jnp.concatenate([pown[:, cols], pown[:, body:]], axis=0).astype(bf16),
            first,
            preferred_element_type=f32,
        ).astype(bf16)
        for s in range(n):
            spread[s, :, cols] = scattered[s * SLOTS : (s + 1) * SLOTS]
    pltpu.make_async_copy(spread.at[me], back.at[me], t_recv).start()

    def return_body(k, c):
        to_token(lax.rem(me + k, n)).start()
        return c

    lax.fori_loop(1, n, return_body, 0)

    q_copy.wait_send()

    def drain_body(k, c):
        r = lax.rem(me + k, n)

        @pl.when(me <= jnp.maximum(r, n - 1 - r))
        def _():
            ck, cb = kv_copy(r)
            cb.wait_send()
            ck.wait_send()

        return c

    lax.fori_loop(1, n, drain_body, 0)

    def o_drain(k, c):
        slot = lax.rem(k, 2)
        t = lax.div(k, 2)

        @pl.when(jnp.logical_not(o_self(slot, t)))
        def _():
            o_copy(slot, t).wait_send()

        return c

    lax.fori_loop(0, 2 * n_tp, o_drain, 0)

    def w_drain(k, c):
        for s in range(2):
            w_share(k, s, w_ref).wait_send()

            @pl.when(k != nz - 2)
            def _():
                w_ring(k, s, w_ref).wait_send()

        w_share_rest(k, w_ref).wait_send()

        @pl.when(k < nz - 1)
        def _():
            for i in range(4):
                w_plane(k, i, neighbours[i], w_ref).wait_send()

        return c

    lax.fori_loop(0, nz, w_drain, 0)

    def drain(k, c):
        for s in range(parts):
            give(k, s).wait_send()

            @pl.when(k < nz - 1)
            def _():
                reduce(k, s).wait_send()

        @pl.when(k != nz - 2)
        def _():
            ring(k).wait_send()

        share(k).wait_send()

        def drain_send(i, c):
            to_expert(k, lax.rem(me + i, n)).wait_send()
            return c

        lax.fori_loop(1, n, drain_send, 0)
        return c

    lax.fori_loop(0, nz, drain, 0)

    pltpu.make_async_copy(back, back, t_recv).wait()
    rows_back = back[...].reshape(padded, body)
    tails_back = unfolded(rows_back)
    diagonal = lax.broadcasted_iota(jnp.int32, (tok_dev, tok_dev), 0) == lax.broadcasted_iota(
        jnp.int32, (tok_dev, tok_dev), 1
    )
    mixture = jnp.zeros((tok_dev, body), f32)
    mixture_tail = jnp.zeros((tok_dev, model - body), f32)
    for r in range(ids_ref.shape[0]):
        chosen = place[r]
        tails = jnp.dot(chosen, folds[...], preferred_element_type=f32).astype(bf16)
        weight = jnp.sum(
            jnp.where(diagonal, route_ref[r : r + 1, :], 0.0), axis=1, keepdims=True
        )
        mixture += weight * jnp.dot(chosen, rows_back, preferred_element_type=f32)
        mixture_tail += weight * jnp.dot(tails, tails_back, preferred_element_type=f32)
    out_ref[:, :body] = (stream_ref[:, :body].astype(f32) + mixture).astype(bf16)
    out_ref[:, body:] = (stream_ref[:, body:].astype(f32) + mixture_tail).astype(bf16)

    def drain_back(k, c):
        to_token(lax.rem(me + k, n)).wait_send()
        return c

    lax.fori_loop(1, n, drain_back, 0)


def shards(
    tokens,
    query_vectors,
    key_vectors,
    value_vectors,
    cum_gate,
    out_weight,
    norm_gain,
    gate_weight,
    up_weight,
    down_weight,
    expert_ids,
    route_weights,
):
    n = lax.axis_size("sp")
    n_tp = lax.axis_size("tp")
    nz = n_tp // 2
    rows, width = query_vectors.shape
    tok_dev, model = tokens.shape
    top = expert_ids.shape[1]
    inner = gate_weight.shape[2]
    capacity = max(2, 3 * tok_dev * top // (2 * n))
    assert capacity < SLOTS and capacity % (SLOTS - capacity) == 0 and gate_weight.shape[0] == 1
    each = capacity // (SLOTS - capacity)
    body = model * capacity // SLOTS
    expert_rows = n * capacity
    padded = n * SLOTS
    coef = (width // 2) ** (-0.5) * math.log2(math.e)
    vmem = pl.BlockSpec(memory_space=pltpu.VMEM)
    hbm = pl.BlockSpec(memory_space=pl.ANY)
    bf16, f32 = jnp.bfloat16, jnp.float32
    dma = pltpu.SemaphoreType.DMA
    return pl.pallas_call(
        functools.partial(layer_kernel, n, n_tp, coef, capacity),
        out_shape=jax.ShapeDtypeStruct((tok_dev, model), bf16),
        in_specs=[hbm, hbm, hbm, vmem, hbm, hbm, vmem, vmem, vmem, hbm, hbm, hbm],
        out_specs=vmem,
        scratch_shapes=[
            pltpu.VMEM((rows, width), bf16),
            pltpu.VMEM((rows, width), bf16),
            pltpu.VMEM((rows, width), bf16),
            pltpu.VMEM((width, model), bf16),
            pltpu.VMEM((tok_dev, model), bf16),
            pltpu.VMEM((inner, model), bf16),
            pltpu.VMEM((inner, model), bf16),
            pltpu.VMEM((inner, model), bf16),
            pltpu.VMEM((rows, width), bf16),
            pltpu.VMEM((2, rows, width), bf16),
            pltpu.VMEM((2, rows, width), bf16),
            pltpu.VMEM((2, 1, rows), f32),
            pltpu.VMEM((n, rows, width), bf16),
            pltpu.VMEM((n, 1, rows), f32),
            pltpu.VMEM((2, rows, 1), f32),
            pltpu.VMEM((2, rows, 1), f32),
            pltpu.VMEM((2, rows, width), f32),
            pltpu.VMEM((2, rows, width), bf16),
            pltpu.VMEM((n_tp, 2, tok_dev, width), bf16),
            pltpu.VMEM((n_tp, width, model), bf16),
            pltpu.VMEM((tok_dev, model), f32),
            pltpu.VMEM((tok_dev, model), bf16),
            pltpu.VMEM((top, tok_dev, padded), bf16),
            pltpu.VMEM((expert_rows, padded), bf16),
            pltpu.VMEM((expert_rows, each * padded), bf16),
            pltpu.VMEM((padded, each * padded), bf16),
            pltpu.VMEM((nz, tok_dev, model + padded), bf16),
            pltpu.VMEM((nz, n, SLOTS, body), bf16),
            pltpu.VMEM((nz, n, SLOTS, body), bf16),
            pltpu.VMEM((2, nz, expert_rows, model), bf16),
            pltpu.VMEM((expert_rows, model), f32),
            pltpu.VMEM((nz, expert_rows, model), bf16),
            pltpu.VMEM((nz, expert_rows, model), bf16),
            pltpu.VMEM((nz - 1, expert_rows, model), bf16),
            pltpu.VMEM((nz - 1, expert_rows, model), bf16),
            pltpu.VMEM((n, SLOTS, body), bf16),
            pltpu.VMEM((n, SLOTS, body), bf16),
            dma((8,)),
            dma((n,)),
            dma((n,)),
            dma((n,)),
            dma((n,)),
            dma,
            dma,
            dma((2, n_tp)),
            dma,
            dma((nz, 2)),
            dma((nz, 2)),
            dma((nz, 3)),
            dma((nz, 3)),
            dma((nz - 1, 4)),
            dma((nz - 1,)),
            dma((1,)),
            dma((nz,)),
            dma((nz,)),
            dma((nz, n)),
            dma((nz,)),
            dma((nz,)),
            dma((nz,)),
            dma((nz, 2)),
            dma((nz, 2)),
            dma((nz - 1, 2)),
            dma((nz - 1, 2)),
            dma((n,)),
            dma,
        ],
        compiler_params=pltpu.CompilerParams(
            collective_id=0, has_side_effects=True, vmem_limit_bytes=67000000
        ),
        name="layer",
    )(
        query_vectors,
        key_vectors,
        value_vectors,
        cum_gate.T,
        out_weight,
        tokens,
        norm_gain[None, :],
        expert_ids.T,
        route_weights.T,
        jnp.swapaxes(gate_weight[0], 0, 1),
        jnp.swapaxes(up_weight[0], 0, 1),
        down_weight[0],
    )


def solution(mesh):
    in_specs = (
        P(("sp", "tp"), None),
        P("sp", "tp"),
        P("sp", "tp"),
        P("sp", "tp"),
        P("sp", "tp"),
        P("tp", None),
        P(),
        P("sp", None, "tp"),
        P("sp", None, "tp"),
        P("sp", "tp", None),
        P(("sp", "tp"), None),
        P(("sp", "tp"), None),
    )
    out_specs = P(("sp", "tp"), None)
    return jax.shard_map(shards, mesh=mesh, in_specs=in_specs, out_specs=out_specs, check_vma=False)
```

```python
import functools
import math

import jax
import jax.numpy as jnp
from jax import lax
from jax.experimental import pallas as pl
from jax.experimental.pallas import tpu as pltpu
from jax.sharding import PartitionSpec as P

NEG_LARGE = -1e30
MESH = pl.DeviceIdType.MESH
SLOTS = 8


def layer_kernel(
    n,
    n_tp,
    coef,
    capacity,
    q_hbm,
    k_hbm,
    v_hbm,
    gate_ref,
    w_hbm,
    tok_hbm,
    gain_ref,
    ids_ref,
    route_ref,
    wg_hbm,
    wu_hbm,
    wd_hbm,
    out_ref,
    q_ref,
    k_ref,
    v_ref,
    w_ref,
    tok_ref,
    gate,
    up,
    down,
    qraw,
    qbuf,
    kvsend,
    bsend,
    kvbuf,
    bbuf,
    peak,
    total,
    acc,
    obuf,
    rbuf,
    wbuf,
    proj,
    stream_ref,
    place,
    keep,
    keep_tail,
    folds,
    ext,
    packed,
    arrived,
    xbuf,
    pown,
    psend,
    precv,
    rsend,
    rrecv,
    spread,
    back,
    in_sem,
    kv_send,
    kv_recv,
    b_send,
    b_recv,
    q_send,
    q_recv,
    o_send,
    o_recv,
    w_send,
    w_recv,
    d_send,
    d_recv,
    v_send,
    v_recv,
    own_sem,
    x_send,
    x_recv,
    a_send,
    a_recv,
    s_send,
    s_recv,
    p_send,
    p_recv,
    r_send,
    r_recv,
    t_send,
    t_recv,
):
    me = lax.axis_index("sp")
    mt = lax.axis_index("tp")
    nz = n_tp // 2
    z = lax.div(mt, 2)
    core = lax.rem(mt, 2)
    sign = 1 - 2 * core
    nxt = (me, lax.rem(z + sign + nz, nz) * 2 + core)
    partner = (me, z * 2 + 1 - core)
    mirror = n - 1 - me
    head = lax.div(me, n // 2)
    pair = jnp.minimum(me, mirror)
    last = jnp.maximum(me, mirror)
    own_slot = head
    rows, width = q_ref.shape
    half = width // 2
    tok_dev, model = tok_ref.shape
    bf16, f32 = jnp.bfloat16, jnp.float32
    expert_rows = n * capacity
    padded = n * SLOTS

    loads = [
        pltpu.make_async_copy(a, b, in_sem.at[i])
        for i, (a, b) in enumerate(
            (
                (k_hbm, k_ref),
                (v_hbm, v_ref),
                (q_hbm, q_ref),
                (w_hbm, w_ref),
                (tok_hbm, tok_ref),
                (wg_hbm, gate),
                (wu_hbm, up),
                (wd_hbm, down),
            )
        )
    ]
    for load in loads:
        load.start()

    barrier = pltpu.get_barrier_semaphore()

    def greet_plane(k, c):
        pl.semaphore_signal(
            barrier, inc=1, device_id=(lax.rem(me + k, n), mt), device_id_type=MESH
        )
        return c

    def greet_heads(k, c):
        t = lax.rem(mt + k, n_tp)
        pl.semaphore_signal(barrier, inc=1, device_id=(me, t), device_id_type=MESH)
        pl.semaphore_signal(barrier, inc=1, device_id=(mirror, t), device_id_type=MESH)
        return c

    lax.fori_loop(1, n, greet_plane, 0)
    lax.fori_loop(1, n_tp, greet_heads, 0)

    own_w = pltpu.make_async_copy(w_hbm, wbuf.at[mt], own_sem.at[0])
    own_w.start()
    for load in loads[:5]:
        load.wait()
    lane = lax.broadcasted_iota(jnp.int32, (rows, width), 1)
    low = lane < half
    rolled_k = pltpu.roll(k_ref[...].astype(jnp.float32), half, 1)
    values = v_ref[...].astype(jnp.float32)
    kvsend[0] = jnp.where(low, values, rolled_k).astype(jnp.bfloat16)
    kvsend[1] = jnp.where(low, rolled_k, values).astype(jnp.bfloat16)
    bias_rows = gate_ref[...] * (-math.log2(math.e))
    bsend[0] = bias_rows[0:1]
    bsend[1] = bias_rows[1:2]
    mine = low == (head == 1)

    def prepare(raw):
        rolled = pltpu.roll(raw.astype(jnp.float32), half, 1)
        return jnp.where(mine, rolled, 0.0).astype(jnp.bfloat16)

    qbuf[own_slot] = prepare(q_ref[...])
    peak[...] = jnp.full(peak.shape, NEG_LARGE, jnp.float32)
    total[...] = jnp.zeros(total.shape, jnp.float32)
    acc[...] = jnp.zeros(acc.shape, jnp.float32)

    pl.semaphore_wait(barrier, (n - 1) + 2 * (n_tp - 1))

    q_copy = pltpu.make_async_remote_copy(
        src_ref=q_ref,
        dst_ref=qraw,
        send_sem=q_send,
        recv_sem=q_recv,
        device_id=(mirror, mt),
        device_id_type=MESH,
    )
    q_copy.start()

    w_half = w_ref.shape[0] // 2
    w_sub = w_half // 2
    w_quarter = w_half // 4
    side = math.isqrt(n)
    row = lax.div(me, side)
    column = lax.rem(me, side)
    colour = lax.rem(row + column, 2)
    neighbours = (
        row * side + lax.rem(column + 1, side),
        row * side + lax.rem(column + side - 1, side),
        lax.rem(row + 1, side) * side + column,
        lax.rem(row + side - 1, side) * side + column,
    )

    def sub_rows(s):
        return pl.ds(colour * w_half + s * w_sub, w_sub)

    def quarter_rows(i):
        return pl.ds(colour * w_half + i * w_quarter, w_quarter)

    other_rows = pl.ds((1 - colour) * w_half, w_half)

    def w_mine(k):
        return lax.rem(z - sign * (1 + k) + 2 * nz, nz) * 2 + core

    def w_theirs(k):
        return lax.rem(z + sign * (1 + k) + 2 * nz, nz) * 2 + 1 - core

    def w_ring(k, s, src):
        return pltpu.make_async_remote_copy(
            src_ref=src.at[sub_rows(s)],
            dst_ref=wbuf.at[w_mine(k), sub_rows(s)],
            send_sem=w_send.at[k, s],
            recv_sem=w_recv.at[lax.rem(k + 1, nz), s],
            device_id=nxt,
            device_id_type=MESH,
        )

    def w_plane(k, i, target, src):
        return pltpu.make_async_remote_copy(
            src_ref=src.at[quarter_rows(i)],
            dst_ref=wbuf.at[w_mine(k), quarter_rows(i)],
            send_sem=v_send.at[k, i],
            recv_sem=v_recv.at[k],
            device_id=(target, mt),
            device_id_type=MESH,
        )

    def w_share(k, s, src):
        return pltpu.make_async_remote_copy(
            src_ref=src.at[sub_rows(s)],
            dst_ref=wbuf.at[w_mine(k), sub_rows(s)],
            send_sem=d_send.at[k, s],
            recv_sem=d_recv.at[k, s],
            device_id=partner,
            device_id_type=MESH,
        )

    def w_share_rest(k, src):
        return pltpu.make_async_remote_copy(
            src_ref=src.at[other_rows],
            dst_ref=wbuf.at[w_mine(k), other_rows],
            send_sem=d_send.at[k, 2],
            recv_sem=d_recv.at[k, 2],
            device_id=partner,
            device_id_type=MESH,
        )

    for s in range(2):
        w_ring(nz - 1, s, w_ref).start()

    def kv_copy(r):
        hr = lax.div(r, n // 2)
        return (
            pltpu.make_async_remote_copy(
                src_ref=kvsend.at[hr],
                dst_ref=kvbuf.at[me],
                send_sem=kv_send.at[r],
                recv_sem=kv_recv.at[me],
                device_id=(r, mt),
                device_id_type=MESH,
            ),
            pltpu.make_async_remote_copy(
                src_ref=bsend.at[hr],
                dst_ref=bbuf.at[me],
                send_sem=b_send.at[r],
                recv_sem=b_recv.at[me],
                device_id=(r, mt),
                device_id_type=MESH,
            ),
        )

    def send_body(k, c):
        r = lax.rem(me + k, n)

        @pl.when(me <= jnp.maximum(r, n - 1 - r))
        def _():
            ck, cb = kv_copy(r)
            cb.start()
            ck.start()

        return c

    lax.fori_loop(1, n, send_body, 0)
    for s in range(2):
        w_share(nz - 1, s, w_ref).start()
    w_share_rest(nz - 1, w_ref).start()

    sub = min(256, rows)

    def tile(slot, kv_at, bias_at, diagonal):
        for i in range(rows // sub):
            kv = kv_at[...]
            rs = pl.ds(i * sub, sub)
            s = lax.dot_general(
                qbuf[slot, rs, :], kv, (((1,), (1,)), ((), ())), preferred_element_type=jnp.float32
            )
            s = s * coef + bias_at[...]
            if diagonal:
                qp = lax.broadcasted_iota(jnp.int32, s.shape, 0) + i * sub
                kp = lax.broadcasted_iota(jnp.int32, s.shape, 1)
                s = jnp.where(kp <= qp, s, NEG_LARGE)
            old = peak[slot, rs, :]
            new = jnp.maximum(old, jnp.max(s, axis=1, keepdims=True))
            e = jnp.exp2(s - new)
            alpha = jnp.exp2(old - new)
            total[slot, rs, :] = total[slot, rs, :] * alpha + jnp.sum(e, axis=1, keepdims=True)
            acc[slot, rs, :] = acc[slot, rs, :] * alpha + jnp.dot(
                e.astype(jnp.bfloat16), kv, preferred_element_type=jnp.float32
            )
            peak[slot, rs, :] = new

    tile(own_slot, kvsend.at[head], bsend.at[head], True)
    pltpu.make_async_copy(q_ref, qraw, q_recv).wait()
    qbuf[1 - own_slot] = prepare(qraw[...])

    @pl.when(me < last)
    def _():
        tile(1, kvsend.at[head], bsend.at[head], False)

    def w_event(i):
        k = lax.div(i, 2)
        s = lax.rem(i, 2)
        block = wbuf.at[w_mine(k)]
        pltpu.make_async_copy(
            w_ref.at[pl.ds(0, w_sub)], block.at[sub_rows(s)], w_recv.at[k, s]
        ).wait()

        @pl.when(k < nz - 2)
        def _():
            w_ring(k, s, block).start()

        for j in range(2):
            target = jnp.where(s == 0, neighbours[j], neighbours[2 + j])
            w_plane(k, 2 * s + j, target, block).start()
        w_share(k, s, block).start()

    def w_rest(k, c):
        block = wbuf.at[w_mine(k)]
        pltpu.make_async_copy(
            w_ref.at[pl.ds(0, w_half)], block.at[other_rows], v_recv.at[k]
        ).wait()
        w_share_rest(k, block).start()
        return c

    def w_partner(k, t):
        for s in range(2):
            pltpu.make_async_copy(
                w_ref.at[pl.ds(0, w_sub)], wbuf.at[t, sub_rows(s)], d_recv.at[k, s]
            ).wait()
        pltpu.make_async_copy(
            w_ref.at[pl.ds(0, w_half)], wbuf.at[t, other_rows], d_recv.at[k, 2]
        ).wait()

    events = 2 * (nz - 1)
    early = max(0, min(events, n - 2))

    def compute_body(k, c):
        j = lax.rem(me - k + n, n)

        @pl.when(jnp.logical_and(k >= 2, k - 2 < early))
        def _():
            w_event(k - 2)

        @pl.when(j <= last)
        def _():
            pltpu.make_async_copy(kvsend.at[0], kvbuf.at[j], kv_recv.at[j]).wait()
            pltpu.make_async_copy(bsend.at[0], bbuf.at[j], b_recv.at[j]).wait()

            def slot_body(slot, c):
                end = jnp.where(slot == 0, pair, last)

                @pl.when(j == end)
                def _():
                    tile(slot, kvbuf.at[j], bbuf.at[j], True)

                @pl.when(j < end)
                def _():
                    tile(slot, kvbuf.at[j], bbuf.at[j], False)

                return c

            lax.fori_loop(0, 2, slot_body, 0)

        return c

    lax.fori_loop(1, n, compute_body, 0)

    for slot in range(2):
        obuf[slot] = (acc[slot] / total[slot]).astype(jnp.bfloat16)

    def o_target(slot):
        return jnp.where(slot == 0, pair, last)

    def o_copy(slot, t):
        return pltpu.make_async_remote_copy(
            src_ref=obuf.at[slot, pl.ds(t * tok_dev, tok_dev)],
            dst_ref=rbuf.at[mt, head],
            send_sem=o_send.at[slot, t],
            recv_sem=o_recv,
            device_id=(o_target(slot), t),
            device_id_type=MESH,
        )

    def o_self(slot, t):
        return jnp.logical_and(o_target(slot) == me, t == mt)

    def o_body(k, c):
        slot = lax.rem(k, 2)
        t = lax.rem(mt + n_tp // 2 + lax.div(k, 2), n_tp)

        @pl.when(jnp.logical_not(o_self(slot, t)))
        def _():
            o_copy(slot, t).start()

        @pl.when(o_self(slot, t))
        def _():
            pltpu.make_async_copy(
                obuf.at[slot, pl.ds(t * tok_dev, tok_dev)], rbuf.at[mt, head], o_recv
            ).start()

        return c

    lax.fori_loop(0, 2 * n_tp, o_body, 0)

    def late_event(i, c):
        w_event(i)
        return c

    lax.fori_loop(early, events, late_event, 0)
    lax.fori_loop(0, nz - 1, w_rest, 0)

    number = lax.broadcasted_iota(jnp.int32, (n, tok_dev), 0)
    before = (
        lax.broadcasted_iota(jnp.int32, (tok_dev, tok_dev), 0)
        < lax.broadcasted_iota(jnp.int32, (tok_dev, tok_dev), 1)
    ).astype(bf16)
    expand = (
        lax.div(lax.broadcasted_iota(jnp.int32, (padded, n), 0), SLOTS)
        == lax.broadcasted_iota(jnp.int32, (padded, n), 1)
    ).astype(bf16)
    inside = lax.rem(lax.broadcasted_iota(jnp.int32, (padded, tok_dev), 0), SLOTS).astype(f32)
    eye = (
        lax.broadcasted_iota(jnp.int32, (padded, padded), 0)
        == lax.broadcasted_iota(jnp.int32, (padded, padded), 1)
    ).astype(bf16)
    first = (((0,), (0,)), ((), ()))
    taken = jnp.zeros((n, 1), f32)
    for r in range(ids_ref.shape[0]):
        named = (number == ids_ref[r : r + 1, :]).astype(f32)
        rank = jnp.dot(named.astype(bf16), before, preferred_element_type=f32) + taken
        taken = taken + jnp.sum(named, axis=1, keepdims=True)
        named_at = jnp.dot(expand, named.astype(bf16), preferred_element_type=f32)
        rank_at = jnp.dot(expand, rank.astype(bf16), preferred_element_type=f32)
        placed = jnp.where(rank_at == inside, named_at, 0.0).astype(bf16)
        place[r] = lax.dot_general(placed, eye, first, preferred_element_type=f32).astype(bf16)
    compact = lax.broadcasted_iota(jnp.int32, (expert_rows, padded), 0)
    spaced = lax.broadcasted_iota(jnp.int32, (expert_rows, padded), 1)
    keep[...] = (
        lax.div(compact, capacity) * SLOTS + lax.rem(compact, capacity) == spaced
    ).astype(bf16)
    spare = SLOTS - capacity
    each = capacity // spare
    third = lax.broadcasted_iota(jnp.int32, (expert_rows, each * padded), 1)
    kept = lax.broadcasted_iota(jnp.int32, (expert_rows, each * padded), 0)
    kept_in = lax.rem(kept, capacity)
    keep_tail[...] = jnp.logical_and(
        lax.rem(third, padded)
        == lax.div(kept, capacity) * SLOTS + capacity + lax.div(kept_in, each),
        lax.div(third, padded) == lax.rem(kept_in, each),
    ).astype(bf16)
    slot = lax.broadcasted_iota(jnp.int32, (padded, each * padded), 0)
    target = lax.broadcasted_iota(jnp.int32, (padded, each * padded), 1)
    target_row = lax.rem(target, padded)
    target_in = lax.rem(target_row, SLOTS)
    folds[...] = jnp.logical_and(
        target_in >= capacity,
        slot
        == lax.div(target_row, SLOTS) * SLOTS
        + (target_in - capacity) * each
        + lax.div(target, padded),
    ).astype(bf16)
    sent_to = place[0]
    for r in range(1, ids_ref.shape[0]):
        sent_to = sent_to + place[r]
    ext[nz - 1, :, model:] = sent_to

    pltpu.make_async_copy(rbuf, rbuf, o_recv).wait()
    own_w.wait()
    w_partner(nz - 1, z * 2 + 1 - core)
    low32 = lax.broadcasted_iota(jnp.int32, (tok_dev, width), 1) < half

    def product(t):
        piece = jnp.where(
            low32, rbuf[t, 0].astype(jnp.float32), rbuf[t, 1].astype(jnp.float32)
        ).astype(jnp.bfloat16)
        return jnp.dot(piece, wbuf[t], preferred_element_type=jnp.float32)

    proj[...] = product(mt)
    proj[...] += product(z * 2 + 1 - core)

    def project(k, c):
        w_partner(k, w_theirs(k))
        proj[...] += product(w_mine(k))
        proj[...] += product(w_theirs(k))
        return c

    lax.fori_loop(0, nz - 1, project, 0)
    stream = (tok_ref[...].astype(f32) + proj[...]).astype(bf16)
    stream_ref[...] = stream
    stream_wide = stream.astype(f32)
    inverse = lax.rsqrt(jnp.mean(stream_wide * stream_wide, axis=1, keepdims=True) + 1e-05)
    ext[nz - 1, :, :model] = (stream_wide * inverse * gain_ref[...]).astype(bf16)

    def ring(k):
        return pltpu.make_async_remote_copy(
            src_ref=ext.at[k],
            dst_ref=ext.at[lax.rem(k + 1, nz)],
            send_sem=x_send.at[k],
            recv_sem=x_recv.at[lax.rem(k + 1, nz)],
            device_id=nxt,
            device_id_type=MESH,
        )

    def to_expert(k, e):
        return pltpu.make_async_remote_copy(
            src_ref=packed.at[k, e],
            dst_ref=arrived.at[k, me],
            send_sem=a_send.at[k, e],
            recv_sem=a_recv.at[k],
            device_id=(e, mt),
            device_id_type=MESH,
        )

    def share(k):
        return pltpu.make_async_remote_copy(
            src_ref=xbuf.at[core, k],
            dst_ref=xbuf.at[core, k],
            send_sem=s_send.at[k],
            recv_sem=s_recv.at[k],
            device_id=partner,
            device_id_type=MESH,
        )

    parts = 2
    part_rows = expert_rows // parts

    def part(s):
        return pl.ds(s * part_rows, part_rows)

    def give(k, s):
        return pltpu.make_async_remote_copy(
            src_ref=psend.at[k, part(s)],
            dst_ref=precv.at[k, part(s)],
            send_sem=p_send.at[k, s],
            recv_sem=p_recv.at[k, s],
            device_id=partner,
            device_id_type=MESH,
        )

    def reduce(k, s):
        return pltpu.make_async_remote_copy(
            src_ref=rsend.at[k, part(s)],
            dst_ref=rrecv.at[k, part(s)],
            send_sem=r_send.at[k, s],
            recv_sem=r_recv.at[k, s],
            device_id=nxt,
            device_id_type=MESH,
        )

    def to_token(s):
        return pltpu.make_async_remote_copy(
            src_ref=spread.at[s],
            dst_ref=back.at[me],
            send_sem=t_send.at[s],
            recv_sem=t_recv,
            device_id=(s, mt),
            device_id_type=MESH,
        )

    body = model * capacity // SLOTS
    fold = body // each

    def unfolded(flat):
        return jnp.concatenate([flat[:, j * fold : (j + 1) * fold] for j in range(each)], axis=0)

    def dispatch(k):
        @pl.when(k < nz - 1)
        def _():
            pltpu.make_async_copy(ext.at[0], ext.at[k], x_recv.at[k]).wait()

        @pl.when(k != nz - 2)
        def _():
            ring(k).start()

        main = ext[k, :, model:]
        tails = jnp.dot(main, folds[...], preferred_element_type=f32).astype(bf16)
        last_columns = ext[k, :, body:model]
        for j in range(each):
            cols = slice(j * fold, (j + 1) * fold)
            block = lax.dot_general(
                jnp.concatenate([main, tails[:, j * padded : (j + 1) * padded]], axis=0),
                jnp.concatenate([ext[k, :, cols], last_columns], axis=0),
                first,
                preferred_element_type=f32,
            ).astype(bf16)
            for e in range(n):
                packed[k, e, :, cols] = block[e * SLOTS : (e + 1) * SLOTS]
        pltpu.make_async_copy(packed.at[k, me], arrived.at[k, me], a_recv.at[k]).start()

        def send(i, c):
            to_expert(k, lax.rem(me + i, n)).start()
            return c

        lax.fori_loop(1, n, send, 0)

    def first_dispatch(i, c):
        dispatch(lax.rem(i + nz - 1, nz))
        return c

    ahead = min(3, nz - 1)
    lax.fori_loop(0, ahead + 1, first_dispatch, 0)
    for load in loads[5:]:
        load.wait()

    col_tile = min(512, model)
    across = (((1,), (1,)), ((), ()))

    def gather(k):
        pltpu.make_async_copy(arrived.at[k], arrived.at[k], a_recv.at[k]).wait()
        flat = arrived[k].reshape(padded, body)
        xbuf[core, k, :, :body] = jnp.dot(
            keep[...], flat, preferred_element_type=f32
        ).astype(bf16)
        xbuf[core, k, :, body:] = jnp.dot(
            keep_tail[...], unfolded(flat), preferred_element_type=f32
        ).astype(bf16)
        share(k).start()

    gather(0)

    def step(k, c):
        pltpu.make_async_copy(xbuf.at[1 - core, 0], xbuf.at[1 - core, k], s_recv.at[k]).wait()

        x = jnp.concatenate([xbuf[1 - core, k], xbuf[core, k]], axis=0)
        g = lax.dot_general(x, gate[...], across, preferred_element_type=f32)
        u = lax.dot_general(x, up[...], across, preferred_element_type=f32)
        hidden = (g / (1.0 + jnp.exp(-g)) * u).astype(bf16)
        for i in range(model // col_tile):
            cols = slice(i * col_tile, (i + 1) * col_tile)
            p = jnp.dot(hidden, down[:, cols], preferred_element_type=f32)
            psend[k, :, cols] = p[:expert_rows].astype(bf16)
            pown[:, cols] = p[expert_rows:]
        for s in range(parts):
            give(k, s).start()

        @pl.when(k + ahead < nz - 1)
        def _():
            dispatch(k + ahead)

        @pl.when(k < nz - 1)
        def _():
            gather(k + 1)

        for s in range(parts):
            give(k, s).wait_recv()
            both = pown[part(s), :] + precv[k, part(s), :].astype(f32)

            @pl.when(k > 0)
            def _():
                kk = jnp.maximum(k - 1, 0)
                reduce(kk, s).wait_recv()
                pown[part(s), :] = both + rrecv[kk, part(s), :].astype(f32)

            @pl.when(k == 0)
            def _():
                pown[part(s), :] = both

            @pl.when(k < nz - 1)
            def _():
                rsend[k, part(s), :] = pown[part(s), :].astype(bf16)
                reduce(k, s).start()

        return c

    lax.fori_loop(0, nz, step, 0)

    for j in range(each):
        cols = slice(j * fold, (j + 1) * fold)
        scattered = lax.dot_general(
            jnp.concatenate([keep[...], keep_tail[:, j * padded : (j + 1) * padded]], axis=0),
            jnp.concatenate([pown[:, cols], pown[:, body:]], axis=0).astype(bf16),
            first,
            preferred_element_type=f32,
        ).astype(bf16)
        for s in range(n):
            spread[s, :, cols] = scattered[s * SLOTS : (s + 1) * SLOTS]
    pltpu.make_async_copy(spread.at[me], back.at[me], t_recv).start()

    def return_body(k, c):
        to_token(lax.rem(me + k, n)).start()
        return c

    lax.fori_loop(1, n, return_body, 0)

    q_copy.wait_send()

    def drain_body(k, c):
        r = lax.rem(me + k, n)

        @pl.when(me <= jnp.maximum(r, n - 1 - r))
        def _():
            ck, cb = kv_copy(r)
            cb.wait_send()
            ck.wait_send()

        return c

    lax.fori_loop(1, n, drain_body, 0)

    def o_drain(k, c):
        slot = lax.rem(k, 2)
        t = lax.div(k, 2)

        @pl.when(jnp.logical_not(o_self(slot, t)))
        def _():
            o_copy(slot, t).wait_send()

        return c

    lax.fori_loop(0, 2 * n_tp, o_drain, 0)

    def w_drain(k, c):
        for s in range(2):
            w_share(k, s, w_ref).wait_send()

            @pl.when(k != nz - 2)
            def _():
                w_ring(k, s, w_ref).wait_send()

        w_share_rest(k, w_ref).wait_send()

        @pl.when(k < nz - 1)
        def _():
            for i in range(4):
                w_plane(k, i, neighbours[i], w_ref).wait_send()

        return c

    lax.fori_loop(0, nz, w_drain, 0)

    def drain(k, c):
        for s in range(parts):
            give(k, s).wait_send()

            @pl.when(k < nz - 1)
            def _():
                reduce(k, s).wait_send()

        @pl.when(k != nz - 2)
        def _():
            ring(k).wait_send()

        share(k).wait_send()

        def drain_send(i, c):
            to_expert(k, lax.rem(me + i, n)).wait_send()
            return c

        lax.fori_loop(1, n, drain_send, 0)
        return c

    lax.fori_loop(0, nz, drain, 0)

    pltpu.make_async_copy(back, back, t_recv).wait()
    rows_back = back[...].reshape(padded, body)
    tails_back = unfolded(rows_back)
    diagonal = lax.broadcasted_iota(jnp.int32, (tok_dev, tok_dev), 0) == lax.broadcasted_iota(
        jnp.int32, (tok_dev, tok_dev), 1
    )
    mixture = jnp.zeros((tok_dev, body), f32)
    mixture_tail = jnp.zeros((tok_dev, model - body), f32)
    for r in range(ids_ref.shape[0]):
        chosen = place[r]
        tails = jnp.dot(chosen, folds[...], preferred_element_type=f32).astype(bf16)
        weight = jnp.sum(
            jnp.where(diagonal, route_ref[r : r + 1, :], 0.0), axis=1, keepdims=True
        )
        mixture += weight * jnp.dot(chosen, rows_back, preferred_element_type=f32)
        mixture_tail += weight * jnp.dot(tails, tails_back, preferred_element_type=f32)
    out_ref[:, :body] = (stream_ref[:, :body].astype(f32) + mixture).astype(bf16)
    out_ref[:, body:] = (stream_ref[:, body:].astype(f32) + mixture_tail).astype(bf16)

    def drain_back(k, c):
        to_token(lax.rem(me + k, n)).wait_send()
        return c

    lax.fori_loop(1, n, drain_back, 0)


def shards(
    tokens,
    query_vectors,
    key_vectors,
    value_vectors,
    cum_gate,
    out_weight,
    norm_gain,
    gate_weight,
    up_weight,
    down_weight,
    expert_ids,
    route_weights,
):
    n = lax.axis_size("sp")
    n_tp = lax.axis_size("tp")
    nz = n_tp // 2
    rows, width = query_vectors.shape
    tok_dev, model = tokens.shape
    top = expert_ids.shape[1]
    inner = gate_weight.shape[2]
    capacity = max(2, 3 * tok_dev * top // (2 * n))
    assert capacity < SLOTS and capacity % (SLOTS - capacity) == 0 and gate_weight.shape[0] == 1
    each = capacity // (SLOTS - capacity)
    body = model * capacity // SLOTS
    expert_rows = n * capacity
    padded = n * SLOTS
    coef = (width // 2) ** (-0.5) * math.log2(math.e)
    vmem = pl.BlockSpec(memory_space=pltpu.VMEM)
    hbm = pl.BlockSpec(memory_space=pl.ANY)
    bf16, f32 = jnp.bfloat16, jnp.float32
    dma = pltpu.SemaphoreType.DMA
    return pl.pallas_call(
        functools.partial(layer_kernel, n, n_tp, coef, capacity),
        out_shape=jax.ShapeDtypeStruct((tok_dev, model), bf16),
        in_specs=[hbm, hbm, hbm, vmem, hbm, hbm, vmem, vmem, vmem, hbm, hbm, hbm],
        out_specs=vmem,
        scratch_shapes=[
            pltpu.VMEM((rows, width), bf16),
            pltpu.VMEM((rows, width), bf16),
            pltpu.VMEM((rows, width), bf16),
            pltpu.VMEM((width, model), bf16),
            pltpu.VMEM((tok_dev, model), bf16),
            pltpu.VMEM((inner, model), bf16),
            pltpu.VMEM((inner, model), bf16),
            pltpu.VMEM((inner, model), bf16),
            pltpu.VMEM((rows, width), bf16),
            pltpu.VMEM((2, rows, width), bf16),
            pltpu.VMEM((2, rows, width), bf16),
            pltpu.VMEM((2, 1, rows), f32),
            pltpu.VMEM((n, rows, width), bf16),
            pltpu.VMEM((n, 1, rows), f32),
            pltpu.VMEM((2, rows, 1), f32),
            pltpu.VMEM((2, rows, 1), f32),
            pltpu.VMEM((2, rows, width), f32),
            pltpu.VMEM((2, rows, width), bf16),
            pltpu.VMEM((n_tp, 2, tok_dev, width), bf16),
            pltpu.VMEM((n_tp, width, model), bf16),
            pltpu.VMEM((tok_dev, model), f32),
            pltpu.VMEM((tok_dev, model), bf16),
            pltpu.VMEM((top, tok_dev, padded), bf16),
            pltpu.VMEM((expert_rows, padded), bf16),
            pltpu.VMEM((expert_rows, each * padded), bf16),
            pltpu.VMEM((padded, each * padded), bf16),
            pltpu.VMEM((nz, tok_dev, model + padded), bf16),
            pltpu.VMEM((nz, n, SLOTS, body), bf16),
            pltpu.VMEM((nz, n, SLOTS, body), bf16),
            pltpu.VMEM((2, nz, expert_rows, model), bf16),
            pltpu.VMEM((expert_rows, model), f32),
            pltpu.VMEM((nz, expert_rows, model), bf16),
            pltpu.VMEM((nz, expert_rows, model), bf16),
            pltpu.VMEM((nz - 1, expert_rows, model), bf16),
            pltpu.VMEM((nz - 1, expert_rows, model), bf16),
            pltpu.VMEM((n, SLOTS, body), bf16),
            pltpu.VMEM((n, SLOTS, body), bf16),
            dma((8,)),
            dma((n,)),
            dma((n,)),
            dma((n,)),
            dma((n,)),
            dma,
            dma,
            dma((2, n_tp)),
            dma,
            dma((nz, 2)),
            dma((nz, 2)),
            dma((nz, 3)),
            dma((nz, 3)),
            dma((nz - 1, 4)),
            dma((nz - 1,)),
            dma((1,)),
            dma((nz,)),
            dma((nz,)),
            dma((nz, n)),
            dma((nz,)),
            dma((nz,)),
            dma((nz,)),
            dma((nz, 2)),
            dma((nz, 2)),
            dma((nz - 1, 2)),
            dma((nz - 1, 2)),
            dma((n,)),
            dma,
        ],
        compiler_params=pltpu.CompilerParams(
            collective_id=0, has_side_effects=True, vmem_limit_bytes=67000000
        ),
        name="layer",
    )(
        query_vectors,
        key_vectors,
        value_vectors,
        cum_gate.T,
        out_weight,
        tokens,
        norm_gain[None, :],
        expert_ids.T,
        route_weights.T,
        jnp.swapaxes(gate_weight[0], 0, 1),
        jnp.swapaxes(up_weight[0], 0, 1),
        down_weight[0],
    )


def solution(mesh):
    in_specs = (
        P(("sp", "tp"), None),
        P("sp", "tp"),
        P("sp", "tp"),
        P("sp", "tp"),
        P("sp", "tp"),
        P("tp", None),
        P(),
        P("sp", None, "tp"),
        P("sp", None, "tp"),
        P("sp", "tp", None),
        P(("sp", "tp"), None),
        P(("sp", "tp"), None),
    )
    out_specs = P(("sp", "tp"), None)
    return jax.shard_map(shards, mesh=mesh, in_specs=in_specs, out_specs=out_specs, check_vma=False)
```

```python
import functools
import math

import jax
import jax.numpy as jnp
from jax import lax
from jax.experimental import pallas as pl
from jax.experimental.pallas import tpu as pltpu
from jax.sharding import PartitionSpec as P

NEG_LARGE = -1e30
MESH = pl.DeviceIdType.MESH
SLOTS = 8


def layer_kernel(
    n,
    n_tp,
    coef,
    capacity,
    q_hbm,
    k_hbm,
    v_hbm,
    gate_ref,
    w_hbm,
    tok_hbm,
    gain_ref,
    ids_ref,
    route_ref,
    wg_hbm,
    wu_hbm,
    wd_hbm,
    out_ref,
    q_ref,
    k_ref,
    v_ref,
    w_ref,
    tok_ref,
    gate,
    up,
    down,
    qraw,
    qbuf,
    kvsend,
    bsend,
    kvbuf,
    bbuf,
    peak,
    total,
    acc,
    obuf,
    rbuf,
    wbuf,
    attended,
    proj,
    stream_ref,
    place,
    keep,
    keep_tail,
    folds,
    ext,
    packed,
    arrived,
    xbuf,
    pown,
    psend,
    precv,
    rsend,
    rrecv,
    spread,
    back,
    in_sem,
    kv_send,
    kv_recv,
    b_send,
    b_recv,
    q_send,
    q_recv,
    o_send,
    o_recv,
    w_send,
    w_recv,
    d_send,
    d_recv,
    v_send,
    v_recv,
    own_sem,
    x_send,
    x_recv,
    a_send,
    a_recv,
    s_send,
    s_recv,
    p_send,
    p_recv,
    r_send,
    r_recv,
    t_send,
    t_recv,
):
    me = lax.axis_index("sp")
    mt = lax.axis_index("tp")
    nz = n_tp // 2
    z = lax.div(mt, 2)
    core = lax.rem(mt, 2)
    sign = 1 - 2 * core
    nxt = (me, lax.rem(z + sign + nz, nz) * 2 + core)
    partner = (me, z * 2 + 1 - core)
    mirror = n - 1 - me
    head = lax.div(me, n // 2)
    pair = jnp.minimum(me, mirror)
    last = jnp.maximum(me, mirror)
    own_slot = head
    rows, width = q_ref.shape
    half = width // 2
    tok_dev, model = tok_ref.shape
    bf16, f32 = jnp.bfloat16, jnp.float32
    expert_rows = n * capacity
    padded = n * SLOTS

    loads = [
        pltpu.make_async_copy(a, b, in_sem.at[i])
        for i, (a, b) in enumerate(
            (
                (k_hbm, k_ref),
                (v_hbm, v_ref),
                (q_hbm, q_ref),
                (w_hbm, w_ref),
                (tok_hbm, tok_ref),
                (wg_hbm, gate),
                (wu_hbm, up),
                (wd_hbm, down),
            )
        )
    ]
    for load in loads:
        load.start()

    barrier = pltpu.get_barrier_semaphore()

    def greet_plane(k, c):
        pl.semaphore_signal(
            barrier, inc=1, device_id=(lax.rem(me + k, n), mt), device_id_type=MESH
        )
        return c

    def greet_heads(k, c):
        t = lax.rem(mt + k, n_tp)
        pl.semaphore_signal(barrier, inc=1, device_id=(me, t), device_id_type=MESH)
        pl.semaphore_signal(barrier, inc=1, device_id=(mirror, t), device_id_type=MESH)
        return c

    lax.fori_loop(1, n, greet_plane, 0)
    lax.fori_loop(1, n_tp, greet_heads, 0)

    own_w = pltpu.make_async_copy(w_hbm, wbuf.at[mt], own_sem.at[0])
    own_w.start()
    for load in loads[:5]:
        load.wait()
    lane = lax.broadcasted_iota(jnp.int32, (rows, width), 1)
    low = lane < half
    rolled_k = pltpu.roll(k_ref[...].astype(jnp.float32), half, 1)
    values = v_ref[...].astype(jnp.float32)
    kvsend[0] = jnp.where(low, values, rolled_k).astype(jnp.bfloat16)
    kvsend[1] = jnp.where(low, rolled_k, values).astype(jnp.bfloat16)
    bias_rows = gate_ref[...] * (-math.log2(math.e))
    bsend[0] = bias_rows[0:1]
    bsend[1] = bias_rows[1:2]
    mine = low == (head == 1)

    def prepare(raw):
        rolled = pltpu.roll(raw.astype(jnp.float32), half, 1)
        return jnp.where(mine, rolled, 0.0).astype(jnp.bfloat16)

    qbuf[own_slot] = prepare(q_ref[...])
    peak[...] = jnp.full(peak.shape, NEG_LARGE, jnp.float32)
    total[...] = jnp.zeros(total.shape, jnp.float32)
    acc[...] = jnp.zeros(acc.shape, jnp.float32)

    pl.semaphore_wait(barrier, (n - 1) + 2 * (n_tp - 1))

    q_copy = pltpu.make_async_remote_copy(
        src_ref=q_ref,
        dst_ref=qraw,
        send_sem=q_send,
        recv_sem=q_recv,
        device_id=(mirror, mt),
        device_id_type=MESH,
    )
    q_copy.start()

    w_half = w_ref.shape[0] // 2
    w_sub = w_half // 2
    w_quarter = w_half // 4
    side = math.isqrt(n)
    row = lax.div(me, side)
    column = lax.rem(me, side)
    colour = lax.rem(row + column, 2)
    neighbours = (
        row * side + lax.rem(column + 1, side),
        row * side + lax.rem(column + side - 1, side),
        lax.rem(row + 1, side) * side + column,
        lax.rem(row + side - 1, side) * side + column,
    )

    def sub_rows(s):
        return pl.ds(colour * w_half + s * w_sub, w_sub)

    def quarter_rows(i):
        return pl.ds(colour * w_half + i * w_quarter, w_quarter)

    other_rows = pl.ds((1 - colour) * w_half, w_half)

    def w_mine(k):
        return lax.rem(z - sign * (1 + k) + 2 * nz, nz) * 2 + core

    def w_theirs(k):
        return lax.rem(z + sign * (1 + k) + 2 * nz, nz) * 2 + 1 - core

    def w_ring(k, s, src):
        return pltpu.make_async_remote_copy(
            src_ref=src.at[sub_rows(s)],
            dst_ref=wbuf.at[w_mine(k), sub_rows(s)],
            send_sem=w_send.at[k, s],
            recv_sem=w_recv.at[lax.rem(k + 1, nz), s],
            device_id=nxt,
            device_id_type=MESH,
        )

    def w_plane(k, i, target, src):
        return pltpu.make_async_remote_copy(
            src_ref=src.at[quarter_rows(i)],
            dst_ref=wbuf.at[w_mine(k), quarter_rows(i)],
            send_sem=v_send.at[k, i],
            recv_sem=v_recv.at[k],
            device_id=(target, mt),
            device_id_type=MESH,
        )

    def w_share(k, s, src):
        return pltpu.make_async_remote_copy(
            src_ref=src.at[sub_rows(s)],
            dst_ref=wbuf.at[w_mine(k), sub_rows(s)],
            send_sem=d_send.at[k, s],
            recv_sem=d_recv.at[k, s],
            device_id=partner,
            device_id_type=MESH,
        )

    def w_share_rest(k, src):
        return pltpu.make_async_remote_copy(
            src_ref=src.at[other_rows],
            dst_ref=wbuf.at[w_mine(k), other_rows],
            send_sem=d_send.at[k, 2],
            recv_sem=d_recv.at[k, 2],
            device_id=partner,
            device_id_type=MESH,
        )

    for s in range(2):
        w_ring(nz - 1, s, w_ref).start()

    def kv_copy(r):
        hr = lax.div(r, n // 2)
        return (
            pltpu.make_async_remote_copy(
                src_ref=kvsend.at[hr],
                dst_ref=kvbuf.at[me],
                send_sem=kv_send.at[r],
                recv_sem=kv_recv.at[me],
                device_id=(r, mt),
                device_id_type=MESH,
            ),
            pltpu.make_async_remote_copy(
                src_ref=bsend.at[hr],
                dst_ref=bbuf.at[me],
                send_sem=b_send.at[r],
                recv_sem=b_recv.at[me],
                device_id=(r, mt),
                device_id_type=MESH,
            ),
        )

    def send_body(k, c):
        r = lax.rem(me + k, n)

        @pl.when(me <= jnp.maximum(r, n - 1 - r))
        def _():
            ck, cb = kv_copy(r)
            cb.start()
            ck.start()

        return c

    lax.fori_loop(1, n, send_body, 0)
    for s in range(2):
        w_share(nz - 1, s, w_ref).start()
    w_share_rest(nz - 1, w_ref).start()

    sub = min(256, rows)

    def tile(slot, kv_at, bias_at, diagonal):
        for i in range(rows // sub):
            kv = kv_at[...]
            rs = pl.ds(i * sub, sub)
            s = lax.dot_general(
                qbuf[slot, rs, :], kv, (((1,), (1,)), ((), ())), preferred_element_type=jnp.float32
            )
            s = s * coef + bias_at[...]
            if diagonal:
                qp = lax.broadcasted_iota(jnp.int32, s.shape, 0) + i * sub
                kp = lax.broadcasted_iota(jnp.int32, s.shape, 1)
                s = jnp.where(kp <= qp, s, NEG_LARGE)
            old = peak[slot, rs, :]
            new = jnp.maximum(old, jnp.max(s, axis=1, keepdims=True))
            e = jnp.exp2(s - new)
            alpha = jnp.exp2(old - new)
            total[slot, rs, :] = total[slot, rs, :] * alpha + jnp.sum(e, axis=1, keepdims=True)
            acc[slot, rs, :] = acc[slot, rs, :] * alpha + jnp.dot(
                e.astype(jnp.bfloat16), kv, preferred_element_type=jnp.float32
            )
            peak[slot, rs, :] = new

    tile(own_slot, kvsend.at[head], bsend.at[head], True)
    pltpu.make_async_copy(q_ref, qraw, q_recv).wait()
    qbuf[1 - own_slot] = prepare(qraw[...])

    @pl.when(me < last)
    def _():
        tile(1, kvsend.at[head], bsend.at[head], False)

    def w_event(i):
        k = lax.div(i, 2)
        s = lax.rem(i, 2)
        block = wbuf.at[w_mine(k)]
        pltpu.make_async_copy(
            w_ref.at[pl.ds(0, w_sub)], block.at[sub_rows(s)], w_recv.at[k, s]
        ).wait()

        @pl.when(k < nz - 2)
        def _():
            w_ring(k, s, block).start()

        w_share(k, s, block).start()

    def w_pass(i, c):
        k = lax.div(i, 2)
        s = lax.rem(i, 2)
        for j in range(2):
            target = jnp.where(s == 0, neighbours[j], neighbours[2 + j])
            w_plane(k, 2 * s + j, target, wbuf.at[w_mine(k)]).start()
        return c

    def w_rest(k, c):
        block = wbuf.at[w_mine(k)]
        pltpu.make_async_copy(
            w_ref.at[pl.ds(0, w_half)], block.at[other_rows], v_recv.at[k]
        ).wait()
        w_share_rest(k, block).start()
        return c

    def w_partner(k, t):
        for s in range(2):
            pltpu.make_async_copy(
                w_ref.at[pl.ds(0, w_sub)], wbuf.at[t, sub_rows(s)], d_recv.at[k, s]
            ).wait()
        pltpu.make_async_copy(
            w_ref.at[pl.ds(0, w_half)], wbuf.at[t, other_rows], d_recv.at[k, 2]
        ).wait()

    events = 2 * (nz - 1)
    early = max(0, min(events, n - 1))
    passed = early

    def compute_body(k, c):
        j = lax.rem(me - k + n, n)

        @pl.when(k - 1 < early)
        def _():
            w_event(k - 1)

        @pl.when(k - 1 < early)
        def _():
            w_pass(k - 1, 0)

        @pl.when(j <= last)
        def _():
            pltpu.make_async_copy(kvsend.at[0], kvbuf.at[j], kv_recv.at[j]).wait()
            pltpu.make_async_copy(bsend.at[0], bbuf.at[j], b_recv.at[j]).wait()

            def slot_body(slot, c):
                end = jnp.where(slot == 0, pair, last)

                @pl.when(j == end)
                def _():
                    tile(slot, kvbuf.at[j], bbuf.at[j], True)

                @pl.when(j < end)
                def _():
                    tile(slot, kvbuf.at[j], bbuf.at[j], False)

                return c

            lax.fori_loop(0, 2, slot_body, 0)

        return c

    lax.fori_loop(1, n, compute_body, 0)

    for slot in range(2):
        obuf[slot] = (acc[slot] / total[slot]).astype(jnp.bfloat16)

    def o_target(slot):
        return jnp.where(slot == 0, pair, last)

    def o_copy(slot, t):
        return pltpu.make_async_remote_copy(
            src_ref=obuf.at[slot, pl.ds(t * tok_dev, tok_dev)],
            dst_ref=rbuf.at[mt, head],
            send_sem=o_send.at[slot, t],
            recv_sem=o_recv,
            device_id=(o_target(slot), t),
            device_id_type=MESH,
        )

    def o_self(slot, t):
        return jnp.logical_and(o_target(slot) == me, t == mt)

    def o_body(k, c):
        slot = lax.rem(k, 2)
        t = lax.rem(mt + n_tp // 2 + lax.div(k, 2), n_tp)

        @pl.when(jnp.logical_not(o_self(slot, t)))
        def _():
            o_copy(slot, t).start()

        @pl.when(o_self(slot, t))
        def _():
            pltpu.make_async_copy(
                obuf.at[slot, pl.ds(t * tok_dev, tok_dev)], rbuf.at[mt, head], o_recv
            ).start()

        return c

    lax.fori_loop(0, 2 * n_tp, o_body, 0)

    def late_event(i, c):
        w_event(i)
        return c

    lax.fori_loop(early, events, late_event, 0)
    lax.fori_loop(passed, events, w_pass, 0)
    lax.fori_loop(0, nz - 1, w_rest, 0)

    number = lax.broadcasted_iota(jnp.int32, (n, tok_dev), 0)
    before = (
        lax.broadcasted_iota(jnp.int32, (tok_dev, tok_dev), 0)
        < lax.broadcasted_iota(jnp.int32, (tok_dev, tok_dev), 1)
    ).astype(bf16)
    expand = (
        lax.div(lax.broadcasted_iota(jnp.int32, (padded, n), 0), SLOTS)
        == lax.broadcasted_iota(jnp.int32, (padded, n), 1)
    ).astype(bf16)
    inside = lax.rem(lax.broadcasted_iota(jnp.int32, (padded, tok_dev), 0), SLOTS).astype(f32)
    eye = (
        lax.broadcasted_iota(jnp.int32, (padded, padded), 0)
        == lax.broadcasted_iota(jnp.int32, (padded, padded), 1)
    ).astype(bf16)
    first = (((0,), (0,)), ((), ()))
    taken = jnp.zeros((n, 1), f32)
    for r in range(ids_ref.shape[0]):
        named = (number == ids_ref[r : r + 1, :]).astype(f32)
        rank = jnp.dot(named.astype(bf16), before, preferred_element_type=f32) + taken
        taken = taken + jnp.sum(named, axis=1, keepdims=True)
        named_at = jnp.dot(expand, named.astype(bf16), preferred_element_type=f32)
        rank_at = jnp.dot(expand, rank.astype(bf16), preferred_element_type=f32)
        placed = jnp.where(rank_at == inside, named_at, 0.0).astype(bf16)
        place[r] = lax.dot_general(placed, eye, first, preferred_element_type=f32).astype(bf16)
    compact = lax.broadcasted_iota(jnp.int32, (expert_rows, padded), 0)
    spaced = lax.broadcasted_iota(jnp.int32, (expert_rows, padded), 1)
    keep[...] = (
        lax.div(compact, capacity) * SLOTS + lax.rem(compact, capacity) == spaced
    ).astype(bf16)
    spare = SLOTS - capacity
    each = capacity // spare
    third = lax.broadcasted_iota(jnp.int32, (expert_rows, each * padded), 1)
    kept = lax.broadcasted_iota(jnp.int32, (expert_rows, each * padded), 0)
    kept_in = lax.rem(kept, capacity)
    keep_tail[...] = jnp.logical_and(
        lax.rem(third, padded)
        == lax.div(kept, capacity) * SLOTS + capacity + lax.div(kept_in, each),
        lax.div(third, padded) == lax.rem(kept_in, each),
    ).astype(bf16)
    slot = lax.broadcasted_iota(jnp.int32, (padded, each * padded), 0)
    target = lax.broadcasted_iota(jnp.int32, (padded, each * padded), 1)
    target_row = lax.rem(target, padded)
    target_in = lax.rem(target_row, SLOTS)
    folds[...] = jnp.logical_and(
        target_in >= capacity,
        slot
        == lax.div(target_row, SLOTS) * SLOTS
        + (target_in - capacity) * each
        + lax.div(target, padded),
    ).astype(bf16)
    sent_to = place[0]
    for r in range(1, ids_ref.shape[0]):
        sent_to = sent_to + place[r]
    ext[nz - 1, :, model:] = sent_to

    pltpu.make_async_copy(rbuf, rbuf, o_recv).wait()
    own_w.wait()
    w_partner(nz - 1, z * 2 + 1 - core)
    low32 = lax.broadcasted_iota(jnp.int32, (tok_dev, width), 1) < half

    def w_arrived(k, c):
        w_partner(k, w_theirs(k))
        return c

    lax.fori_loop(0, nz - 1, w_arrived, 0)
    for t in range(n_tp):
        attended[:, t * width : (t + 1) * width] = jnp.where(
            low32, rbuf[t, 0].astype(f32), rbuf[t, 1].astype(f32)
        ).astype(bf16)
    out_tile = min(512, model)
    for i in range(model // out_tile):
        cols = slice(i * out_tile, (i + 1) * out_tile)
        sums = jnp.zeros((tok_dev, out_tile), f32)
        for t in range(0, n_tp, 2):
            sums += jnp.dot(
                attended[:, t * width : (t + 2) * width],
                wbuf[t : t + 2, :, cols].reshape(2 * width, out_tile),
                preferred_element_type=f32,
            )
        proj[:, cols] = sums
    stream = (tok_ref[...].astype(f32) + proj[...]).astype(bf16)
    stream_ref[...] = stream
    stream_wide = stream.astype(f32)
    inverse = lax.rsqrt(jnp.mean(stream_wide * stream_wide, axis=1, keepdims=True) + 1e-05)
    ext[nz - 1, :, :model] = (stream_wide * inverse * gain_ref[...]).astype(bf16)

    def ring(k):
        return pltpu.make_async_remote_copy(
            src_ref=ext.at[k],
            dst_ref=ext.at[lax.rem(k + 1, nz)],
            send_sem=x_send.at[k],
            recv_sem=x_recv.at[lax.rem(k + 1, nz)],
            device_id=nxt,
            device_id_type=MESH,
        )

    def to_expert(k, e):
        return pltpu.make_async_remote_copy(
            src_ref=packed.at[k, e],
            dst_ref=arrived.at[k, me],
            send_sem=a_send.at[k, e],
            recv_sem=a_recv.at[k],
            device_id=(e, mt),
            device_id_type=MESH,
        )

    def share(k):
        return pltpu.make_async_remote_copy(
            src_ref=xbuf.at[core, k],
            dst_ref=xbuf.at[core, k],
            send_sem=s_send.at[k],
            recv_sem=s_recv.at[k],
            device_id=partner,
            device_id_type=MESH,
        )

    parts = 3
    part_rows = expert_rows // parts

    def part(s):
        return pl.ds(s * part_rows, part_rows)

    def give(k, s):
        return pltpu.make_async_remote_copy(
            src_ref=psend.at[k, part(s)],
            dst_ref=precv.at[k, part(s)],
            send_sem=p_send.at[k, s],
            recv_sem=p_recv.at[k, s],
            device_id=partner,
            device_id_type=MESH,
        )

    def reduce(k, s):
        return pltpu.make_async_remote_copy(
            src_ref=rsend.at[k, part(s)],
            dst_ref=rrecv.at[k, part(s)],
            send_sem=r_send.at[k, s],
            recv_sem=r_recv.at[k, s],
            device_id=nxt,
            device_id_type=MESH,
        )

    def to_token(s):
        return pltpu.make_async_remote_copy(
            src_ref=spread.at[s],
            dst_ref=back.at[me],
            send_sem=t_send.at[s],
            recv_sem=t_recv,
            device_id=(s, mt),
            device_id_type=MESH,
        )

    body = model * capacity // SLOTS
    fold = body // each

    def unfolded(flat):
        return jnp.concatenate([flat[:, j * fold : (j + 1) * fold] for j in range(each)], axis=0)

    def dispatch(k):
        @pl.when(k < nz - 1)
        def _():
            pltpu.make_async_copy(ext.at[0], ext.at[k], x_recv.at[k]).wait()

        @pl.when(k != nz - 2)
        def _():
            ring(k).start()

        main = ext[k, :, model:]
        tails = jnp.dot(main, folds[...], preferred_element_type=f32).astype(bf16)
        last_columns = ext[k, :, body:model]
        for j in range(each):
            cols = slice(j * fold, (j + 1) * fold)
            block = lax.dot_general(
                jnp.concatenate([main, tails[:, j * padded : (j + 1) * padded]], axis=0),
                jnp.concatenate([ext[k, :, cols], last_columns], axis=0),
                first,
                preferred_element_type=f32,
            ).astype(bf16)
            for e in range(n):
                packed[k, e, :, cols] = block[e * SLOTS : (e + 1) * SLOTS]
        pltpu.make_async_copy(packed.at[k, me], arrived.at[k, me], a_recv.at[k]).start()

        def send(i, c):
            to_expert(k, lax.rem(me + i, n)).start()
            return c

        lax.fori_loop(1, n, send, 0)

    def first_dispatch(i, c):
        dispatch(lax.rem(i + nz - 1, nz))
        return c

    ahead = min(3, nz - 1)
    lax.fori_loop(0, ahead + 1, first_dispatch, 0)
    for load in loads[5:]:
        load.wait()

    col_tile = min(512, model)
    across = (((1,), (1,)), ((), ()))

    def gather(k):
        pltpu.make_async_copy(arrived.at[k], arrived.at[k], a_recv.at[k]).wait()
        flat = arrived[k].reshape(padded, body)
        xbuf[core, k, :, :body] = jnp.dot(
            keep[...], flat, preferred_element_type=f32
        ).astype(bf16)
        xbuf[core, k, :, body:] = jnp.dot(
            keep_tail[...], unfolded(flat), preferred_element_type=f32
        ).astype(bf16)
        share(k).start()

    gather(0)

    def step(k, c):
        pltpu.make_async_copy(xbuf.at[1 - core, 0], xbuf.at[1 - core, k], s_recv.at[k]).wait()

        x = jnp.concatenate([xbuf[1 - core, k], xbuf[core, k]], axis=0)
        g = lax.dot_general(x, gate[...], across, preferred_element_type=f32)
        u = lax.dot_general(x, up[...], across, preferred_element_type=f32)
        hidden = (g / (1.0 + jnp.exp(-g)) * u).astype(bf16)
        for i in range(model // col_tile):
            cols = slice(i * col_tile, (i + 1) * col_tile)
            p = jnp.dot(hidden, down[:, cols], preferred_element_type=f32)
            psend[k, :, cols] = p[:expert_rows].astype(bf16)
            pown[:, cols] = p[expert_rows:]
        for s in range(parts):
            give(k, s).start()

        @pl.when(k + ahead < nz - 1)
        def _():
            dispatch(k + ahead)

        @pl.when(k < nz - 1)
        def _():
            gather(k + 1)

        for s in range(parts):
            give(k, s).wait_recv()
            both = pown[part(s), :] + precv[k, part(s), :].astype(f32)

            @pl.when(k > 0)
            def _():
                kk = jnp.maximum(k - 1, 0)
                reduce(kk, s).wait_recv()
                pown[part(s), :] = both + rrecv[kk, part(s), :].astype(f32)

            @pl.when(k == 0)
            def _():
                pown[part(s), :] = both

            @pl.when(k < nz - 1)
            def _():
                rsend[k, part(s), :] = pown[part(s), :].astype(bf16)
                reduce(k, s).start()

        return c

    lax.fori_loop(0, nz, step, 0)

    for j in range(each):
        cols = slice(j * fold, (j + 1) * fold)
        scattered = lax.dot_general(
            jnp.concatenate([keep[...], keep_tail[:, j * padded : (j + 1) * padded]], axis=0),
            jnp.concatenate([pown[:, cols], pown[:, body:]], axis=0).astype(bf16),
            first,
            preferred_element_type=f32,
        ).astype(bf16)
        for s in range(n):
            spread[s, :, cols] = scattered[s * SLOTS : (s + 1) * SLOTS]
    pltpu.make_async_copy(spread.at[me], back.at[me], t_recv).start()

    def return_body(k, c):
        to_token(lax.rem(me + k, n)).start()
        return c

    lax.fori_loop(1, n, return_body, 0)

    q_copy.wait_send()

    def drain_body(k, c):
        r = lax.rem(me + k, n)

        @pl.when(me <= jnp.maximum(r, n - 1 - r))
        def _():
            ck, cb = kv_copy(r)
            cb.wait_send()
            ck.wait_send()

        return c

    lax.fori_loop(1, n, drain_body, 0)

    def o_drain(k, c):
        slot = lax.rem(k, 2)
        t = lax.div(k, 2)

        @pl.when(jnp.logical_not(o_self(slot, t)))
        def _():
            o_copy(slot, t).wait_send()

        return c

    lax.fori_loop(0, 2 * n_tp, o_drain, 0)

    def w_drain(k, c):
        for s in range(2):
            w_share(k, s, w_ref).wait_send()

            @pl.when(k != nz - 2)
            def _():
                w_ring(k, s, w_ref).wait_send()

        w_share_rest(k, w_ref).wait_send()

        @pl.when(k < nz - 1)
        def _():
            for i in range(4):
                w_plane(k, i, neighbours[i], w_ref).wait_send()

        return c

    lax.fori_loop(0, nz, w_drain, 0)

    def drain(k, c):
        for s in range(parts):
            give(k, s).wait_send()

            @pl.when(k < nz - 1)
            def _():
                reduce(k, s).wait_send()

        @pl.when(k != nz - 2)
        def _():
            ring(k).wait_send()

        share(k).wait_send()

        def drain_send(i, c):
            to_expert(k, lax.rem(me + i, n)).wait_send()
            return c

        lax.fori_loop(1, n, drain_send, 0)
        return c

    lax.fori_loop(0, nz, drain, 0)

    pltpu.make_async_copy(back, back, t_recv).wait()
    rows_back = back[...].reshape(padded, body)
    tails_back = unfolded(rows_back)
    diagonal = lax.broadcasted_iota(jnp.int32, (tok_dev, tok_dev), 0) == lax.broadcasted_iota(
        jnp.int32, (tok_dev, tok_dev), 1
    )
    mixture = jnp.zeros((tok_dev, body), f32)
    mixture_tail = jnp.zeros((tok_dev, model - body), f32)
    for r in range(ids_ref.shape[0]):
        chosen = place[r]
        tails = jnp.dot(chosen, folds[...], preferred_element_type=f32).astype(bf16)
        weight = jnp.sum(
            jnp.where(diagonal, route_ref[r : r + 1, :], 0.0), axis=1, keepdims=True
        )
        mixture += weight * jnp.dot(chosen, rows_back, preferred_element_type=f32)
        mixture_tail += weight * jnp.dot(tails, tails_back, preferred_element_type=f32)
    out_ref[:, :body] = (stream_ref[:, :body].astype(f32) + mixture).astype(bf16)
    out_ref[:, body:] = (stream_ref[:, body:].astype(f32) + mixture_tail).astype(bf16)

    def drain_back(k, c):
        to_token(lax.rem(me + k, n)).wait_send()
        return c

    lax.fori_loop(1, n, drain_back, 0)


def shards(
    tokens,
    query_vectors,
    key_vectors,
    value_vectors,
    cum_gate,
    out_weight,
    norm_gain,
    gate_weight,
    up_weight,
    down_weight,
    expert_ids,
    route_weights,
):
    n = lax.axis_size("sp")
    n_tp = lax.axis_size("tp")
    nz = n_tp // 2
    rows, width = query_vectors.shape
    tok_dev, model = tokens.shape
    top = expert_ids.shape[1]
    inner = gate_weight.shape[2]
    capacity = max(2, 3 * tok_dev * top // (2 * n))
    assert capacity < SLOTS and capacity % (SLOTS - capacity) == 0 and gate_weight.shape[0] == 1
    each = capacity // (SLOTS - capacity)
    body = model * capacity // SLOTS
    expert_rows = n * capacity
    padded = n * SLOTS
    coef = (width // 2) ** (-0.5) * math.log2(math.e)
    vmem = pl.BlockSpec(memory_space=pltpu.VMEM)
    hbm = pl.BlockSpec(memory_space=pl.ANY)
    bf16, f32 = jnp.bfloat16, jnp.float32
    dma = pltpu.SemaphoreType.DMA
    return pl.pallas_call(
        functools.partial(layer_kernel, n, n_tp, coef, capacity),
        out_shape=jax.ShapeDtypeStruct((tok_dev, model), bf16),
        in_specs=[hbm, hbm, hbm, vmem, hbm, hbm, vmem, vmem, vmem, hbm, hbm, hbm],
        out_specs=vmem,
        scratch_shapes=[
            pltpu.VMEM((rows, width), bf16),
            pltpu.VMEM((rows, width), bf16),
            pltpu.VMEM((rows, width), bf16),
            pltpu.VMEM((width, model), bf16),
            pltpu.VMEM((tok_dev, model), bf16),
            pltpu.VMEM((inner, model), bf16),
            pltpu.VMEM((inner, model), bf16),
            pltpu.VMEM((inner, model), bf16),
            pltpu.VMEM((rows, width), bf16),
            pltpu.VMEM((2, rows, width), bf16),
            pltpu.VMEM((2, rows, width), bf16),
            pltpu.VMEM((2, 1, rows), f32),
            pltpu.VMEM((n, rows, width), bf16),
            pltpu.VMEM((n, 1, rows), f32),
            pltpu.VMEM((2, rows, 1), f32),
            pltpu.VMEM((2, rows, 1), f32),
            pltpu.VMEM((2, rows, width), f32),
            pltpu.VMEM((2, rows, width), bf16),
            pltpu.VMEM((n_tp, 2, tok_dev, width), bf16),
            pltpu.VMEM((n_tp, width, model), bf16),
            pltpu.VMEM((tok_dev, model), bf16),
            pltpu.VMEM((tok_dev, model), f32),
            pltpu.VMEM((tok_dev, model), bf16),
            pltpu.VMEM((top, tok_dev, padded), bf16),
            pltpu.VMEM((expert_rows, padded), bf16),
            pltpu.VMEM((expert_rows, each * padded), bf16),
            pltpu.VMEM((padded, each * padded), bf16),
            pltpu.VMEM((nz, tok_dev, model + padded), bf16),
            pltpu.VMEM((nz, n, SLOTS, body), bf16),
            pltpu.VMEM((nz, n, SLOTS, body), bf16),
            pltpu.VMEM((2, nz, expert_rows, model), bf16),
            pltpu.VMEM((expert_rows, model), f32),
            pltpu.VMEM((nz, expert_rows, model), bf16),
            pltpu.VMEM((nz, expert_rows, model), bf16),
            pltpu.VMEM((nz - 1, expert_rows, model), bf16),
            pltpu.VMEM((nz - 1, expert_rows, model), bf16),
            pltpu.VMEM((n, SLOTS, body), bf16),
            pltpu.VMEM((n, SLOTS, body), bf16),
            dma((8,)),
            dma((n,)),
            dma((n,)),
            dma((n,)),
            dma((n,)),
            dma,
            dma,
            dma((2, n_tp)),
            dma,
            dma((nz, 2)),
            dma((nz, 2)),
            dma((nz, 3)),
            dma((nz, 3)),
            dma((nz - 1, 4)),
            dma((nz - 1,)),
            dma((1,)),
            dma((nz,)),
            dma((nz,)),
            dma((nz, n)),
            dma((nz,)),
            dma((nz,)),
            dma((nz,)),
            dma((nz, 3)),
            dma((nz, 3)),
            dma((nz - 1, 3)),
            dma((nz - 1, 3)),
            dma((n,)),
            dma,
        ],
        compiler_params=pltpu.CompilerParams(
            collective_id=0, has_side_effects=True, vmem_limit_bytes=67000000
        ),
        name="layer",
    )(
        query_vectors,
        key_vectors,
        value_vectors,
        cum_gate.T,
        out_weight,
        tokens,
        norm_gain[None, :],
        expert_ids.T,
        route_weights.T,
        jnp.swapaxes(gate_weight[0], 0, 1),
        jnp.swapaxes(up_weight[0], 0, 1),
        down_weight[0],
    )


def solution(mesh):
    in_specs = (
        P(("sp", "tp"), None),
        P("sp", "tp"),
        P("sp", "tp"),
        P("sp", "tp"),
        P("sp", "tp"),
        P("tp", None),
        P(),
        P("sp", None, "tp"),
        P("sp", None, "tp"),
        P("sp", "tp", None),
        P(("sp", "tp"), None),
        P(("sp", "tp"), None),
    )
    out_specs = P(("sp", "tp"), None)
    return jax.shard_map(shards, mesh=mesh, in_specs=in_specs, out_specs=out_specs, check_vma=False)
```
